32 devices in a mesh: sp: 4 (over y, x), dp: 8 (over z, core).
Axes of the slice: x: 2, y: 2, z: 4, core: 2. Of those that a mesh axis runs over, the one named last changes fastest.
Arguments:
- value_half: bfloat16 [8, 1024, 2048], P('dp', 'sp'), may hold values from -6 to 6
- gate_half: bfloat16 [8, 1024, 2048], P('dp', 'sp'), may hold values from -6 to 6
- upstream: bfloat16 [8, 1024, 2048], P('dp', 'sp'), may hold values from -6 to 6
- conv_taps: float32 [31, 2048], P(None, 'sp'), may hold values from -1 to 1
- norm_gain: float32 [2048], replicated, may hold values from 0.1 to 1.9
- out_weight: bfloat16 [2048, 2048], P('dp'), may hold values from -0.125 to 0.125
Outputs:
- grad_value: bfloat16 [8, 1024, 2048], P('dp', 'sp')
- grad_gate: bfloat16 [8, 1024, 2048], P('dp', 'sp')
- grad_taps: float32 [31, 2048], P(None, 'sp')
- grad_gain: float32 [2048], replicated
- grad_weight: float32 [2048, 2048], P('dp')
The draws below stay inside these ranges and needn't reach their ends.
All inputs are finite; a program needn't handle non-finite values.
Results may differ from the reference program's by a relative error of at most 0.0062.
Values may be sent and summed in bfloat16 or wider, within the bound.
A program may use at most 128 MiB of HBM per device.

```python
import jax
import jax.numpy as jnp
from jax import lax

D = 2048
KERNEL = 31
LENGTH = 1024
BATCH = 8


def spiked(drawn, rng, source, target, parts, factor):
    owner, partner = [(jnp.arange(drawn.shape[dim]) // (drawn.shape[dim] // parts)).reshape([-1 if axis == dim else 1 for axis in range(drawn.ndim)]) for dim in (source, target)]
    chosen = jax.random.permutation(rng, parts)[partner]
    strong = (owner == chosen) | (owner == (partner + parts // 2) % parts)
    return jnp.where(strong, factor * drawn, drawn)


def block_levels(stream_key, dims, pieces, low, largest):
    level = 1.0
    for axis_at, blocks in pieces:
        draws = jax.random.uniform(jax.random.fold_in(jax.random.fold_in(stream_key, 6), axis_at), (blocks,), jnp.float32, low / len(pieces), largest / len(pieces))
        level = level * jnp.repeat(jnp.exp(draws), dims[axis_at] // blocks).reshape((-1,) + (1,) * (len(dims) - 1 - axis_at))
    return level


def normal_values(own_key, shape, scale, bound, pieces=(), held_as=jnp.bfloat16):
    drawn = scale * jax.random.normal(own_key, shape, jnp.float32)
    if pieces:
        drawn = drawn * block_levels(own_key, shape, pieces, -0.22, 0.18)
    return jnp.clip(drawn, -bound, bound).astype(held_as)


def bell_draw_with(rng, shape, spread, limit, cuts, heavy, dtype=jnp.bfloat16):
    drawn = spread * jax.random.normal(rng, shape, jnp.float32)
    if cuts:
        drawn = drawn * block_levels(rng, shape, cuts, -0.22, 0.18)
    return jnp.clip(spiked(drawn, jax.random.fold_in(rng, 3), *heavy), -limit, limit).astype(dtype)


def setup_inputs(seed: int = 0) -> dict:
    splits = jax.random.split(jax.random.key(seed), 7)
    return {
        "value_half": normal_values(splits[0], (BATCH, LENGTH, D), 1.0, 6.0, ((0, 8), (1, 4))),
        "gate_half": normal_values(splits[1], (BATCH, LENGTH, D), 1.0, 6.0, ((0, 8), (1, 4))),
        "upstream": bell_draw_with(splits[2], (BATCH, LENGTH, D), 1.0, 6.0, ((0, 8), (1, 4)), (0, 2, 8, 2.0)),
        "conv_taps": normal_values(splits[3], (KERNEL, D), 0.18, 1.0, ((1, 4),), jnp.float32),
        "norm_gain": jnp.clip(1.0 + 0.18 * jax.random.normal(splits[4], (D,), jnp.float32), 0.1, 1.9),
        "out_weight": normal_values(splits[5], (D, D), D ** -0.5, 0.125, ((0, 8),)),
    }


NORM_EPS = 1e-05

def one_sequence(sequence, conv_taps, norm_gain, out_weight):
    value_half, gate_half, upstream = sequence
    tap_count = conv_taps.shape[0]
    length = value_half.shape[0]
    sig_gate = jax.nn.sigmoid(gate_half.astype(jnp.float32))
    value_wide = value_half.astype(jnp.float32)
    glu = (value_wide * sig_gate).astype(jnp.bfloat16)
    glu_wide = lax.optimization_barrier(glu).astype(jnp.float32)
    padded = jnp.pad(glu_wide, ((tap_count - 1, 0), (0, 0)))
    conv_out = jnp.zeros_like(glu_wide)
    for offset in range(tap_count):
        conv_out = conv_out + conv_taps[offset] * padded[offset:offset + length]
    conv_out = lax.optimization_barrier(conv_out.astype(jnp.bfloat16)).astype(jnp.float32)
    row_mean = lax.optimization_barrier(jnp.mean(conv_out, axis=-1, keepdims=True))
    centered = conv_out - row_mean
    inv_scale = lax.rsqrt(lax.optimization_barrier(jnp.mean(centered * centered, axis=-1, keepdims=True)) + NORM_EPS)
    normed = centered * inv_scale
    scaled = normed * norm_gain
    sig_scaled = jax.nn.sigmoid(scaled)
    activated = (scaled * sig_scaled).astype(jnp.bfloat16)
    grad_act = jnp.dot(upstream, out_weight, preferred_element_type=jnp.float32)
    grad_scaled = grad_act * sig_scaled * (1.0 + scaled * (1.0 - sig_scaled))
    gain_term = lax.optimization_barrier(jnp.sum(grad_scaled * normed, axis=0))
    grad_normed = grad_scaled * norm_gain
    grad_conv_out = inv_scale * (grad_normed - lax.optimization_barrier(jnp.mean(grad_normed, axis=-1, keepdims=True)) - normed * lax.optimization_barrier(jnp.mean(grad_normed * normed, axis=-1, keepdims=True)))
    grad_conv_out = lax.optimization_barrier(grad_conv_out.astype(jnp.bfloat16)).astype(jnp.float32)
    grad_padded = jnp.pad(grad_conv_out, ((0, tap_count - 1), (0, 0)))
    grad_glu = jnp.zeros_like(grad_conv_out)
    tap_terms = []
    for offset in range(tap_count):
        first = tap_count - 1 - offset
        grad_glu = grad_glu + conv_taps[offset] * grad_padded[first:first + length]
        tap_terms.append(lax.optimization_barrier(jnp.sum(grad_conv_out * padded[offset:offset + length], axis=0)))
    grad_glu = lax.optimization_barrier(grad_glu.astype(jnp.bfloat16)).astype(jnp.float32)
    grad_value = (grad_glu * sig_gate).astype(jnp.bfloat16)
    grad_gate = (grad_glu * value_wide * sig_gate * (1.0 - sig_gate)).astype(jnp.bfloat16)
    return (grad_value, grad_gate, activated, jnp.stack(tap_terms), gain_term)

def reference(value_half, gate_half, upstream, conv_taps, norm_gain, out_weight):

    def mapped(sequence):
        return one_sequence(sequence, conv_taps, norm_gain, out_weight)
    grad_value, grad_gate, activated, tap_terms, gain_terms = lax.map(mapped, (value_half, gate_half, upstream))
    model_width = value_half.shape[2]
    grad_weight = lax.dot_general(upstream.reshape(-1, model_width), activated.reshape(-1, model_width), (((0,), (0,)), ((), ())), preferred_element_type=jnp.float32)
    grad_taps = lax.optimization_barrier(jnp.sum(tap_terms, axis=0))
    grad_gain = lax.optimization_barrier(jnp.sum(gain_terms, axis=0))
    return (grad_value, grad_gate, grad_taps, grad_gain, grad_weight)
```

```python
import functools

import jax
import jax.numpy as jnp
from jax import lax
from jax.experimental import pallas as pl
from jax.experimental.pallas import tpu as pltpu
from jax.sharding import PartitionSpec as P

NORM_EPS = 1e-05
VMEM = pl.BlockSpec(memory_space=pltpu.VMEM)


def when(condition, act):
    if condition is None:
        act()
    else:
        pl.when(condition)(lambda: act())


class Copies:
    def __init__(self, send, recv, local):
        self.send, self.recv, self.local = send, recv, local
        self.n_remote = self.n_local = 0
        self.remote, self.locals = [], []

    def start(self, src, dst, target, sends=None, receives=None):
        i = self.n_remote
        self.n_remote += 1
        copy = pltpu.make_async_remote_copy(
            src_ref=src,
            dst_ref=dst,
            send_sem=self.send.at[i],
            recv_sem=self.recv.at[i],
            device_id=target,
            device_id_type=pl.DeviceIdType.MESH,
        )
        when(sends, copy.start)
        self.remote.append([copy, False, sends, receives])
        return len(self.remote) - 1

    def keep(self, src, dst):
        copy = pltpu.make_async_copy(src, dst, self.local.at[self.n_local])
        self.n_local += 1
        copy.start()
        self.locals.append(copy)

    def arrive(self, i):
        when(self.remote[i][3], self.remote[i][0].wait_recv)
        self.remote[i][1] = True

    def finish(self):
        for copy, arrived, sends, receives in self.remote:
            if not arrived:
                when(receives, copy.wait_recv)
            when(sends, copy.wait_send)
        for copy in self.locals:
            copy.wait()


def greet(axes):
    barrier = pltpu.get_barrier_semaphore()
    count = 0
    for axis in axes:
        n = lax.axis_size(axis)
        me = lax.axis_index(axis)
        for k in range(1, n):
            pl.semaphore_signal(
                barrier,
                inc=1,
                device_id={axis: lax.rem(me + k, n)},
                device_id_type=pl.DeviceIdType.MESH,
            )
            count += 1
    pl.semaphore_wait(barrier, count)


def direct(copies, kind, axis, src, dst):
    n = lax.axis_size(axis)
    me = lax.axis_index(axis)
    if kind == "next" or kind == "prev":
        copies.start(src, dst, {axis: lax.rem(me + (1 if kind == "next" else n - 1), n)})
        return
    if kind == "pair":
        copies.start(src, dst, {axis: me + 1 - 2 * lax.rem(me, 2)})
        return
    if kind == "rows":
        nz, z, c = n // 2, me // 2, lax.rem(me, 2)
        copies.keep(src.at[z], dst.at[z])
        for k in range(1, nz):
            peer = lax.rem(z + k, nz)
            copies.start(src.at[peer], dst.at[z], {axis: 2 * peer + c})
        return
    copies.keep(src.at[me] if kind == "scatter" else src, dst.at[me])
    for k in range(1, n):
        peer = lax.rem(me + k, n)
        copies.start(src.at[peer] if kind == "scatter" else src, dst.at[me], {axis: peer})


def spread_gather(copies, src, dst):
    ns, nz = lax.axis_size("sp"), lax.axis_size("dp") // 2
    s, d = lax.axis_index("sp"), lax.axis_index("dp")
    z, c = d // 2, lax.rem(d, 2)
    partner = {"dp": d + 1 - 2 * c}
    first = [
        copies.start(src.at[s], dst.at[d, s], {"dp": 2 * lax.rem(z + k, nz) + c})
        for k in range(1, nz)
    ]
    yield
    copies.keep(src, dst.at[d])
    copies.start(src, dst.at[d], partner)
    second = {}
    for k in range(1, nz):
        copies.arrive(first[k - 1])
        piece = dst.at[2 * lax.rem(z + nz - k, nz) + c, s]
        for j in range(1, ns):
            second[k, j] = copies.start(piece, piece, {"sp": lax.rem(s + j, ns)})
        copies.start(piece, piece, partner)
    yield
    for k in range(1, nz):
        for j in range(1, ns):
            copies.arrive(second[k, j])
            piece = dst.at[2 * lax.rem(z + nz - k, nz) + c, lax.rem(s + ns - j, ns)]
            copies.start(piece, piece, partner)


def line_gather(copies, src, dst):
    nz = lax.axis_size("dp") // 2
    d = lax.axis_index("dp")
    z, c = d // 2, lax.rem(d, 2)
    partner = {"dp": d + 1 - 2 * c}
    up = {"dp": 2 * lax.rem(z + 1, nz) + c}
    down = {"dp": 2 * lax.rem(z + nz - 1, nz) + c}
    below, above = {}, {}

    def send(k):
        low, high = 2 * lax.rem(z + nz - k, nz) + c, 2 * lax.rem(z + k, nz) + c
        low_src, high_src = (dst.at[low], dst.at[high]) if k else (src, src)
        below[k] = copies.start(
            low_src, dst.at[low], up, jnp.logical_and(z >= k, z < nz - 1), z >= k + 1
        )
        above[k] = copies.start(
            high_src, dst.at[high], down, jnp.logical_and(z + k < nz, z > 0), z + k + 1 < nz
        )

    send(0)
    yield
    copies.keep(src, dst.at[d])
    copies.start(src, dst.at[d], partner)
    for k in range(1, nz):
        copies.arrive(below[k - 1])
        copies.arrive(above[k - 1])
        if k < nz - 1:
            send(k)
        low, high = dst.at[2 * lax.rem(z + nz - k, nz) + c], dst.at[2 * lax.rem(z + k, nz) + c]
        copies.start(low, low, partner, z >= k, z >= k)
        copies.start(high, high, partner, z + k < nz, z + k < nz)
        yield


def run(axes, items, *refs):
    n = len(items)
    copies = Copies(*refs[2 * n :])
    greet(axes)
    waiting = []
    for i, (kind, axis) in enumerate(items):
        src, dst = refs[i], refs[n + i]
        if kind == "spread":
            waiting.append(spread_gather(copies, src, dst))
        elif kind == "line":
            waiting.append(line_gather(copies, src, dst))
        elif kind == "later":
            waiting.append(later(copies, axis, src, dst))
        else:
            direct(copies, kind, axis, src, dst)
    while waiting:
        waiting = [steps for steps in waiting if next(steps, waiting) is None]
    copies.finish()


def later(copies, axis, src, dst):
    yield
    direct(copies, "scatter", axis, src, dst)


def exchange(collective_id, *items):
    ns, nd = lax.axis_size("sp"), lax.axis_size("dp")
    shapes, remote, local = [], 0, 0
    for kind, axis, x in items:
        n = lax.axis_size(axis)
        if kind == "rows":
            shape = x.shape
            remote += n // 2 - 1
            local += 1
        elif kind in ("next", "prev", "pair"):
            shape = x.shape
            remote += 1
        elif kind in ("scatter", "later"):
            shape = x.shape
            remote += n - 1
            local += 1
        else:
            shape = (n,) + x.shape
            local += 1
            if kind == "gather":
                remote += n - 1
            elif kind == "spread":
                remote += (nd // 2 - 1) * 2 * ns + 1
            else:
                remote += (nd // 2 - 1) * 4 + 1
        shapes.append(jax.ShapeDtypeStruct(shape, x.dtype))
    axes = tuple(a for a in ("sp", "dp") if any(axis == a or kind == "spread" for kind, axis, _ in items))
    return pl.pallas_call(
        functools.partial(run, axes, tuple((kind, axis) for kind, axis, _ in items)),
        out_shape=shapes,
        in_specs=[VMEM] * len(items),
        out_specs=[VMEM] * len(items),
        scratch_shapes=[
            pltpu.SemaphoreType.DMA((remote,)),
            pltpu.SemaphoreType.DMA((remote,)),
            pltpu.SemaphoreType.DMA((max(local, 1),)),
        ],
        compiler_params=pltpu.CompilerParams(
            collective_id=collective_id, has_side_effects=True, vmem_limit_bytes=48 * 1024 * 1024
        ),
    )(*[x for _, _, x in items])


def body(value_half, gate_half, upstream, conv_taps, norm_gain, out_weight):
    f32 = jnp.float32
    tap_count = conv_taps.shape[0]
    halo = tap_count - 1
    nsp, ndp = lax.axis_size("sp"), lax.axis_size("dp")
    at_start = lax.axis_index("sp") == 0
    at_end = lax.axis_index("sp") == nsp - 1
    edge = (halo + 15) // 16 * 16

    value = value_half[0].astype(f32)
    gate = gate_half[0].astype(f32)
    length = value.shape[0]
    channels = value.shape[1]
    up = upstream[0]
    rows = out_weight.shape[0]

    tail = (value[length - edge :] * jax.nn.sigmoid(gate[length - edge :])).astype(jnp.bfloat16)
    up_blocks = jnp.swapaxes(up.reshape(length, ndp, rows), 0, 1)
    before, taps = exchange(1, ("next", "sp", tail), ("gather", "sp", conv_taps))
    before = jnp.where(at_start, 0, before)[edge - halo :]
    taps = jnp.swapaxes(taps, 0, 1).reshape(tap_count, channels)
    sig_gate = jax.nn.sigmoid(gate)
    glu = (value * sig_gate).astype(jnp.bfloat16)
    padded = jnp.concatenate([before, glu], axis=0).astype(f32)
    conv = jnp.zeros((length, padded.shape[1]), f32)
    for j in range(tap_count):
        conv = conv + taps[j] * padded[j : j + length]
    conv = conv.astype(jnp.bfloat16).astype(f32)
    mean = jnp.mean(conv, axis=-1, keepdims=True)
    centered = conv - mean
    inv = lax.rsqrt(jnp.mean(centered * centered, axis=-1, keepdims=True) + NORM_EPS)
    normed = centered * inv
    scaled = normed * norm_gain
    sig = jax.nn.sigmoid(scaled)
    activated = (scaled * sig).astype(jnp.bfloat16)

    half = channels // 2
    nz, piece = ndp // 2, rows // nsp
    core = lax.rem(lax.axis_index("dp"), 2)
    by_core = up.reshape(length, nz, 2, nsp, piece)

    def partial(which):
        columns = lax.dynamic_index_in_dim(by_core, which, 2, keepdims=False)
        columns = jnp.swapaxes(columns, 1, 2).reshape(length, nsp * nz * piece)
        return lax.dot_general(
            columns, activated[:, half:], (((0,), (0,)), ((), ())), preferred_element_type=f32
        )

    weight, act_all, up_columns, from_partner = exchange(
        2,
        ("spread", "dp", out_weight.reshape(nsp, rows // nsp, channels)),
        ("line", "dp", activated[:, :half]),
        ("later", "dp", up_blocks),
        ("pair", "dp", partial(1 - core).astype(jnp.bfloat16)),
    )
    weight = weight.reshape(ndp * rows, channels)
    act_all = act_all.reshape(ndp * length, half)
    up_columns = up_columns.reshape(ndp * length, rows)
    owned = lax.dot_general(
        up_columns, act_all, (((0,), (0,)), ((), ())), preferred_element_type=f32
    )
    summed = (partial(core) + from_partner.astype(f32)).astype(jnp.bfloat16)
    summed = summed.reshape(nsp, nz, piece, half)

    grad_act = jnp.dot(up, weight, preferred_element_type=f32)
    grad_scaled = grad_act * sig * (1.0 + scaled * (1.0 - sig))
    gain_part = jnp.sum(grad_scaled * normed, axis=0)
    g = grad_scaled * norm_gain
    grad_conv = inv * (
        g
        - jnp.mean(g, axis=-1, keepdims=True)
        - normed * jnp.mean(g * normed, axis=-1, keepdims=True)
    )
    grad_conv = grad_conv.astype(jnp.bfloat16)
    after, gain_got, owned_got, summed_got = exchange(
        3,
        ("prev", "sp", grad_conv[:edge]),
        ("gather", "sp", gain_part[None]),
        ("scatter", "sp", owned.astype(jnp.bfloat16).reshape(nsp, piece, half)),
        ("scatter", "sp", summed),
    )
    after = jnp.where(at_end, 0, after)[:halo]
    extended = jnp.concatenate([grad_conv, after], axis=0).astype(f32)
    here = grad_conv.astype(f32)
    grad_glu = jnp.zeros_like(here)
    terms = []
    for j in range(tap_count):
        first = halo - j
        grad_glu = grad_glu + taps[j] * extended[first : first + length]
        terms.append(jnp.sum(here * padded[j : j + length], axis=0))
    grad_glu = grad_glu.astype(jnp.bfloat16).astype(f32)
    grad_value = (grad_glu * sig_gate).astype(jnp.bfloat16)
    grad_gate = (grad_glu * value * sig_gate * (1.0 - sig_gate)).astype(jnp.bfloat16)

    width = conv_taps.shape[1]
    tap_blocks = jnp.swapaxes(jnp.stack(terms).reshape(tap_count, nsp, width), 0, 1)
    gain_got, tap_got, low_weight, high_got = exchange(
        4,
        ("gather", "dp", jnp.sum(gain_got, axis=0)),
        ("scatter", "sp", tap_blocks),
        ("gather", "sp", jnp.sum(owned_got.astype(f32), axis=0).astype(jnp.bfloat16)),
        ("rows", "dp", jnp.sum(summed_got.astype(f32), axis=0).astype(jnp.bfloat16)),
    )
    tap_got, high_weight = exchange(
        5,
        ("gather", "dp", jnp.sum(tap_got, axis=0)),
        ("gather", "sp", jnp.sum(high_got.astype(f32), axis=0).astype(jnp.bfloat16)),
    )
    grad_gain = jnp.sum(gain_got, axis=0)[0]
    grad_taps = jnp.sum(tap_got, axis=0)
    grad_weight = jnp.concatenate(
        [low_weight.reshape(rows, half), high_weight.reshape(rows, half)], axis=1
    ).astype(f32)
    return (grad_value[None], grad_gate[None], grad_taps, grad_gain, grad_weight)


BLOCK = 64
LANES = 128


class Net:
    def __init__(self, send, recv, local):
        self.send, self.recv, self.local = send, recv, local
        self.n = self.m = 0
        self.open = []
        self.landing = []

    def ids(self, count):
        self.n += count
        return self.n - count

    def put(self, src, dst, to, slot=None, sends=None):
        i = self.ids(1)
        copy = pltpu.make_async_remote_copy(
            src_ref=src,
            dst_ref=dst,
            send_sem=self.send.at[i],
            recv_sem=self.recv.at[i if slot is None else slot],
            device_id=to,
            device_id_type=pl.DeviceIdType.MESH,
        )
        copy.start()
        self.open.append(copy)
        return copy

    def arrival(self, ref, slot, to):
        pltpu.make_async_remote_copy(
            src_ref=ref,
            dst_ref=ref,
            send_sem=self.send.at[0],
            recv_sem=self.recv.at[slot],
            device_id=to,
            device_id_type=pl.DeviceIdType.MESH,
        ).wait_recv()

    def load(self, src, dst):
        copy = pltpu.make_async_copy(src, dst, self.local.at[self.m])
        self.m += 1
        copy.start()
        return copy

    def finish(self):
        for copy in self.open:
            copy.wait_send()


def nearest(z, nz, i):
    low, high = z, nz - 1 - z
    both = 2 * jnp.minimum(low, high)
    away = jnp.where(i < both, i // 2 + 1, i - both // 2 + 1)
    up = jnp.where(i < both, i % 2 == 0, high > low)
    return jnp.where(up, z + away, z - away)


def fused(
    value_hbm, gate_hbm, up_hbm, taps_hbm, gain_hbm, weight_hbm,
    grad_value, grad_gate, grad_taps, grad_gain, grad_weight,
    value, gate, ups, taps, gain, weight, tail, before, padded, conv, scale, acts, act,
    parts, got_x, got_y, got_xy, got_yx, plane, got_z, final, halves, give_x, give_y,
    grad_act, head, after, grads, tap_sums, gain_sum, terms, got_terms, got_dp, row_part, both_parts,
    tap_other, gain_rows,
    send, recv, local,
):
    f32, bf16 = jnp.float32, jnp.bfloat16
    nsp, ndp = lax.axis_size("sp"), lax.axis_size("dp")
    nz = ndp // 2
    s, d = lax.axis_index("sp"), lax.axis_index("dp")
    z, c = d // 2, lax.rem(d, 2)
    xn, yn = s + 1 - 2 * lax.rem(s, 2), lax.rem(s + 2, nsp)
    dg = nsp - 1 - s
    length, channels = value.shape
    halo = before.shape[0]
    tap_count = taps.shape[1]
    width = taps.shape[2]
    rows = weight.shape[0] // ndp
    half = channels // 2
    side = half // 2
    quarter = channels // nsp
    share = 2 * rows // nsp
    tiles = channels // LANES
    at_row = tap_count - (terms.shape[1] - 8)
    net = Net(send, recv, local)
    to_x, to_y, to_d, partner = {"sp": xn}, {"sp": yn}, {"sp": dg}, {"dp": d + 1 - 2 * c}

    def at_chip(peer):
        return {"dp": 2 * peer + c}

    def al(i, n):
        return pl.multiple_of(i, n)

    in_up = net.load(up_hbm.at[0], ups.at[pl.ds(0, length)])
    in_weight = net.load(weight_hbm, weight.at[pl.ds(al(d * rows, rows), rows)])
    in_value = net.load(value_hbm.at[0], value)
    in_gate = net.load(gate_hbm.at[0], gate)
    in_taps = net.load(taps_hbm, taps.at[s])
    in_gain = net.load(gain_hbm, gain)

    barrier = pltpu.get_barrier_semaphore()
    peers = [to_x, to_y, to_d, partner] + [at_chip(lax.rem(z + k, nz)) for k in range(1, nz)]
    for peer in peers:
        pl.semaphore_signal(barrier, inc=1, device_id=peer, device_id_type=pl.DeviceIdType.MESH)
    pl.semaphore_wait(barrier, len(peers))

    def piece(owner, q, h):
        r = rows // 2
        return weight.at[
            pl.ds(al(owner * rows + h * r, r), r), pl.ds(al(q * quarter, quarter), quarter)
        ]

    hops = [(i, h) for i in range(nz - 1) for h in range(2)]
    in_weight.wait()
    w_slots = net.ids(2 * nz)
    for i, h in hops:
        peer = nearest(z, nz, i)
        net.put(piece(d, s, h), piece(d, s, h), at_chip(peer), w_slots + 2 * z + h)
    in_up.wait()
    own_rows = weight.at[pl.ds(al(d * rows, rows), rows)]
    own_weight = net.put(own_rows, own_rows, partner)
    own_up = net.put(ups.at[pl.ds(0, length)], ups.at[pl.ds(length, length)], partner)
    in_taps.wait()
    tap_copies = [net.put(taps.at[s], taps.at[s], to) for to in (to_x, to_y, to_d)]

    arrived = {}
    mates = {}

    def first(i, h):
        src = nearest(z, nz, i)
        owner = 2 * src + c
        net.arrival(piece(owner, s, h), w_slots + 2 * src + h, partner)
        p = piece(owner, s, h)
        arrived[i, h] = [net.put(p, p, to_x), net.put(p, p, to_y)]
        mates.setdefault(i, []).append(net.put(p, p, partner))

    def second(i, h):
        owner = 2 * nearest(z, nz, i) + c
        from_x, from_y = arrived[i, h]
        px, py = piece(owner, xn, h), piece(owner, yn, h)
        if h == 0:
            from_x.wait_recv()
            arrived[i, h] = net.put(px, px, to_y)
            from_y.wait_recv()
        else:
            from_y.wait_recv()
            arrived[i, h] = net.put(py, py, to_x)
            from_x.wait_recv()
        mates[i] += [net.put(px, px, partner), net.put(py, py, partner)]

    def third(i, h):
        owner = 2 * nearest(z, nz, i) + c
        arrived[i, h].wait_recv()
        p = piece(owner, dg, h)
        mates[i].append(net.put(p, p, partner))

    weight_steps = []
    for n in range(len(hops) + 2):
        if n < len(hops):
            weight_steps.append(functools.partial(first, *hops[n]))
        if 1 <= n <= len(hops):
            weight_steps.append(functools.partial(second, *hops[n - 1]))
        if n >= 2:
            weight_steps.append(functools.partial(third, *hops[n - 2]))

    def gather_weight(count):
        for _ in range(min(count, len(weight_steps))):
            weight_steps.pop(0)()

    in_value.wait()
    in_gate.wait()
    v = value[length - halo :, :].astype(f32)
    tail[...] = (v * jax.nn.sigmoid(gate[length - halo :, :].astype(f32))).astype(bf16)

    def glu_rows(i, _):
        r = al(i * 16, 16)
        v = value[pl.ds(r, 16), :].astype(f32)
        g = (v * jax.nn.sigmoid(gate[pl.ds(r, 16), :].astype(f32))).astype(bf16)
        padded[pl.ds(al(r + halo, 8), 16), :] = g.astype(f32)
        return 0

    lax.fori_loop(0, 2, glu_rows, 0)
    left = net.put(tail, before, {"sp": lax.rem(s + 1, nsp)})
    lax.fori_loop(2, length // 16, glu_rows, 0)
    gather_weight(1)
    for copy in tap_copies:
        copy.wait_recv()
    left.wait_recv()
    b = before[...].astype(f32)
    padded[pl.ds(0, halo), :] = jnp.where(s == 0, jnp.zeros_like(b), b)

    per_block = width // LANES

    def tap(t, j):
        q, lane = t // per_block, lax.rem(t, per_block)
        return taps[q, pl.ds(j, 1), pl.ds(al(lane * LANES, LANES), LANES)]

    def turned(window, r):
        return window if r == 0 else pltpu.roll(window, window.shape[0] - r, 0)

    def conv_tile(t, _):
        cols = pl.ds(al(t * LANES, LANES), LANES)

        def block(i, _):
            r0 = al(i * BLOCK, BLOCK)
            window = padded[pl.ds(r0, BLOCK + halo), cols]
            total = jnp.zeros((BLOCK, LANES), f32)
            for r in range(8):
                moved = turned(window, r)
                for o in range(r, halo + 1, 8):
                    j = o - (halo - tap_count + 1)
                    if 0 <= j < tap_count:
                        total = total + tap(t, j) * moved[o - r : o - r + BLOCK]
            conv[pl.ds(r0, BLOCK), cols] = total.astype(bf16).astype(f32)
            return 0

        return lax.fori_loop(0, length // BLOCK, block, 0)

    part = tiles // 4
    for n in range(4):
        lax.fori_loop(n * part, (n + 1) * part, conv_tile, 0)
        gather_weight(1)

    in_gain.wait()

    def norm_rows(i, _):
        r = al(i * 16, 16)
        rr = pl.ds(r, 16)
        x = conv[rr, :]
        mean = jnp.mean(x, axis=-1, keepdims=True)
        x = x - mean
        inv = lax.rsqrt(jnp.mean(x * x, axis=-1, keepdims=True) + NORM_EPS)
        normed = x * inv
        conv[rr, :] = normed
        scale[rr, :] = jnp.broadcast_to(inv, (16, LANES))
        scaled = normed * gain[...]
        act[rr, :] = (scaled * jax.nn.sigmoid(scaled)).astype(bf16)
        return 0

    blocks = length // 16
    lax.fori_loop(0, blocks // 2, norm_rows, 0)
    gather_weight(1)
    lax.fori_loop(blocks // 2, blocks, norm_rows, 0)

    mine = pl.ds(al(c * half, half), half)
    other = pl.ds(al((1 - c) * half, half), half)
    act_copy = net.put(act.at[:, other], acts.at[pl.ds(length, length)], partner)
    acts[pl.ds(0, length), :] = act[:, mine]
    gather_weight(2)
    own_up.wait_recv()
    act_copy.wait_recv()

    def target(k):
        return nearest(z, nz, nz - 2 - k) if k < nz - 1 else z

    phase_one, phase_two = {}, {}

    def unit(ref, q, h):
        return ref.at[pl.ds(al(q * share, share), share), pl.ds(h * side, side)]

    def multiply(k):
        t = target(k)
        step = min(256, 2 * rows)

        def some(m, _):
            u = ups[:, pl.ds(al(t * 2 * rows + m * step, step), step)]
            p = lax.dot_general(u, acts[...], (((0,), (0,)), ((), ())), preferred_element_type=f32)
            parts[k, pl.ds(al(m * step, step), step), :] = p.astype(bf16)
            return 0

        lax.fori_loop(0, 2 * rows // step, some, 0)

    def scatter_one(k):
        p = parts.at[k]
        phase_one[k] = [
            net.put(unit(p, dg, 0), got_x.at[k, 1], to_x),
            net.put(unit(p, dg, 1), got_y.at[k, 1], to_y),
            net.put(unit(p, xn, 0), got_x.at[k, 0], to_x),
            net.put(unit(p, yn, 1), got_y.at[k, 0], to_y),
        ]

    def own(k, q, h):
        return parts[k, pl.ds(al(q * share, share), share), pl.ds(h * side, side)].astype(f32)

    def scatter_two(k):
        diag_x, diag_y, mine_x, mine_y = phase_one[k]
        diag_x.wait_recv()
        give_y[k] = (own(k, yn, 0) + got_x[k, 1].astype(f32)).astype(bf16)
        diag_y.wait_recv()
        give_x[k] = (own(k, xn, 1) + got_y[k, 1].astype(f32)).astype(bf16)
        phase_two[k] = [
            net.put(give_y.at[k], got_xy.at[k], to_y),
            net.put(give_x.at[k], got_yx.at[k], to_x),
        ]
        mine_x.wait_recv()
        mine_y.wait_recv()

    z_slots = net.ids(nz)

    def scatter_three(k):
        for copy in phase_two[k]:
            copy.wait_recv()
        low = own(k, s, 0) + got_x[k, 0].astype(f32) + got_xy[k].astype(f32)
        high = own(k, s, 1) + got_y[k, 0].astype(f32) + got_yx[k].astype(f32)
        plane[k, :, pl.ds(0, side)] = low.astype(bf16)
        plane[k, :, pl.ds(side, side)] = high.astype(bf16)
        if k < nz - 1:
            net.put(plane.at[k], got_z.at[z], at_chip(target(k)), z_slots + z)

    multiply(0)
    gather_weight(2)
    scatter_one(0)
    multiply(1)
    gather_weight(2)

    def product(owner, start):
        w = weight[pl.ds(al(owner * rows, rows), rows), :]
        u = ups[pl.ds(0, length), pl.ds(al(owner * rows, rows), rows)]
        p = jnp.dot(u, w, preferred_element_type=f32)
        grad_act[...] = p if start else grad_act[...] + p

    product(d, True)
    own_weight.wait_recv()

    def blocks_of(src):
        def one(i, _):
            product(2 * src + i, False)
            return 0

        lax.fori_loop(0, 2, one, 0)

    product(d + 1 - 2 * c, False)
    gather_weight(2)
    scatter_one(1)
    multiply(2)
    gather_weight(2)
    for i in range(nz - 1):
        gather_weight(2 if i < nz - 2 else len(weight_steps))
        if i == nz - 2:
            scatter_one(2)
            multiply(3)
        for copy in mates[i]:
            copy.wait_recv()
        blocks_of(nearest(z, nz, i))
    for k in range(3, nz):
        if k > 3:
            multiply(k)
        scatter_one(k)

    gain_sum[...] = jnp.zeros_like(gain_sum)

    def back_rows(i, _):
        r = al(i * 16, 16)
        rr = pl.ds(r, 16)
        normed = conv[rr, :]
        scaled = normed * gain[...]
        sig = jax.nn.sigmoid(scaled)
        gs = grad_act[rr, :] * sig * (1.0 + scaled * (1.0 - sig))
        gn = gs * normed
        gain_sum[...] += gn[:8] + gn[8:]
        g = gs * gain[...]
        m1 = jnp.mean(g, axis=-1, keepdims=True)
        m2 = jnp.mean(g * normed, axis=-1, keepdims=True)
        gc = (scale[rr, 0:1] * (g - m1 - normed * m2)).astype(bf16)
        grads[rr, :] = gc.astype(f32)
        return 0

    lax.fori_loop(0, halo // 16, back_rows, 0)
    head[...] = grads[pl.ds(0, halo), :].astype(bf16)
    scatter_two(0)
    right = net.put(head, after, {"sp": lax.rem(s + nsp - 1, nsp)})
    lax.fori_loop(halo // 16, blocks // 2, back_rows, 0)
    scatter_three(0)
    lax.fori_loop(blocks // 2, blocks, back_rows, 0)
    scatter_two(1)
    right.wait_recv()
    a = after[...].astype(f32)
    grads[pl.ds(length, halo), :] = jnp.where(s == nsp - 1, jnp.zeros_like(a), a)

    tap_sums[...] = jnp.zeros_like(tap_sums)

    def back_tile(t, _):
        cols = pl.ds(al(t * LANES, LANES), LANES)

        def block(i, _):
            r0 = al(i * BLOCK, BLOCK)
            rr = pl.ds(r0, BLOCK)
            window = grads[pl.ds(r0, BLOCK + halo), cols]
            total = jnp.zeros((BLOCK, LANES), f32)
            for r in range(8):
                moved = turned(window, r)
                for o in range(r, tap_count, 8):
                    total = total + tap(t, tap_count - 1 - o) * moved[o - r : o - r + BLOCK]
            gg = total.astype(bf16).astype(f32)
            sg = jax.nn.sigmoid(gate[rr, cols].astype(f32))
            grad_value[rr, cols] = (gg * sg).astype(bf16)
            grad_gate[rr, cols] = (gg * value[rr, cols].astype(f32) * sg * (1.0 - sg)).astype(bf16)
            gc = window[:BLOCK]
            window = padded[pl.ds(r0, BLOCK + halo), cols]
            for r in range(8):
                moved = turned(window, r)
                for o in range(r, halo + 1, 8):
                    j = o - (halo - tap_count + 1)
                    if 0 <= j < tap_count:
                        term = (gc * moved[o - r : o - r + BLOCK]).reshape(BLOCK // 8, 8, LANES)
                        tap_sums[j, :, cols] += jnp.sum(term, axis=0)
            return 0

        lax.fori_loop(0, length // BLOCK, block, 0)
        q, lane = t // per_block, lax.rem(t, per_block)
        lanes = pl.ds(al(lane * LANES, LANES), LANES)
        terms[q, pl.ds(0, tap_count), lanes] = jnp.sum(tap_sums[:, :, cols], axis=1)
        return 0

    order = []
    for k in range(nz):
        if k >= 1:
            order.append(functools.partial(scatter_three, k))
        if k + 2 <= nz - 1:
            order.append(functools.partial(scatter_two, k + 2))
    pieces = 8
    part = tiles // pieces
    for n in range(pieces):
        lax.fori_loop(n * part, (n + 1) * part, back_tile, 0)
        if n >= 2 and order:
            order.pop(0)()
    for q in range(nsp):
        total = jnp.sum(gain_sum[:, pl.ds(q * width, width)], axis=0, keepdims=True)
        terms[q, pl.ds(tap_count, 1), :] = total
    scattered = [
        net.put(terms.at[peer], got_terms.at[s], to)
        for peer, to in ((dg, to_d), (xn, to_x), (yn, to_y))
    ]
    while order:
        order.pop(0)()
    got_terms[s] = terms[s]
    for copy in scattered:
        copy.wait_recv()
    total = got_terms[0]
    for q in range(1, nsp):
        total = total + got_terms[q]
    row_part[...] = total
    got_dp[z] = total
    tap_slots = net.ids(nz)
    for i in range(nz - 1):
        net.put(row_part, got_dp.at[z], at_chip(nearest(z, nz, i)), tap_slots + z)

    for i in range(nz - 1):
        src = nearest(z, nz, i)
        net.arrival(got_z.at[src], z_slots + src, partner)
    total = plane[nz - 1].astype(f32)
    for i in range(nz - 1):
        total = total + got_z[nearest(z, nz, i)].astype(f32)
    final[pl.ds(al(s * share, share), share), :] = total.astype(bf16)

    def done(q, h):
        return unit(final, q, h)

    sent = {
        (axis, h): net.put(done(s, h), done(s, h), to_x if axis == "x" else to_y)
        for axis, h in (("x", 0), ("y", 1), ("y", 0), ("x", 1))
    }
    for i in range(nz - 1):
        src = nearest(z, nz, i)
        net.arrival(got_dp.at[src], tap_slots + src, partner)
    total = got_dp[0]
    for i in range(1, nz):
        total = total + got_dp[i]
    both_parts[...] = total
    tap_pair = net.put(both_parts, tap_other, partner)
    sent["x", 0].wait_recv()
    low = net.put(done(xn, 0), done(xn, 0), to_y)
    sent["y", 1].wait_recv()
    high = net.put(done(yn, 1), done(yn, 1), to_x)
    tap_pair.wait_recv()
    total = both_parts[...] + tap_other[...]
    grad_taps[...] = total[:tap_count]
    gain_rows[s] = total[total.shape[0] - 8 :]
    gains = [net.put(gain_rows.at[s], gain_rows.at[s], to) for to in (to_d, to_x, to_y)]
    sent["y", 0].wait_recv()
    sent["x", 1].wait_recv()
    low.wait_recv()
    high.wait_recv()
    mine_rows = pl.ds(al(c * rows, rows), rows)
    other_rows = pl.ds(al((1 - c) * rows, rows), rows)
    last = net.put(final.at[other_rows], halves, partner)
    grad_weight[:, mine] = final[mine_rows, :].astype(f32)
    for copy in gains:
        copy.wait_recv()
    for q in range(nsp):
        grad_gain[:, pl.ds(q * width, width)] = gain_rows[q][at_row : at_row + 1]
    last.wait_recv()
    grad_weight[:, other] = halves[...].astype(f32)
    net.finish()


def fused_body(value_half, gate_half, upstream, conv_taps, norm_gain, out_weight):
    f32, bf16 = jnp.float32, jnp.bfloat16
    nsp, ndp = lax.axis_size("sp"), lax.axis_size("dp")
    nz = ndp // 2
    _, length, channels = value_half.shape
    rows = out_weight.shape[0]
    tap_count, width = conv_taps.shape
    halo = (tap_count - 1 + 15) // 16 * 16
    half, side, share = channels // 2, channels // 4, 2 * rows // nsp
    tap_rows = (tap_count + 8) // 8 * 8

    def shape(*dims, dtype=bf16):
        return jax.ShapeDtypeStruct(dims, dtype)

    def vmem(*dims, dtype=bf16):
        return pltpu.VMEM(dims, dtype)

    any_space = pl.BlockSpec(memory_space=pl.ANY)
    remote = 60 + 30 * nz
    grad_value, grad_gate, grad_taps, grad_gain, grad_weight = pl.pallas_call(
        fused,
        out_shape=[
            shape(length, channels),
            shape(length, channels),
            shape(tap_count, width, dtype=f32),
            shape(1, channels, dtype=f32),
            shape(rows, channels, dtype=f32),
        ],
        in_specs=[any_space] * 6,
        out_specs=[VMEM] * 5,
        scratch_shapes=[
            vmem(length, channels),
            vmem(length, channels),
            vmem(2 * length, channels),
            vmem(nsp, tap_count, width, dtype=f32),
            vmem(1, channels, dtype=f32),
            vmem(ndp * rows, channels),
            vmem(halo, channels),
            vmem(halo, channels),
            vmem(length + halo, channels, dtype=f32),
            vmem(length, channels, dtype=f32),
            vmem(length, LANES, dtype=f32),
            vmem(2 * length, half),
            vmem(length, channels),
            vmem(nz, 2 * rows, half),
            vmem(nz, 2, share, side),
            vmem(nz, 2, share, side),
            vmem(nz, share, side),
            vmem(nz, share, side),
            vmem(nz, share, half),
            vmem(nz, share, half),
            vmem(2 * rows, half),
            vmem(rows, half),
            vmem(nz, share, side),
            vmem(nz, share, side),
            vmem(length, channels, dtype=f32),
            vmem(halo, channels),
            vmem(halo, channels),
            vmem(length + halo, channels, dtype=f32),
            vmem(tap_count, 8, channels, dtype=f32),
            vmem(8, channels, dtype=f32),
            vmem(nsp, tap_rows, width, dtype=f32),
            vmem(nsp, tap_rows, width, dtype=f32),
            vmem(nz, tap_rows, width, dtype=f32),
            vmem(tap_rows, width, dtype=f32),
            vmem(tap_rows, width, dtype=f32),
            vmem(tap_rows, width, dtype=f32),
            vmem(nsp, 8, width, dtype=f32),
            pltpu.SemaphoreType.DMA((remote,)),
            pltpu.SemaphoreType.DMA((remote,)),
            pltpu.SemaphoreType.DMA((8,)),
        ],
        compiler_params=pltpu.CompilerParams(
            collective_id=7, has_side_effects=True, vmem_limit_bytes=60 * 1024 * 1024
        ),
    )(value_half, gate_half, upstream, conv_taps, norm_gain[None], out_weight)
    return (grad_value[None], grad_gate[None], grad_taps, grad_gain[0], grad_weight)


def solution(mesh):
    tokens = P("dp", "sp", None)
    quarters = mesh.shape["sp"] == 4 and mesh.shape["dp"] >= 4
    return jax.shard_map(
        fused_body if quarters else body,
        mesh=mesh,
        in_specs=(tokens, tokens, tokens, P(None, "sp"), P(), P("dp", None)),
        out_specs=(tokens, tokens, P(None, "sp"), P(), P("dp", None)),
        check_vma=False,
    )
```

```python
import functools

import jax
import jax.numpy as jnp
from jax import lax
from jax.experimental import pallas as pl
from jax.experimental.pallas import tpu as pltpu
from jax.sharding import PartitionSpec as P

NORM_EPS = 1e-05
VMEM = pl.BlockSpec(memory_space=pltpu.VMEM)


def when(condition, act):
    if condition is None:
        act()
    else:
        pl.when(condition)(lambda: act())


class Copies:
    def __init__(self, send, recv, local):
        self.send, self.recv, self.local = send, recv, local
        self.n_remote = self.n_local = 0
        self.remote, self.locals = [], []

    def start(self, src, dst, target, sends=None, receives=None):
        i = self.n_remote
        self.n_remote += 1
        copy = pltpu.make_async_remote_copy(
            src_ref=src,
            dst_ref=dst,
            send_sem=self.send.at[i],
            recv_sem=self.recv.at[i],
            device_id=target,
            device_id_type=pl.DeviceIdType.MESH,
        )
        when(sends, copy.start)
        self.remote.append([copy, False, sends, receives])
        return len(self.remote) - 1

    def keep(self, src, dst):
        copy = pltpu.make_async_copy(src, dst, self.local.at[self.n_local])
        self.n_local += 1
        copy.start()
        self.locals.append(copy)

    def arrive(self, i):
        when(self.remote[i][3], self.remote[i][0].wait_recv)
        self.remote[i][1] = True

    def finish(self):
        for copy, arrived, sends, receives in self.remote:
            if not arrived:
                when(receives, copy.wait_recv)
            when(sends, copy.wait_send)
        for copy in self.locals:
            copy.wait()


def greet(axes):
    barrier = pltpu.get_barrier_semaphore()
    count = 0
    for axis in axes:
        n = lax.axis_size(axis)
        me = lax.axis_index(axis)
        for k in range(1, n):
            pl.semaphore_signal(
                barrier,
                inc=1,
                device_id={axis: lax.rem(me + k, n)},
                device_id_type=pl.DeviceIdType.MESH,
            )
            count += 1
    pl.semaphore_wait(barrier, count)


def direct(copies, kind, axis, src, dst):
    n = lax.axis_size(axis)
    me = lax.axis_index(axis)
    if kind == "next" or kind == "prev":
        copies.start(src, dst, {axis: lax.rem(me + (1 if kind == "next" else n - 1), n)})
        return
    if kind == "pair":
        copies.start(src, dst, {axis: me + 1 - 2 * lax.rem(me, 2)})
        return
    if kind == "rows":
        nz, z, c = n // 2, me // 2, lax.rem(me, 2)
        copies.keep(src.at[z], dst.at[z])
        for k in range(1, nz):
            peer = lax.rem(z + k, nz)
            copies.start(src.at[peer], dst.at[z], {axis: 2 * peer + c})
        return
    copies.keep(src.at[me] if kind == "scatter" else src, dst.at[me])
    for k in range(1, n):
        peer = lax.rem(me + k, n)
        copies.start(src.at[peer] if kind == "scatter" else src, dst.at[me], {axis: peer})


def spread_gather(copies, src, dst):
    ns, nz = lax.axis_size("sp"), lax.axis_size("dp") // 2
    s, d = lax.axis_index("sp"), lax.axis_index("dp")
    z, c = d // 2, lax.rem(d, 2)
    partner = {"dp": d + 1 - 2 * c}
    first = [
        copies.start(src.at[s], dst.at[d, s], {"dp": 2 * lax.rem(z + k, nz) + c})
        for k in range(1, nz)
    ]
    yield
    copies.keep(src, dst.at[d])
    copies.start(src, dst.at[d], partner)
    second = {}
    for k in range(1, nz):
        copies.arrive(first[k - 1])
        piece = dst.at[2 * lax.rem(z + nz - k, nz) + c, s]
        for j in range(1, ns):
            second[k, j] = copies.start(piece, piece, {"sp": lax.rem(s + j, ns)})
        copies.start(piece, piece, partner)
    yield
    for k in range(1, nz):
        for j in range(1, ns):
            copies.arrive(second[k, j])
            piece = dst.at[2 * lax.rem(z + nz - k, nz) + c, lax.rem(s + ns - j, ns)]
            copies.start(piece, piece, partner)


def line_gather(copies, src, dst):
    nz = lax.axis_size("dp") // 2
    d = lax.axis_index("dp")
    z, c = d // 2, lax.rem(d, 2)
    partner = {"dp": d + 1 - 2 * c}
    up = {"dp": 2 * lax.rem(z + 1, nz) + c}
    down = {"dp": 2 * lax.rem(z + nz - 1, nz) + c}
    below, above = {}, {}

    def send(k):
        low, high = 2 * lax.rem(z + nz - k, nz) + c, 2 * lax.rem(z + k, nz) + c
        low_src, high_src = (dst.at[low], dst.at[high]) if k else (src, src)
        below[k] = copies.start(
            low_src, dst.at[low], up, jnp.logical_and(z >= k, z < nz - 1), z >= k + 1
        )
        above[k] = copies.start(
            high_src, dst.at[high], down, jnp.logical_and(z + k < nz, z > 0), z + k + 1 < nz
        )

    send(0)
    yield
    copies.keep(src, dst.at[d])
    copies.start(src, dst.at[d], partner)
    for k in range(1, nz):
        copies.arrive(below[k - 1])
        copies.arrive(above[k - 1])
        if k < nz - 1:
            send(k)
        low, high = dst.at[2 * lax.rem(z + nz - k, nz) + c], dst.at[2 * lax.rem(z + k, nz) + c]
        copies.start(low, low, partner, z >= k, z >= k)
        copies.start(high, high, partner, z + k < nz, z + k < nz)
        yield


def run(axes, items, *refs):
    n = len(items)
    copies = Copies(*refs[2 * n :])
    greet(axes)
    waiting = []
    for i, (kind, axis) in enumerate(items):
        src, dst = refs[i], refs[n + i]
        if kind == "spread":
            waiting.append(spread_gather(copies, src, dst))
        elif kind == "line":
            waiting.append(line_gather(copies, src, dst))
        elif kind == "later":
            waiting.append(later(copies, axis, src, dst))
        else:
            direct(copies, kind, axis, src, dst)
    while waiting:
        waiting = [steps for steps in waiting if next(steps, waiting) is None]
    copies.finish()


def later(copies, axis, src, dst):
    yield
    direct(copies, "scatter", axis, src, dst)


def exchange(collective_id, *items):
    ns, nd = lax.axis_size("sp"), lax.axis_size("dp")
    shapes, remote, local = [], 0, 0
    for kind, axis, x in items:
        n = lax.axis_size(axis)
        if kind == "rows":
            shape = x.shape
            remote += n // 2 - 1
            local += 1
        elif kind in ("next", "prev", "pair"):
            shape = x.shape
            remote += 1
        elif kind in ("scatter", "later"):
            shape = x.shape
            remote += n - 1
            local += 1
        else:
            shape = (n,) + x.shape
            local += 1
            if kind == "gather":
                remote += n - 1
            elif kind == "spread":
                remote += (nd // 2 - 1) * 2 * ns + 1
            else:
                remote += (nd // 2 - 1) * 4 + 1
        shapes.append(jax.ShapeDtypeStruct(shape, x.dtype))
    axes = tuple(a for a in ("sp", "dp") if any(axis == a or kind == "spread" for kind, axis, _ in items))
    return pl.pallas_call(
        functools.partial(run, axes, tuple((kind, axis) for kind, axis, _ in items)),
        out_shape=shapes,
        in_specs=[VMEM] * len(items),
        out_specs=[VMEM] * len(items),
        scratch_shapes=[
            pltpu.SemaphoreType.DMA((remote,)),
            pltpu.SemaphoreType.DMA((remote,)),
            pltpu.SemaphoreType.DMA((max(local, 1),)),
        ],
        compiler_params=pltpu.CompilerParams(
            collective_id=collective_id, has_side_effects=True, vmem_limit_bytes=48 * 1024 * 1024
        ),
    )(*[x for _, _, x in items])


def body(value_half, gate_half, upstream, conv_taps, norm_gain, out_weight):
    f32 = jnp.float32
    tap_count = conv_taps.shape[0]
    halo = tap_count - 1
    nsp, ndp = lax.axis_size("sp"), lax.axis_size("dp")
    at_start = lax.axis_index("sp") == 0
    at_end = lax.axis_index("sp") == nsp - 1
    edge = (halo + 15) // 16 * 16

    value = value_half[0].astype(f32)
    gate = gate_half[0].astype(f32)
    length = value.shape[0]
    channels = value.shape[1]
    up = upstream[0]
    rows = out_weight.shape[0]

    tail = (value[length - edge :] * jax.nn.sigmoid(gate[length - edge :])).astype(jnp.bfloat16)
    up_blocks = jnp.swapaxes(up.reshape(length, ndp, rows), 0, 1)
    before, taps = exchange(1, ("next", "sp", tail), ("gather", "sp", conv_taps))
    before = jnp.where(at_start, 0, before)[edge - halo :]
    taps = jnp.swapaxes(taps, 0, 1).reshape(tap_count, channels)
    sig_gate = jax.nn.sigmoid(gate)
    glu = (value * sig_gate).astype(jnp.bfloat16)
    padded = jnp.concatenate([before, glu], axis=0).astype(f32)
    conv = jnp.zeros((length, padded.shape[1]), f32)
    for j in range(tap_count):
        conv = conv + taps[j] * padded[j : j + length]
    conv = conv.astype(jnp.bfloat16).astype(f32)
    mean = jnp.mean(conv, axis=-1, keepdims=True)
    centered = conv - mean
    inv = lax.rsqrt(jnp.mean(centered * centered, axis=-1, keepdims=True) + NORM_EPS)
    normed = centered * inv
    scaled = normed * norm_gain
    sig = jax.nn.sigmoid(scaled)
    activated = (scaled * sig).astype(jnp.bfloat16)

    half = channels // 2
    nz, piece = ndp // 2, rows // nsp
    core = lax.rem(lax.axis_index("dp"), 2)
    by_core = up.reshape(length, nz, 2, nsp, piece)

    def partial(which):
        columns = lax.dynamic_index_in_dim(by_core, which, 2, keepdims=False)
        columns = jnp.swapaxes(columns, 1, 2).reshape(length, nsp * nz * piece)
        return lax.dot_general(
            columns, activated[:, half:], (((0,), (0,)), ((), ())), preferred_element_type=f32
        )

    weight, act_all, up_columns, from_partner = exchange(
        2,
        ("spread", "dp", out_weight.reshape(nsp, rows // nsp, channels)),
        ("line", "dp", activated[:, :half]),
        ("later", "dp", up_blocks),
        ("pair", "dp", partial(1 - core).astype(jnp.bfloat16)),
    )
    weight = weight.reshape(ndp * rows, channels)
    act_all = act_all.reshape(ndp * length, half)
    up_columns = up_columns.reshape(ndp * length, rows)
    owned = lax.dot_general(
        up_columns, act_all, (((0,), (0,)), ((), ())), preferred_element_type=f32
    )
    summed = (partial(core) + from_partner.astype(f32)).astype(jnp.bfloat16)
    summed = summed.reshape(nsp, nz, piece, half)

    grad_act = jnp.dot(up, weight, preferred_element_type=f32)
    grad_scaled = grad_act * sig * (1.0 + scaled * (1.0 - sig))
    gain_part = jnp.sum(grad_scaled * normed, axis=0)
    g = grad_scaled * norm_gain
    grad_conv = inv * (
        g
        - jnp.mean(g, axis=-1, keepdims=True)
        - normed * jnp.mean(g * normed, axis=-1, keepdims=True)
    )
    grad_conv = grad_conv.astype(jnp.bfloat16)
    after, gain_got, owned_got, summed_got = exchange(
        3,
        ("prev", "sp", grad_conv[:edge]),
        ("gather", "sp", gain_part[None]),
        ("scatter", "sp", owned.astype(jnp.bfloat16).reshape(nsp, piece, half)),
        ("scatter", "sp", summed),
    )
    after = jnp.where(at_end, 0, after)[:halo]
    extended = jnp.concatenate([grad_conv, after], axis=0).astype(f32)
    here = grad_conv.astype(f32)
    grad_glu = jnp.zeros_like(here)
    terms = []
    for j in range(tap_count):
        first = halo - j
        grad_glu = grad_glu + taps[j] * extended[first : first + length]
        terms.append(jnp.sum(here * padded[j : j + length], axis=0))
    grad_glu = grad_glu.astype(jnp.bfloat16).astype(f32)
    grad_value = (grad_glu * sig_gate).astype(jnp.bfloat16)
    grad_gate = (grad_glu * value * sig_gate * (1.0 - sig_gate)).astype(jnp.bfloat16)

    width = conv_taps.shape[1]
    tap_blocks = jnp.swapaxes(jnp.stack(terms).reshape(tap_count, nsp, width), 0, 1)
    gain_got, tap_got, low_weight, high_got = exchange(
        4,
        ("gather", "dp", jnp.sum(gain_got, axis=0)),
        ("scatter", "sp", tap_blocks),
        ("gather", "sp", jnp.sum(owned_got.astype(f32), axis=0).astype(jnp.bfloat16)),
        ("rows", "dp", jnp.sum(summed_got.astype(f32), axis=0).astype(jnp.bfloat16)),
    )
    tap_got, high_weight = exchange(
        5,
        ("gather", "dp", jnp.sum(tap_got, axis=0)),
        ("gather", "sp", jnp.sum(high_got.astype(f32), axis=0).astype(jnp.bfloat16)),
    )
    grad_gain = jnp.sum(gain_got, axis=0)[0]
    grad_taps = jnp.sum(tap_got, axis=0)
    grad_weight = jnp.concatenate(
        [low_weight.reshape(rows, half), high_weight.reshape(rows, half)], axis=1
    ).astype(f32)
    return (grad_value[None], grad_gate[None], grad_taps, grad_gain, grad_weight)


BLOCK = 64
LANES = 128


class Net:
    def __init__(self, send, recv, local):
        self.send, self.recv, self.local = send, recv, local
        self.n = self.m = 0
        self.open = []
        self.landing = []

    def ids(self, count):
        self.n += count
        return self.n - count

    def put(self, src, dst, to, slot=None, sends=None):
        i = self.ids(1)
        copy = pltpu.make_async_remote_copy(
            src_ref=src,
            dst_ref=dst,
            send_sem=self.send.at[i],
            recv_sem=self.recv.at[i if slot is None else slot],
            device_id=to,
            device_id_type=pl.DeviceIdType.MESH,
        )
        when(sends, copy.start)
        self.open.append((copy, sends))
        return copy

    def arrival(self, ref, slot, to):
        pltpu.make_async_remote_copy(
            src_ref=ref,
            dst_ref=ref,
            send_sem=self.send.at[0],
            recv_sem=self.recv.at[slot],
            device_id=to,
            device_id_type=pl.DeviceIdType.MESH,
        ).wait_recv()

    def load(self, src, dst):
        copy = pltpu.make_async_copy(src, dst, self.local.at[self.m])
        self.m += 1
        copy.start()
        return copy

    def finish(self):
        for copy, sends in self.open:
            when(sends, copy.wait_send)


def nearest(z, nz, i):
    low, high = z, nz - 1 - z
    both = 2 * jnp.minimum(low, high)
    away = jnp.where(i < both, i // 2 + 1, i - both // 2 + 1)
    up = jnp.where(i < both, i % 2 == 0, high > low)
    return jnp.where(up, z + away, z - away)


def fused(
    value_hbm, gate_hbm, up_hbm, taps_hbm, gain_hbm, weight_hbm,
    grad_value, grad_gate, grad_taps, grad_gain, grad_weight,
    value, gate, ups, taps, gain, weight, tail, before, padded, conv, scale, acts, act,
    parts, got_x, got_y, got_xy, got_yx, plane, got_z, final, halves, give_x, give_y,
    got_e, early, e_x, e_y, e_xy, e_yx, e_give_x, e_give_y,
    grad_act, head, after, grads, tap_sums, gain_sum, terms, got_terms, got_dp, row_part, both_parts,
    tap_other, gain_rows,
    send, recv, local,
):
    f32, bf16 = jnp.float32, jnp.bfloat16
    nsp, ndp = lax.axis_size("sp"), lax.axis_size("dp")
    nz = ndp // 2
    s, d = lax.axis_index("sp"), lax.axis_index("dp")
    z, c = d // 2, lax.rem(d, 2)
    xn, yn = s + 1 - 2 * lax.rem(s, 2), lax.rem(s + 2, nsp)
    dg = nsp - 1 - s
    length, channels = value.shape
    halo = before.shape[0]
    tap_count = taps.shape[1]
    width = taps.shape[2]
    rows = weight.shape[0] // ndp
    half = channels // 2
    lead = got_e.shape[2]
    rest = half - lead
    side, e_side = rest // 2, lead // 2
    quarter = channels // nsp
    share = 2 * rows // nsp
    tiles = channels // LANES
    at_row = tap_count - (terms.shape[1] - 8)
    net = Net(send, recv, local)
    to_x, to_y, to_d, partner = {"sp": xn}, {"sp": yn}, {"sp": dg}, {"dp": d + 1 - 2 * c}

    def at_chip(peer):
        return {"dp": 2 * peer + c}

    def al(i, n):
        return pl.multiple_of(i, n)

    in_up = net.load(up_hbm.at[0], ups.at[pl.ds(0, length)])
    in_weight = net.load(weight_hbm, weight.at[pl.ds(al(d * rows, rows), rows)])
    in_value = net.load(value_hbm.at[0], value)
    in_gate = net.load(gate_hbm.at[0], gate)
    in_taps = net.load(taps_hbm, taps.at[s])
    in_gain = net.load(gain_hbm, gain)

    barrier = pltpu.get_barrier_semaphore()
    peers = [to_x, to_y, to_d, partner] + [at_chip(lax.rem(z + k, nz)) for k in range(1, nz)]
    for peer in peers:
        pl.semaphore_signal(barrier, inc=1, device_id=peer, device_id_type=pl.DeviceIdType.MESH)
    pl.semaphore_wait(barrier, len(peers))

    def piece(owner, q, h):
        r = rows // 2
        return weight.at[
            pl.ds(al(owner * rows + h * r, r), r), pl.ds(al(q * quarter, quarter), quarter)
        ]

    above, below = at_chip(lax.rem(z + 1, nz)), at_chip(lax.rem(z + nz - 1, nz))

    def along(src, h):
        p, slot = piece(2 * src + c, s, h), w_slots + 2 * src + h
        net.put(p, p, above, slot, jnp.logical_and(src <= z, z < nz - 1))
        net.put(p, p, below, slot, jnp.logical_and(src >= z, z > 0))

    in_taps.wait()
    tap_copies = [net.put(taps.at[s], taps.at[s], to) for to in (to_x, to_y, to_d)]
    w_slots = net.ids(2 * nz)
    in_weight.wait()
    for h in range(2):
        along(z, h)

    arrived = {}
    mates = {}

    def first(i, h):
        src = nearest(z, nz, i)
        owner = 2 * src + c
        net.arrival(piece(owner, s, h), w_slots + 2 * src + h, partner)
        along(src, h)
        p = piece(owner, s, h)
        arrived[i, h] = [net.put(p, p, to_x), net.put(p, p, to_y)]
        mates.setdefault(i, []).append(net.put(p, p, partner))

    def second(i, h):
        owner = 2 * nearest(z, nz, i) + c
        from_x, from_y = arrived[i, h]
        px, py = piece(owner, xn, h), piece(owner, yn, h)
        if h == 0:
            from_x.wait_recv()
            arrived[i, h] = net.put(px, px, to_y)
            from_y.wait_recv()
        else:
            from_y.wait_recv()
            arrived[i, h] = net.put(py, py, to_x)
            from_x.wait_recv()
        mates[i] += [net.put(px, px, partner), net.put(py, py, partner)]

    def third(i, h):
        owner = 2 * nearest(z, nz, i) + c
        arrived[i, h].wait_recv()
        p = piece(owner, dg, h)
        mates[i].append(net.put(p, p, partner))

    in_value.wait()
    in_gate.wait()
    v = value[length - halo :, :].astype(f32)
    tail[...] = (v * jax.nn.sigmoid(gate[length - halo :, :].astype(f32))).astype(bf16)

    def glu_rows(i, _):
        r = al(i * 16, 16)
        v = value[pl.ds(r, 16), :].astype(f32)
        g = (v * jax.nn.sigmoid(gate[pl.ds(r, 16), :].astype(f32))).astype(bf16)
        padded[pl.ds(al(r + halo, 8), 16), :] = g.astype(f32)
        return 0

    lax.fori_loop(0, 2, glu_rows, 0)
    left = net.put(tail, before, {"sp": lax.rem(s + 1, nsp)}, None, s < nsp - 1)
    in_up.wait()
    own_rows = weight.at[pl.ds(al(d * rows, rows), rows)]
    own_up = net.put(ups.at[pl.ds(0, length)], ups.at[pl.ds(length, length)], partner)
    own_weight = net.put(own_rows, own_rows, partner)
    lax.fori_loop(2, length // 16, glu_rows, 0)

    def tap_from(n):
        tap_copies[n].wait_recv()

    def left_halo():
        when(s > 0, left.wait_recv)

        @pl.when(s == 0)
        def _():
            before[...] = jnp.zeros_like(before)

        padded[pl.ds(0, halo), :] = before[...].astype(f32)

    per_block = width // LANES

    def tap(t, j):
        q, lane = t // per_block, lax.rem(t, per_block)
        return taps[q, pl.ds(j, 1), pl.ds(al(lane * LANES, LANES), LANES)]

    def turned(window, r):
        return window if r == 0 else pltpu.roll(window, window.shape[0] - r, 0)

    def conv_block(t, i):
        cols = pl.ds(al(t * LANES, LANES), LANES)
        r0 = al(i * BLOCK, BLOCK)
        window = padded[pl.ds(r0, BLOCK + halo), cols]
        total = jnp.zeros((BLOCK, LANES), f32)
        for r in range(8):
            moved = turned(window, r)
            for o in range(r, halo + 1, 8):
                j = o - (halo - tap_count + 1)
                if 0 <= j < tap_count:
                    total = total + tap(t, j) * moved[o - r : o - r + BLOCK]
        conv[pl.ds(r0, BLOCK), cols] = total.astype(bf16).astype(f32)

    row_blocks = length // BLOCK

    def conv_quarter(n):
        q = (s, xn, yn, dg)[n]
        inner = row_blocks - 1

        def one(m, _):
            conv_block(q * per_block + m // inner, 1 + lax.rem(m, inner))
            return 0

        lax.fori_loop(0, per_block * inner, one, 0)

    def conv_head(n):
        def one(t, _):
            conv_block(t, 0)
            return 0

        lax.fori_loop(n * tiles // 2, (n + 1) * tiles // 2, one, 0)

    in_gain.wait()

    def norm_rows(i, _):
        r = al(i * 16, 16)
        rr = pl.ds(r, 16)
        x = conv[rr, :]
        mean = jnp.mean(x, axis=-1, keepdims=True)
        x = x - mean
        inv = lax.rsqrt(jnp.mean(x * x, axis=-1, keepdims=True) + NORM_EPS)
        normed = x * inv
        conv[rr, :] = normed
        scale[rr, :] = jnp.broadcast_to(inv, (16, LANES))
        scaled = normed * gain[...]
        act[rr, :] = (scaled * jax.nn.sigmoid(scaled)).astype(bf16)
        return 0

    blocks = length // 16

    def norm(n):
        lax.fori_loop(n * blocks // 4, (n + 1) * blocks // 4, norm_rows, 0)

    mine = pl.ds(al(c * half, half), half)
    other = pl.ds(al((1 - c) * half, half), half)
    swapped = []

    def swap():
        swapped.append(net.put(act.at[:, other], acts.at[pl.ds(length, length)], partner))
        acts[pl.ds(0, length), :] = act[:, mine]

    def swap_done():
        own_up.wait_recv()
        swapped[0].wait_recv()

    def target(k):
        return nearest(z, nz, nz - 2 - k) if k < nz - 1 else z

    def multiply(k):
        t = target(k)
        step = min(256, 2 * rows)

        def some(m, _):
            u = ups[:, pl.ds(al(t * 2 * rows + m * step, step), step)]
            p = lax.dot_general(u, acts[...], (((0,), (0,)), ((), ())), preferred_element_type=f32)
            parts[k, pl.ds(al(m * step, step), step), :] = p.astype(bf16)
            return 0

        lax.fori_loop(0, 2 * rows // step, some, 0)

    class Plane:
        def __init__(self, src, w, x, y, xy, yx, give_x, give_y):
            self.src, self.w = src, w
            self.x, self.y, self.xy, self.yx = x, y, xy, yx
            self.give_x, self.give_y = give_x, give_y

        def at(self, q, h):
            return pl.ds(al(q * share, share), share), pl.ds(h * self.w, self.w)

        def part(self, q, h):
            return self.src[self.at(q, h)].astype(f32)

        def send(self):
            def unit(q, h):
                return self.src.at[self.at(q, h)]

            self.far_x = net.put(unit(dg, 0), self.x.at[1], to_x)
            self.far_y = net.put(unit(dg, 1), self.y.at[1], to_y)
            self.near_x = net.put(unit(xn, 0), self.x.at[0], to_x)
            self.near_y = net.put(unit(yn, 1), self.y.at[0], to_y)

        def turn_x(self):
            self.far_x.wait_recv()
            self.give_y[...] = (self.part(yn, 0) + self.x[1].astype(f32)).astype(bf16)
            self.last_y = net.put(self.give_y, self.xy, to_y)

        def turn_y(self):
            self.far_y.wait_recv()
            self.give_x[...] = (self.part(xn, 1) + self.y[1].astype(f32)).astype(bf16)
            self.last_x = net.put(self.give_x, self.yx, to_x)

        def total(self):
            for copy in (self.near_x, self.near_y, self.last_x, self.last_y):
                copy.wait_recv()
            low = self.part(s, 0) + self.x[0].astype(f32) + self.xy[...].astype(f32)
            high = self.part(s, 1) + self.y[0].astype(f32) + self.yx[...].astype(f32)
            return low.astype(bf16), high.astype(bf16)

    chunks = [
        Plane(
            parts.at[k], side, got_x.at[k], got_y.at[k], got_xy.at[k], got_yx.at[k],
            give_x.at[k], give_y.at[k],
        )
        for k in range(nz)
    ]
    ahead = Plane(early, e_side, e_x, e_y, e_xy, e_yx, e_give_x, e_give_y)
    z_slots, e_slots = net.ids(nz), net.ids(nz)

    def load(k):
        chunks[k].send()

    def turn_x(k):
        chunks[k].turn_x()

    def turn_y(k):
        chunks[k].turn_y()

    def hand_on(k):
        low, high = chunks[k].total()
        plane[k, :, pl.ds(0, side)] = low
        plane[k, :, pl.ds(side, side)] = high
        if k < nz - 1:
            net.put(plane.at[k], got_z.at[z], at_chip(target(k)), z_slots + z)

    def send_early(k):
        if k < nz - 1:
            tops = parts.at[k, :, pl.ds(rest, lead)]
            net.put(tops, got_e.at[z], at_chip(target(k)), e_slots + z)

    def add_early():
        total = parts[nz - 1, :, pl.ds(rest, lead)].astype(f32)
        for i in range(nz - 1):
            src = nearest(z, nz, i)
            net.arrival(got_e.at[src], e_slots + src, partner)
            total = total + got_e[src].astype(f32)
        early[...] = total.astype(bf16)
        ahead.send()

    def turn_early():
        ahead.turn_x()
        ahead.turn_y()

    def keep_early():
        low, high = ahead.total()
        own = pl.ds(al(s * share, share), share)
        final[own, pl.ds(rest, e_side)] = low
        final[own, pl.ds(rest + e_side, e_side)] = high

    def product(owner, start):
        w = weight[pl.ds(al(owner * rows, rows), rows), :]
        u = ups[pl.ds(0, length), pl.ds(al(owner * rows, rows), rows)]
        p = jnp.dot(u, w, preferred_element_type=f32)
        grad_act[...] = p if start else grad_act[...] + p

    def product_own():
        product(d, True)

    def product_mate():
        own_weight.wait_recv()
        product(d + 1 - 2 * c, False)

    def blocks_of(i):
        assert len(mates[i]) == 8
        for copy in mates[i]:
            copy.wait_recv()
        src = nearest(z, nz, i)

        def one(n, _):
            product(2 * src + n, False)
            return 0

        lax.fori_loop(0, 2, one, 0)

    gain_sum[...] = jnp.zeros_like(gain_sum)

    def back_rows(i, _):
        r = al(i * 16, 16)
        rr = pl.ds(r, 16)
        normed = conv[rr, :]
        scaled = normed * gain[...]
        sig = jax.nn.sigmoid(scaled)
        gs = grad_act[rr, :] * sig * (1.0 + scaled * (1.0 - sig))
        gn = gs * normed
        gain_sum[...] += gn[:8] + gn[8:]
        g = gs * gain[...]
        m1 = jnp.mean(g, axis=-1, keepdims=True)
        m2 = jnp.mean(g * normed, axis=-1, keepdims=True)
        gc = (scale[rr, 0:1] * (g - m1 - normed * m2)).astype(bf16)
        grads[rr, :] = gc.astype(f32)
        return 0

    ready = []

    def back_head():
        lax.fori_loop(0, halo // 16, back_rows, 0)
        head[...] = grads[pl.ds(0, halo), :].astype(bf16)
        ready.append(net.put(head, after, {"sp": lax.rem(s + nsp - 1, nsp)}, None, s > 0))

    def back(n):
        mid = (blocks + halo // 16) // 2
        lax.fori_loop((halo // 16, mid)[n], (mid, blocks)[n], back_rows, 0)

    def right_halo():
        when(s < nsp - 1, ready[0].wait_recv)

        @pl.when(s == nsp - 1)
        def _():
            after[...] = jnp.zeros_like(after)

        grads[pl.ds(length, halo), :] = after[...].astype(f32)

    tap_sums[...] = jnp.zeros_like(tap_sums)

    def back_block(t, i):
        cols = pl.ds(al(t * LANES, LANES), LANES)
        r0 = al(i * BLOCK, BLOCK)
        rr = pl.ds(r0, BLOCK)
        window = grads[pl.ds(r0, BLOCK + halo), cols]
        total = jnp.zeros((BLOCK, LANES), f32)
        for r in range(8):
            moved = turned(window, r)
            for o in range(r, tap_count, 8):
                total = total + tap(t, tap_count - 1 - o) * moved[o - r : o - r + BLOCK]
        gg = total.astype(bf16).astype(f32)
        sg = jax.nn.sigmoid(gate[rr, cols].astype(f32))
        grad_value[rr, cols] = (gg * sg).astype(bf16)
        grad_gate[rr, cols] = (gg * value[rr, cols].astype(f32) * sg * (1.0 - sg)).astype(bf16)
        gc = window[:BLOCK]
        window = padded[pl.ds(r0, BLOCK + halo), cols]
        for r in range(8):
            moved = turned(window, r)
            for o in range(r, halo + 1, 8):
                j = o - (halo - tap_count + 1)
                if 0 <= j < tap_count:
                    term = (gc * moved[o - r : o - r + BLOCK]).reshape(BLOCK // 8, 8, LANES)
                    tap_sums[j, :, cols] += jnp.sum(term, axis=0)

    def back_tiles(n):
        inner = row_blocks - 1

        def one(m, _):
            back_block(m // inner, lax.rem(m, inner))
            return 0

        step = tiles // 8 * inner
        lax.fori_loop(n * step, (n + 1) * step, one, 0)

    def back_tail(n):
        def one(t, _):
            back_block(t, row_blocks - 1)
            cols = pl.ds(al(t * LANES, LANES), LANES)
            q, lane = t // per_block, lax.rem(t, per_block)
            lanes = pl.ds(al(lane * LANES, LANES), LANES)
            terms[q, pl.ds(0, tap_count), lanes] = jnp.sum(tap_sums[:, :, cols], axis=1)
            return 0

        lax.fori_loop(n * tiles // 2, (n + 1) * tiles // 2, one, 0)

    sums = {}

    def send_terms():
        for q in range(nsp):
            total = jnp.sum(gain_sum[:, pl.ds(q * width, width)], axis=0, keepdims=True)
            terms[q, pl.ds(tap_count, 1), :] = total
        sums["sp"] = [
            net.put(terms.at[peer], got_terms.at[s], to)
            for peer, to in ((dg, to_d), (xn, to_x), (yn, to_y))
        ]
        got_terms[s] = terms[s]

    tap_slots = net.ids(nz)

    def add_terms():
        for copy in sums["sp"]:
            copy.wait_recv()
        total = got_terms[0]
        for q in range(1, nsp):
            total = total + got_terms[q]
        row_part[...] = total
        got_dp[z] = total
        for i in range(nz - 1):
            net.put(row_part, got_dp.at[z], at_chip(nearest(z, nz, i)), tap_slots + z)

    def done(q, h):
        return final.at[pl.ds(al(q * share, share), share), pl.ds(h * half // 2, half // 2)]

    sent = {}

    def finish_rows():
        total = plane[nz - 1].astype(f32)
        for i in range(nz - 1):
            src = nearest(z, nz, i)
            net.arrival(got_z.at[src], z_slots + src, partner)
            total = total + got_z[src].astype(f32)
        final[pl.ds(al(s * share, share), share), pl.ds(0, rest)] = total.astype(bf16)
        for axis, h in (("x", 0), ("y", 1), ("y", 0), ("x", 1)):
            sent[axis, h] = net.put(done(s, h), done(s, h), to_x if axis == "x" else to_y)

    def pair_terms():
        for i in range(nz - 1):
            src = nearest(z, nz, i)
            net.arrival(got_dp.at[src], tap_slots + src, partner)
        total = got_dp[0]
        for i in range(1, nz):
            total = total + got_dp[i]
        both_parts[...] = total
        sums["pair"] = net.put(both_parts, tap_other, partner)

    def spread_rows():
        sent.pop(("x", 0)).wait_recv()
        sent["low"] = net.put(done(xn, 0), done(xn, 0), to_y)
        sent.pop(("y", 1)).wait_recv()
        sent["high"] = net.put(done(yn, 1), done(yn, 1), to_x)

    def keep_taps():
        sums["pair"].wait_recv()
        total = both_parts[...] + tap_other[...]
        grad_taps[...] = total[:tap_count]
        gain_rows[s] = total[total.shape[0] - 8 :]
        sums["gain"] = [net.put(gain_rows.at[s], gain_rows.at[s], to) for to in (to_d, to_x, to_y)]

    mine_rows = pl.ds(al(c * rows, rows), rows)
    other_rows = pl.ds(al((1 - c) * rows, rows), rows)

    def gather_rows():
        for copy in sent.values():
            copy.wait_recv()
        sums["last"] = net.put(final.at[other_rows], halves, partner)
        grad_weight[:, mine] = final[mine_rows, :].astype(f32)

    def keep():
        for copy in sums["gain"]:
            copy.wait_recv()
        for q in range(nsp):
            grad_gain[:, pl.ds(q * width, width)] = gain_rows[q][at_row : at_row + 1]
        sums["last"].wait_recv()
        grad_weight[:, other] = halves[...].astype(f32)

    for step, *at in (
        (tap_from, 1),
        (conv_quarter, 0),
        (first, 0, 0),
        (conv_quarter, 2),
        (tap_from, 2),
        (tap_from, 0),
        (conv_quarter, 3),
        (first, 0, 1),
        (first, 1, 0),
        (conv_quarter, 1),
        (first, 1, 1),
        (left_halo,),
        (norm, 2),
        (product_own,),
        (second, 0, 0),
        (conv_head, 1),
        (first, 2, 0),
        (norm, 3),
        (second, 0, 1),
        (conv_head, 0),
        (norm, 0),
        (norm, 1),
        (product_mate,),
        (swap,),
        (first, 2, 1),
        (second, 1, 0),
        (swap_done,),
        (third, 0, 0),
        (multiply, 0),
        (send_early, 0),
        (third, 0, 1),
        (second, 1, 1),
        (second, 2, 0),
        (multiply, 2),
        (multiply, 3),
        (second, 2, 1),
        (multiply, 1),
        (load, 0),
        (send_early, 1),
        (third, 1, 0),
        (load, 1),
        (third, 1, 1),
        (blocks_of, 0),
        (blocks_of, 1),
        (turn_y, 0),
        (third, 2, 0),
        (turn_x, 0),
        (third, 2, 1),
        (blocks_of, 2),
        (send_early, 2),
        (back_head,),
        (back, 0),
        (back, 1),
        (back_tiles, 0),
        (back_tiles, 1),
        (load, 2),
        (hand_on, 0),
        (back_tiles, 2),
        (right_halo,),
        (send_early, 3),
        (back_tiles, 3),
        (turn_y, 1),
        (turn_x, 1),
        (turn_y, 2),
        (turn_x, 2),
        (load, 3),
        (back_tail, 0),
        (add_early,),
        (back_tiles, 4),
        (hand_on, 1),
        (back_tiles, 5),
        (turn_y, 3),
        (hand_on, 2),
        (turn_x, 3),
        (back_tiles, 6),
        (turn_early,),
        (back_tiles, 7),
        (back_tail, 1),
        (send_terms,),
        (hand_on, 3),
        (keep_early,),
        (finish_rows,),
        (add_terms,),
        (spread_rows,),
        (pair_terms,),
        (keep_taps,),
        (gather_rows,),
        (keep,),
    ):
        step(*at)
    net.finish()


def fused_body(value_half, gate_half, upstream, conv_taps, norm_gain, out_weight):
    f32, bf16 = jnp.float32, jnp.bfloat16
    nsp, ndp = lax.axis_size("sp"), lax.axis_size("dp")
    nz = ndp // 2
    _, length, channels = value_half.shape
    rows = out_weight.shape[0]
    tap_count, width = conv_taps.shape
    halo = (tap_count - 1 + 15) // 16 * 16
    half, share = channels // 2, 2 * rows // nsp
    lead = half // 4
    side, e_side = (half - lead) // 2, lead // 2
    tap_rows = (tap_count + 8) // 8 * 8

    def shape(*dims, dtype=bf16):
        return jax.ShapeDtypeStruct(dims, dtype)

    def vmem(*dims, dtype=bf16):
        return pltpu.VMEM(dims, dtype)

    any_space = pl.BlockSpec(memory_space=pl.ANY)
    remote = 60 + 30 * nz
    grad_value, grad_gate, grad_taps, grad_gain, grad_weight = pl.pallas_call(
        fused,
        out_shape=[
            shape(length, channels),
            shape(length, channels),
            shape(tap_count, width, dtype=f32),
            shape(1, channels, dtype=f32),
            shape(rows, channels, dtype=f32),
        ],
        in_specs=[any_space] * 6,
        out_specs=[VMEM] * 5,
        scratch_shapes=[
            vmem(length, channels),
            vmem(length, channels),
            vmem(2 * length, channels),
            vmem(nsp, tap_count, width, dtype=f32),
            vmem(1, channels, dtype=f32),
            vmem(ndp * rows, channels),
            vmem(halo, channels),
            vmem(halo, channels),
            vmem(length + halo, channels, dtype=f32),
            vmem(length, channels, dtype=f32),
            vmem(length, LANES, dtype=f32),
            vmem(2 * length, half),
            vmem(length, channels),
            vmem(nz, 2 * rows, half),
            vmem(nz, 2, share, side),
            vmem(nz, 2, share, side),
            vmem(nz, share, side),
            vmem(nz, share, side),
            vmem(nz, share, half - lead),
            vmem(nz, share, half - lead),
            vmem(2 * rows, half),
            vmem(rows, half),
            vmem(nz, share, side),
            vmem(nz, share, side),
            vmem(nz, 2 * rows, lead),
            vmem(2 * rows, lead),
            vmem(2, share, e_side),
            vmem(2, share, e_side),
            vmem(share, e_side),
            vmem(share, e_side),
            vmem(share, e_side),
            vmem(share, e_side),
            vmem(length, channels, dtype=f32),
            vmem(halo, channels),
            vmem(halo, channels),
            vmem(length + halo, channels, dtype=f32),
            vmem(tap_count, 8, channels, dtype=f32),
            vmem(8, channels, dtype=f32),
            vmem(nsp, tap_rows, width, dtype=f32),
            vmem(nsp, tap_rows, width, dtype=f32),
            vmem(nz, tap_rows, width, dtype=f32),
            vmem(tap_rows, width, dtype=f32),
            vmem(tap_rows, width, dtype=f32),
            vmem(tap_rows, width, dtype=f32),
            vmem(nsp, 8, width, dtype=f32),
            pltpu.SemaphoreType.DMA((remote,)),
            pltpu.SemaphoreType.DMA((remote,)),
            pltpu.SemaphoreType.DMA((8,)),
        ],
        compiler_params=pltpu.CompilerParams(
            collective_id=7, has_side_effects=True, vmem_limit_bytes=60 * 1024 * 1024
        ),
    )(value_half, gate_half, upstream, conv_taps, norm_gain[None], out_weight)
    return (grad_value[None], grad_gate[None], grad_taps, grad_gain[0], grad_weight)


def solution(mesh):
    tokens = P("dp", "sp", None)
    quarters = mesh.shape["sp"] == 4 and mesh.shape["dp"] == 8
    return jax.shard_map(
        fused_body if quarters else body,
        mesh=mesh,
        in_specs=(tokens, tokens, tokens, P(None, "sp"), P(), P("dp", None)),
        out_specs=(tokens, tokens, P(None, "sp"), P(), P("dp", None)),
        check_vma=False,
    )
```

```python
import functools

import jax
import jax.numpy as jnp
from jax import lax
from jax.experimental import pallas as pl
from jax.experimental.pallas import tpu as pltpu
from jax.sharding import PartitionSpec as P

NORM_EPS = 1e-05
VMEM = pl.BlockSpec(memory_space=pltpu.VMEM)


def when(condition, act):
    if condition is None:
        act()
    else:
        pl.when(condition)(lambda: act())


class Copies:
    def __init__(self, send, recv, local):
        self.send, self.recv, self.local = send, recv, local
        self.n_remote = self.n_local = 0
        self.remote, self.locals = [], []

    def start(self, src, dst, target, sends=None, receives=None):
        i = self.n_remote
        self.n_remote += 1
        copy = pltpu.make_async_remote_copy(
            src_ref=src,
            dst_ref=dst,
            send_sem=self.send.at[i],
            recv_sem=self.recv.at[i],
            device_id=target,
            device_id_type=pl.DeviceIdType.MESH,
        )
        when(sends, copy.start)
        self.remote.append([copy, False, sends, receives])
        return len(self.remote) - 1

    def keep(self, src, dst):
        copy = pltpu.make_async_copy(src, dst, self.local.at[self.n_local])
        self.n_local += 1
        copy.start()
        self.locals.append(copy)

    def arrive(self, i):
        when(self.remote[i][3], self.remote[i][0].wait_recv)
        self.remote[i][1] = True

    def finish(self):
        for copy, arrived, sends, receives in self.remote:
            if not arrived:
                when(receives, copy.wait_recv)
            when(sends, copy.wait_send)
        for copy in self.locals:
            copy.wait()


def greet(axes):
    barrier = pltpu.get_barrier_semaphore()
    count = 0
    for axis in axes:
        n = lax.axis_size(axis)
        me = lax.axis_index(axis)
        for k in range(1, n):
            pl.semaphore_signal(
                barrier,
                inc=1,
                device_id={axis: lax.rem(me + k, n)},
                device_id_type=pl.DeviceIdType.MESH,
            )
            count += 1
    pl.semaphore_wait(barrier, count)


def direct(copies, kind, axis, src, dst):
    n = lax.axis_size(axis)
    me = lax.axis_index(axis)
    if kind == "next" or kind == "prev":
        copies.start(src, dst, {axis: lax.rem(me + (1 if kind == "next" else n - 1), n)})
        return
    if kind == "pair":
        copies.start(src, dst, {axis: me + 1 - 2 * lax.rem(me, 2)})
        return
    if kind == "rows":
        nz, z, c = n // 2, me // 2, lax.rem(me, 2)
        copies.keep(src.at[z], dst.at[z])
        for k in range(1, nz):
            peer = lax.rem(z + k, nz)
            copies.start(src.at[peer], dst.at[z], {axis: 2 * peer + c})
        return
    copies.keep(src.at[me] if kind == "scatter" else src, dst.at[me])
    for k in range(1, n):
        peer = lax.rem(me + k, n)
        copies.start(src.at[peer] if kind == "scatter" else src, dst.at[me], {axis: peer})


def spread_gather(copies, src, dst):
    ns, nz = lax.axis_size("sp"), lax.axis_size("dp") // 2
    s, d = lax.axis_index("sp"), lax.axis_index("dp")
    z, c = d // 2, lax.rem(d, 2)
    partner = {"dp": d + 1 - 2 * c}
    first = [
        copies.start(src.at[s], dst.at[d, s], {"dp": 2 * lax.rem(z + k, nz) + c})
        for k in range(1, nz)
    ]
    yield
    copies.keep(src, dst.at[d])
    copies.start(src, dst.at[d], partner)
    second = {}
    for k in range(1, nz):
        copies.arrive(first[k - 1])
        piece = dst.at[2 * lax.rem(z + nz - k, nz) + c, s]
        for j in range(1, ns):
            second[k, j] = copies.start(piece, piece, {"sp": lax.rem(s + j, ns)})
        copies.start(piece, piece, partner)
    yield
    for k in range(1, nz):
        for j in range(1, ns):
            copies.arrive(second[k, j])
            piece = dst.at[2 * lax.rem(z + nz - k, nz) + c, lax.rem(s + ns - j, ns)]
            copies.start(piece, piece, partner)


def line_gather(copies, src, dst):
    nz = lax.axis_size("dp") // 2
    d = lax.axis_index("dp")
    z, c = d // 2, lax.rem(d, 2)
    partner = {"dp": d + 1 - 2 * c}
    up = {"dp": 2 * lax.rem(z + 1, nz) + c}
    down = {"dp": 2 * lax.rem(z + nz - 1, nz) + c}
    below, above = {}, {}

    def send(k):
        low, high = 2 * lax.rem(z + nz - k, nz) + c, 2 * lax.rem(z + k, nz) + c
        low_src, high_src = (dst.at[low], dst.at[high]) if k else (src, src)
        below[k] = copies.start(
            low_src, dst.at[low], up, jnp.logical_and(z >= k, z < nz - 1), z >= k + 1
        )
        above[k] = copies.start(
            high_src, dst.at[high], down, jnp.logical_and(z + k < nz, z > 0), z + k + 1 < nz
        )

    send(0)
    yield
    copies.keep(src, dst.at[d])
    copies.start(src, dst.at[d], partner)
    for k in range(1, nz):
        copies.arrive(below[k - 1])
        copies.arrive(above[k - 1])
        if k < nz - 1:
            send(k)
        low, high = dst.at[2 * lax.rem(z + nz - k, nz) + c], dst.at[2 * lax.rem(z + k, nz) + c]
        copies.start(low, low, partner, z >= k, z >= k)
        copies.start(high, high, partner, z + k < nz, z + k < nz)
        yield


def run(axes, items, *refs):
    n = len(items)
    copies = Copies(*refs[2 * n :])
    greet(axes)
    waiting = []
    for i, (kind, axis) in enumerate(items):
        src, dst = refs[i], refs[n + i]
        if kind == "spread":
            waiting.append(spread_gather(copies, src, dst))
        elif kind == "line":
            waiting.append(line_gather(copies, src, dst))
        elif kind == "later":
            waiting.append(later(copies, axis, src, dst))
        else:
            direct(copies, kind, axis, src, dst)
    while waiting:
        waiting = [steps for steps in waiting if next(steps, waiting) is None]
    copies.finish()


def later(copies, axis, src, dst):
    yield
    direct(copies, "scatter", axis, src, dst)


def exchange(collective_id, *items):
    ns, nd = lax.axis_size("sp"), lax.axis_size("dp")
    shapes, remote, local = [], 0, 0
    for kind, axis, x in items:
        n = lax.axis_size(axis)
        if kind == "rows":
            shape = x.shape
            remote += n // 2 - 1
            local += 1
        elif kind in ("next", "prev", "pair"):
            shape = x.shape
            remote += 1
        elif kind in ("scatter", "later"):
            shape = x.shape
            remote += n - 1
            local += 1
        else:
            shape = (n,) + x.shape
            local += 1
            if kind == "gather":
                remote += n - 1
            elif kind == "spread":
                remote += (nd // 2 - 1) * 2 * ns + 1
            else:
                remote += (nd // 2 - 1) * 4 + 1
        shapes.append(jax.ShapeDtypeStruct(shape, x.dtype))
    axes = tuple(a for a in ("sp", "dp") if any(axis == a or kind == "spread" for kind, axis, _ in items))
    return pl.pallas_call(
        functools.partial(run, axes, tuple((kind, axis) for kind, axis, _ in items)),
        out_shape=shapes,
        in_specs=[VMEM] * len(items),
        out_specs=[VMEM] * len(items),
        scratch_shapes=[
            pltpu.SemaphoreType.DMA((remote,)),
            pltpu.SemaphoreType.DMA((remote,)),
            pltpu.SemaphoreType.DMA((max(local, 1),)),
        ],
        compiler_params=pltpu.CompilerParams(
            collective_id=collective_id, has_side_effects=True, vmem_limit_bytes=48 * 1024 * 1024
        ),
    )(*[x for _, _, x in items])


def body(value_half, gate_half, upstream, conv_taps, norm_gain, out_weight):
    f32 = jnp.float32
    tap_count = conv_taps.shape[0]
    halo = tap_count - 1
    nsp, ndp = lax.axis_size("sp"), lax.axis_size("dp")
    at_start = lax.axis_index("sp") == 0
    at_end = lax.axis_index("sp") == nsp - 1
    edge = (halo + 15) // 16 * 16

    value = value_half[0].astype(f32)
    gate = gate_half[0].astype(f32)
    length = value.shape[0]
    channels = value.shape[1]
    up = upstream[0]
    rows = out_weight.shape[0]

    tail = (value[length - edge :] * jax.nn.sigmoid(gate[length - edge :])).astype(jnp.bfloat16)
    up_blocks = jnp.swapaxes(up.reshape(length, ndp, rows), 0, 1)
    before, taps = exchange(1, ("next", "sp", tail), ("gather", "sp", conv_taps))
    before = jnp.where(at_start, 0, before)[edge - halo :]
    taps = jnp.swapaxes(taps, 0, 1).reshape(tap_count, channels)
    sig_gate = jax.nn.sigmoid(gate)
    glu = (value * sig_gate).astype(jnp.bfloat16)
    padded = jnp.concatenate([before, glu], axis=0).astype(f32)
    conv = jnp.zeros((length, padded.shape[1]), f32)
    for j in range(tap_count):
        conv = conv + taps[j] * padded[j : j + length]
    conv = conv.astype(jnp.bfloat16).astype(f32)
    mean = jnp.mean(conv, axis=-1, keepdims=True)
    centered = conv - mean
    inv = lax.rsqrt(jnp.mean(centered * centered, axis=-1, keepdims=True) + NORM_EPS)
    normed = centered * inv
    scaled = normed * norm_gain
    sig = jax.nn.sigmoid(scaled)
    activated = (scaled * sig).astype(jnp.bfloat16)

    half = channels // 2
    nz, piece = ndp // 2, rows // nsp
    core = lax.rem(lax.axis_index("dp"), 2)
    by_core = up.reshape(length, nz, 2, nsp, piece)

    def partial(which):
        columns = lax.dynamic_index_in_dim(by_core, which, 2, keepdims=False)
        columns = jnp.swapaxes(columns, 1, 2).reshape(length, nsp * nz * piece)
        return lax.dot_general(
            columns, activated[:, half:], (((0,), (0,)), ((), ())), preferred_element_type=f32
        )

    weight, act_all, up_columns, from_partner = exchange(
        2,
        ("spread", "dp", out_weight.reshape(nsp, rows // nsp, channels)),
        ("line", "dp", activated[:, :half]),
        ("later", "dp", up_blocks),
        ("pair", "dp", partial(1 - core).astype(jnp.bfloat16)),
    )
    weight = weight.reshape(ndp * rows, channels)
    act_all = act_all.reshape(ndp * length, half)
    up_columns = up_columns.reshape(ndp * length, rows)
    owned = lax.dot_general(
        up_columns, act_all, (((0,), (0,)), ((), ())), preferred_element_type=f32
    )
    summed = (partial(core) + from_partner.astype(f32)).astype(jnp.bfloat16)
    summed = summed.reshape(nsp, nz, piece, half)

    grad_act = jnp.dot(up, weight, preferred_element_type=f32)
    grad_scaled = grad_act * sig * (1.0 + scaled * (1.0 - sig))
    gain_part = jnp.sum(grad_scaled * normed, axis=0)
    g = grad_scaled * norm_gain
    grad_conv = inv * (
        g
        - jnp.mean(g, axis=-1, keepdims=True)
        - normed * jnp.mean(g * normed, axis=-1, keepdims=True)
    )
    grad_conv = grad_conv.astype(jnp.bfloat16)
    after, gain_got, owned_got, summed_got = exchange(
        3,
        ("prev", "sp", grad_conv[:edge]),
        ("gather", "sp", gain_part[None]),
        ("scatter", "sp", owned.astype(jnp.bfloat16).reshape(nsp, piece, half)),
        ("scatter", "sp", summed),
    )
    after = jnp.where(at_end, 0, after)[:halo]
    extended = jnp.concatenate([grad_conv, after], axis=0).astype(f32)
    here = grad_conv.astype(f32)
    grad_glu = jnp.zeros_like(here)
    terms = []
    for j in range(tap_count):
        first = halo - j
        grad_glu = grad_glu + taps[j] * extended[first : first + length]
        terms.append(jnp.sum(here * padded[j : j + length], axis=0))
    grad_glu = grad_glu.astype(jnp.bfloat16).astype(f32)
    grad_value = (grad_glu * sig_gate).astype(jnp.bfloat16)
    grad_gate = (grad_glu * value * sig_gate * (1.0 - sig_gate)).astype(jnp.bfloat16)

    width = conv_taps.shape[1]
    tap_blocks = jnp.swapaxes(jnp.stack(terms).reshape(tap_count, nsp, width), 0, 1)
    gain_got, tap_got, low_weight, high_got = exchange(
        4,
        ("gather", "dp", jnp.sum(gain_got, axis=0)),
        ("scatter", "sp", tap_blocks),
        ("gather", "sp", jnp.sum(owned_got.astype(f32), axis=0).astype(jnp.bfloat16)),
        ("rows", "dp", jnp.sum(summed_got.astype(f32), axis=0).astype(jnp.bfloat16)),
    )
    tap_got, high_weight = exchange(
        5,
        ("gather", "dp", jnp.sum(tap_got, axis=0)),
        ("gather", "sp", jnp.sum(high_got.astype(f32), axis=0).astype(jnp.bfloat16)),
    )
    grad_gain = jnp.sum(gain_got, axis=0)[0]
    grad_taps = jnp.sum(tap_got, axis=0)
    grad_weight = jnp.concatenate(
        [low_weight.reshape(rows, half), high_weight.reshape(rows, half)], axis=1
    ).astype(f32)
    return (grad_value[None], grad_gate[None], grad_taps, grad_gain, grad_weight)


BLOCK = 64
LANES = 128


class Net:
    def __init__(self, send, recv, local):
        self.send, self.recv, self.local = send, recv, local
        self.n = self.m = 0
        self.open = []
        self.landing = []

    def ids(self, count):
        self.n += count
        return self.n - count

    def put(self, src, dst, to, slot=None, sends=None):
        i = self.ids(1)
        copy = pltpu.make_async_remote_copy(
            src_ref=src,
            dst_ref=dst,
            send_sem=self.send.at[i],
            recv_sem=self.recv.at[i if slot is None else slot],
            device_id=to,
            device_id_type=pl.DeviceIdType.MESH,
        )
        when(sends, copy.start)
        self.open.append((copy, sends))
        return copy

    def arrival(self, ref, slot, to):
        pltpu.make_async_remote_copy(
            src_ref=ref,
            dst_ref=ref,
            send_sem=self.send.at[0],
            recv_sem=self.recv.at[slot],
            device_id=to,
            device_id_type=pl.DeviceIdType.MESH,
        ).wait_recv()

    def load(self, src, dst):
        copy = pltpu.make_async_copy(src, dst, self.local.at[self.m])
        self.m += 1
        copy.start()
        return copy

    def finish(self):
        for copy, sends in self.open:
            when(sends, copy.wait_send)


def nearest(z, nz, i):
    low, high = z, nz - 1 - z
    both = 2 * jnp.minimum(low, high)
    away = jnp.where(i < both, i // 2 + 1, i - both // 2 + 1)
    up = jnp.where(i < both, i % 2 == 0, high > low)
    return jnp.where(up, z + away, z - away)


def fused(
    value_hbm, gate_hbm, up_hbm, taps_hbm, gain_hbm, weight_hbm,
    grad_value, grad_gate, grad_taps, grad_gain, grad_weight,
    value, gate, ups, taps, gain, weight, tail, before, padded, conv, scale, acts, act,
    parts, got_x, got_y, got_xy, got_yx, plane, got_z, final, halves, give_x, give_y,
    got_e, early, e_x, e_y, e_xy, e_yx, e_give_x, e_give_y,
    grad_act, head, after, grads, tap_sums, gain_sum, terms, got_terms, got_dp, row_part, both_parts,
    tap_other, tap_mate, tap_half, gain_row, gain_mate, gain_pair, gain_sp, gain_part, gain_dp,
    send, recv, local,
):
    f32, bf16 = jnp.float32, jnp.bfloat16
    nsp, ndp = lax.axis_size("sp"), lax.axis_size("dp")
    nz = ndp // 2
    s, d = lax.axis_index("sp"), lax.axis_index("dp")
    z, c = d // 2, lax.rem(d, 2)
    xn, yn = s + 1 - 2 * lax.rem(s, 2), lax.rem(s + 2, nsp)
    dg = nsp - 1 - s
    length, channels = value.shape
    halo = before.shape[0]
    tap_count = taps.shape[1]
    width = taps.shape[2]
    rows = weight.shape[0] // ndp
    half = channels // 2
    lead = got_e.shape[2]
    rest = half - lead
    side, e_side = rest // 2, lead // 2
    quarter = channels // nsp
    share = 2 * rows // nsp
    tiles = channels // LANES
    tap_rows, tap_width = terms.shape[2:]
    net = Net(send, recv, local)
    to_x, to_y, to_d, partner = {"sp": xn}, {"sp": yn}, {"sp": dg}, {"dp": d + 1 - 2 * c}

    def at_chip(peer):
        return {"dp": 2 * peer + c}

    def al(i, n):
        return pl.multiple_of(i, n)

    in_up = net.load(up_hbm.at[0], ups.at[pl.ds(0, length)])
    in_weight = net.load(weight_hbm, weight.at[pl.ds(al(d * rows, rows), rows)])
    in_value = net.load(value_hbm.at[0], value)
    in_gate = net.load(gate_hbm.at[0], gate)
    in_taps = net.load(taps_hbm, taps.at[s])
    in_gain = net.load(gain_hbm, gain)

    barrier = pltpu.get_barrier_semaphore()
    peers = [to_x, to_y, to_d, partner] + [at_chip(lax.rem(z + k, nz)) for k in range(1, nz)]
    for peer in peers:
        pl.semaphore_signal(barrier, inc=1, device_id=peer, device_id_type=pl.DeviceIdType.MESH)
    pl.semaphore_wait(barrier, len(peers))

    def piece(owner, q, h):
        r = rows // 2
        return weight.at[
            pl.ds(al(owner * rows + h * r, r), r), pl.ds(al(q * quarter, quarter), quarter)
        ]

    above, below = at_chip(lax.rem(z + 1, nz)), at_chip(lax.rem(z + nz - 1, nz))

    def along(src, h):
        p, slot = piece(2 * src + c, s, h), w_slots + 2 * src + h
        net.put(p, p, above, slot, jnp.logical_and(src <= z, z < nz - 1))
        net.put(p, p, below, slot, jnp.logical_and(src >= z, z > 0))

    in_taps.wait()
    tap_copies = [net.put(taps.at[s], taps.at[s], to) for to in (to_x, to_y, to_d)]
    w_slots = net.ids(2 * nz)
    in_weight.wait()
    for h in range(2):
        along(z, h)

    arrived = {}
    mates = {}

    def first(i, h):
        src = nearest(z, nz, i)
        owner = 2 * src + c
        net.arrival(piece(owner, s, h), w_slots + 2 * src + h, partner)
        along(src, h)
        p = piece(owner, s, h)
        arrived[i, h] = [net.put(p, p, to_x), net.put(p, p, to_y)]
        mates.setdefault(i, []).append(net.put(p, p, partner))

    def second(i, h):
        owner = 2 * nearest(z, nz, i) + c
        from_x, from_y = arrived[i, h]
        px, py = piece(owner, xn, h), piece(owner, yn, h)
        if h == 0:
            from_x.wait_recv()
            arrived[i, h] = net.put(px, px, to_y)
            from_y.wait_recv()
        else:
            from_y.wait_recv()
            arrived[i, h] = net.put(py, py, to_x)
            from_x.wait_recv()
        mates[i] += [net.put(px, px, partner), net.put(py, py, partner)]

    def third(i, h):
        owner = 2 * nearest(z, nz, i) + c
        arrived[i, h].wait_recv()
        p = piece(owner, dg, h)
        mates[i].append(net.put(p, p, partner))

    in_value.wait()
    in_gate.wait()
    v = value[length - halo :, :].astype(f32)
    tail[...] = (v * jax.nn.sigmoid(gate[length - halo :, :].astype(f32))).astype(bf16)

    def glu_rows(i, _):
        r = al(i * 16, 16)
        v = value[pl.ds(r, 16), :].astype(f32)
        g = (v * jax.nn.sigmoid(gate[pl.ds(r, 16), :].astype(f32))).astype(bf16)
        padded[pl.ds(al(r + halo, 8), 16), :] = g.astype(f32)
        return 0

    lax.fori_loop(0, 2, glu_rows, 0)
    left = net.put(tail, before, {"sp": lax.rem(s + 1, nsp)}, None, s < nsp - 1)
    in_up.wait()
    own_rows = weight.at[pl.ds(al(d * rows, rows), rows)]
    own_up = net.put(ups.at[pl.ds(0, length)], ups.at[pl.ds(length, length)], partner)
    own_weight = net.put(own_rows, own_rows, partner)
    lax.fori_loop(2, length // 16, glu_rows, 0)

    def tap_from(n):
        tap_copies[n].wait_recv()

    def left_halo():
        when(s > 0, left.wait_recv)

        @pl.when(s == 0)
        def _():
            before[...] = jnp.zeros_like(before)

        padded[pl.ds(0, halo), :] = before[...].astype(f32)

    per_block = width // LANES

    def tap(t, j):
        q, lane = t // per_block, lax.rem(t, per_block)
        return taps[q, pl.ds(j, 1), pl.ds(al(lane * LANES, LANES), LANES)]

    def turned(window, r):
        return window if r == 0 else pltpu.roll(window, window.shape[0] - r, 0)

    def conv_block(t, i):
        cols = pl.ds(al(t * LANES, LANES), LANES)
        r0 = al(i * BLOCK, BLOCK)
        window = padded[pl.ds(r0, BLOCK + halo), cols]
        total = jnp.zeros((BLOCK, LANES), f32)
        for r in range(8):
            moved = turned(window, r)
            for o in range(r, halo + 1, 8):
                j = o - (halo - tap_count + 1)
                if 0 <= j < tap_count:
                    total = total + tap(t, j) * moved[o - r : o - r + BLOCK]
        conv[pl.ds(r0, BLOCK), cols] = total.astype(bf16).astype(f32)

    row_blocks = length // BLOCK

    def conv_quarter(n):
        q = (s, xn, yn, dg)[n]
        inner = row_blocks - 1

        def one(m, _):
            conv_block(q * per_block + m // inner, 1 + lax.rem(m, inner))
            return 0

        lax.fori_loop(0, per_block * inner, one, 0)

    def conv_head(n):
        def one(t, _):
            conv_block(t, 0)
            return 0

        lax.fori_loop(n * tiles // 2, (n + 1) * tiles // 2, one, 0)

    in_gain.wait()

    def norm_rows(i, _):
        r = al(i * 16, 16)
        rr = pl.ds(r, 16)
        x = conv[rr, :]
        mean = jnp.mean(x, axis=-1, keepdims=True)
        x = x - mean
        inv = lax.rsqrt(jnp.mean(x * x, axis=-1, keepdims=True) + NORM_EPS)
        normed = x * inv
        conv[rr, :] = normed
        scale[rr, :] = jnp.broadcast_to(inv, (16, LANES))
        scaled = normed * gain[...]
        act[rr, :] = (scaled * jax.nn.sigmoid(scaled)).astype(bf16)
        return 0

    blocks = length // 16

    def norm(n):
        lax.fori_loop(n * blocks // 4, (n + 1) * blocks // 4, norm_rows, 0)

    mine = pl.ds(al(c * half, half), half)
    other = pl.ds(al((1 - c) * half, half), half)
    swapped = []

    def swap():
        swapped.append(net.put(act.at[:, other], acts.at[pl.ds(length, length)], partner))
        acts[pl.ds(0, length), :] = act[:, mine]

    def swap_done():
        own_up.wait_recv()
        swapped[0].wait_recv()

    def target(k):
        return nearest(z, nz, nz - 2 - k) if k < nz - 1 else z

    def multiply(k):
        t = target(k)
        step = min(256, 2 * rows)

        def some(m, _):
            u = ups[:, pl.ds(al(t * 2 * rows + m * step, step), step)]
            p = lax.dot_general(u, acts[...], (((0,), (0,)), ((), ())), preferred_element_type=f32)
            parts[k, pl.ds(al(m * step, step), step), :] = p.astype(bf16)
            return 0

        lax.fori_loop(0, 2 * rows // step, some, 0)

    class Plane:
        def __init__(self, src, w, x, y, xy, yx, give_x, give_y):
            self.src, self.w = src, w
            self.x, self.y, self.xy, self.yx = x, y, xy, yx
            self.give_x, self.give_y = give_x, give_y

        def at(self, q, h):
            return pl.ds(al(q * share, share), share), pl.ds(h * self.w, self.w)

        def part(self, q, h):
            return self.src[self.at(q, h)].astype(f32)

        def send(self):
            def unit(q, h):
                return self.src.at[self.at(q, h)]

            self.far_x = net.put(unit(dg, 0), self.x.at[1], to_x)
            self.far_y = net.put(unit(dg, 1), self.y.at[1], to_y)
            self.near_x = net.put(unit(xn, 0), self.x.at[0], to_x)
            self.near_y = net.put(unit(yn, 1), self.y.at[0], to_y)

        def turn_x(self):
            self.far_x.wait_recv()
            self.give_y[...] = (self.part(yn, 0) + self.x[1].astype(f32)).astype(bf16)
            self.last_y = net.put(self.give_y, self.xy, to_y)

        def turn_y(self):
            self.far_y.wait_recv()
            self.give_x[...] = (self.part(xn, 1) + self.y[1].astype(f32)).astype(bf16)
            self.last_x = net.put(self.give_x, self.yx, to_x)

        def total(self):
            for copy in (self.near_x, self.near_y, self.last_x, self.last_y):
                copy.wait_recv()
            low = self.part(s, 0) + self.x[0].astype(f32) + self.xy[...].astype(f32)
            high = self.part(s, 1) + self.y[0].astype(f32) + self.yx[...].astype(f32)
            return low.astype(bf16), high.astype(bf16)

    chunks = [
        Plane(
            parts.at[k], side, got_x.at[k], got_y.at[k], got_xy.at[k], got_yx.at[k],
            give_x.at[k], give_y.at[k],
        )
        for k in range(nz)
    ]
    ahead = Plane(early, e_side, e_x, e_y, e_xy, e_yx, e_give_x, e_give_y)
    z_slots, e_slots = net.ids(nz), net.ids(nz)

    def load(k):
        chunks[k].send()

    def turn_x(k):
        chunks[k].turn_x()

    def turn_y(k):
        chunks[k].turn_y()

    def hand_on(k):
        low, high = chunks[k].total()
        plane[k, :, pl.ds(0, side)] = low
        plane[k, :, pl.ds(side, side)] = high
        if k < nz - 1:
            net.put(plane.at[k], got_z.at[z], at_chip(target(k)), z_slots + z)

    def send_early(k):
        if k < nz - 1:
            tops = parts.at[k, :, pl.ds(rest, lead)]
            net.put(tops, got_e.at[z], at_chip(target(k)), e_slots + z)

    def add_early():
        total = parts[nz - 1, :, pl.ds(rest, lead)].astype(f32)
        for i in range(nz - 1):
            src = nearest(z, nz, i)
            net.arrival(got_e.at[src], e_slots + src, partner)
            total = total + got_e[src].astype(f32)
        early[...] = total.astype(bf16)
        ahead.send()

    def turn_early():
        ahead.turn_x()
        ahead.turn_y()

    def keep_early():
        low, high = ahead.total()
        own = pl.ds(al(s * share, share), share)
        final[own, pl.ds(rest, e_side)] = low
        final[own, pl.ds(rest + e_side, e_side)] = high

    def product(owner, start):
        w = weight[pl.ds(al(owner * rows, rows), rows), :]
        u = ups[pl.ds(0, length), pl.ds(al(owner * rows, rows), rows)]
        p = jnp.dot(u, w, preferred_element_type=f32)
        grad_act[...] = p if start else grad_act[...] + p

    def product_own():
        product(d, True)

    def product_mate():
        own_weight.wait_recv()
        product(d + 1 - 2 * c, False)

    def blocks_of(i):
        assert len(mates[i]) == 8
        for copy in mates[i]:
            copy.wait_recv()
        src = nearest(z, nz, i)

        def one(n, _):
            product(2 * src + n, False)
            return 0

        lax.fori_loop(0, 2, one, 0)

    gain_sum[...] = jnp.zeros_like(gain_sum)

    def back_rows(i, _):
        r = al(i * 16, 16)
        rr = pl.ds(r, 16)
        normed = conv[rr, :]
        scaled = normed * gain[...]
        sig = jax.nn.sigmoid(scaled)
        gs = grad_act[rr, :] * sig * (1.0 + scaled * (1.0 - sig))
        gn = gs * normed
        gain_sum[...] += gn[:8] + gn[8:]
        g = gs * gain[...]
        m1 = jnp.mean(g, axis=-1, keepdims=True)
        m2 = jnp.mean(g * normed, axis=-1, keepdims=True)
        gc = (scale[rr, 0:1] * (g - m1 - normed * m2)).astype(bf16)
        grads[rr, :] = gc.astype(f32)
        return 0

    ready = []

    def back_head():
        lax.fori_loop(0, halo // 16, back_rows, 0)
        head[...] = grads[pl.ds(0, halo), :].astype(bf16)
        ready.append(net.put(head, after, {"sp": lax.rem(s + nsp - 1, nsp)}, None, s > 0))

    def back(n):
        mid = (blocks + halo // 16) // 2
        lax.fori_loop((halo // 16, mid)[n], (mid, blocks)[n], back_rows, 0)

    def right_halo():
        when(s < nsp - 1, ready[0].wait_recv)

        @pl.when(s == nsp - 1)
        def _():
            after[...] = jnp.zeros_like(after)

        grads[pl.ds(length, halo), :] = after[...].astype(f32)

    tap_sums[...] = jnp.zeros_like(tap_sums)

    def back_block(t, i):
        cols = pl.ds(al(t * LANES, LANES), LANES)
        r0 = al(i * BLOCK, BLOCK)
        rr = pl.ds(r0, BLOCK)
        window = grads[pl.ds(r0, BLOCK + halo), cols]
        total = jnp.zeros((BLOCK, LANES), f32)
        for r in range(8):
            moved = turned(window, r)
            for o in range(r, tap_count, 8):
                total = total + tap(t, tap_count - 1 - o) * moved[o - r : o - r + BLOCK]
        gg = total.astype(bf16).astype(f32)
        sg = jax.nn.sigmoid(gate[rr, cols].astype(f32))
        grad_value[rr, cols] = (gg * sg).astype(bf16)
        grad_gate[rr, cols] = (gg * value[rr, cols].astype(f32) * sg * (1.0 - sg)).astype(bf16)
        gc = window[:BLOCK]
        window = padded[pl.ds(r0, BLOCK + halo), cols]
        for r in range(8):
            moved = turned(window, r)
            for o in range(r, halo + 1, 8):
                j = o - (halo - tap_count + 1)
                if 0 <= j < tap_count:
                    term = (gc * moved[o - r : o - r + BLOCK]).reshape(BLOCK // 8, 8, LANES)
                    tap_sums[j, :, cols] += jnp.sum(term, axis=0)

    def back_tiles(n):
        inner = row_blocks - 1

        def one(m, _):
            back_block(m // inner, lax.rem(m, inner))
            return 0

        step = tiles // 8 * inner
        lax.fori_loop(n * step, (n + 1) * step, one, 0)

    def back_tail(n):
        def one(t, _):
            back_block(t, row_blocks - 1)
            cols = pl.ds(al(t * LANES, LANES), LANES)
            q, lane = t // per_block, lax.rem(t, per_block)
            e, lane = lane // (per_block // 2), lax.rem(lane, per_block // 2)
            lanes = pl.ds(al(lane * LANES, LANES), LANES)
            terms[e, q, pl.ds(0, tap_count), lanes] = jnp.sum(tap_sums[:, :, cols], axis=1)
            return 0

        lax.fori_loop(n * tiles // 2, (n + 1) * tiles // 2, one, 0)

    sums = {}

    def send_gain():
        gain_row[...] = jnp.sum(gain_sum[...], axis=0, keepdims=True)
        sums["gain"] = net.put(gain_row, gain_mate, partner)

    def pair_gain():
        sums["gain"].wait_recv()
        gain_pair[...] = gain_row[...] + gain_mate[...]
        gain_sp[s] = gain_pair[...]
        sums["gain"] = [net.put(gain_pair, gain_sp.at[s], to) for to in (to_d, to_x, to_y)]

    gain_slots = net.ids(nz)

    def line_gain():
        for copy in sums["gain"]:
            copy.wait_recv()
        total = gain_sp[0]
        for q in range(1, nsp):
            total = total + gain_sp[q]
        gain_part[...] = total
        gain_dp[z] = total
        for i in range(nz - 1):
            net.put(gain_part, gain_dp.at[z], at_chip(nearest(z, nz, i)), gain_slots + z)

    def keep_gain():
        for i in range(nz - 1):
            src = nearest(z, nz, i)
            net.arrival(gain_dp.at[src], gain_slots + src, partner)
        total = gain_dp[0]
        for i in range(1, nz):
            total = total + gain_dp[i]
        grad_gain[...] = total

    def send_terms():
        sums["mate"] = net.put(terms.at[1 - c], tap_mate, partner)

    def pair_sums():
        sums["mate"].wait_recv()
        tap_half[...] = terms[c] + tap_mate[...]
        got_terms[s] = tap_half[s]
        sums["sp"] = [
            net.put(tap_half.at[peer], got_terms.at[s], to)
            for peer, to in ((dg, to_d), (xn, to_x), (yn, to_y))
        ]

    tap_slots = net.ids(nz)

    def add_terms():
        for copy in sums["sp"]:
            copy.wait_recv()
        total = got_terms[0]
        for q in range(1, nsp):
            total = total + got_terms[q]
        row_part[...] = total
        got_dp[z] = total
        for i in range(nz - 1):
            net.put(row_part, got_dp.at[z], at_chip(nearest(z, nz, i)), tap_slots + z)

    def done(q, h):
        return final.at[pl.ds(al(q * share, share), share), pl.ds(h * half // 2, half // 2)]

    sent = {}

    def finish_rows():
        total = plane[nz - 1].astype(f32)
        for i in range(nz - 1):
            src = nearest(z, nz, i)
            net.arrival(got_z.at[src], z_slots + src, partner)
            total = total + got_z[src].astype(f32)
        final[pl.ds(al(s * share, share), share), pl.ds(0, rest)] = total.astype(bf16)
        for axis, h in (("x", 0), ("y", 1), ("y", 0), ("x", 1)):
            sent[axis, h] = net.put(done(s, h), done(s, h), to_x if axis == "x" else to_y)

    def pair_terms():
        for i in range(nz - 1):
            src = nearest(z, nz, i)
            net.arrival(got_dp.at[src], tap_slots + src, partner)
        total = got_dp[0]
        for i in range(1, nz):
            total = total + got_dp[i]
        both_parts[...] = total
        sums["pair"] = net.put(both_parts, tap_other, partner)

    def spread_rows():
        sent.pop(("x", 0)).wait_recv()
        sent["low"] = net.put(done(xn, 0), done(xn, 0), to_y)
        sent.pop(("y", 1)).wait_recv()
        sent["high"] = net.put(done(yn, 1), done(yn, 1), to_x)

    def keep_taps():
        sums["pair"].wait_recv()
        grad_taps[:, pl.ds(al(c * tap_width, tap_width), tap_width)] = both_parts[:tap_count]
        theirs = pl.ds(al((1 - c) * tap_width, tap_width), tap_width)
        grad_taps[:, theirs] = tap_other[:tap_count]

    mine_rows = pl.ds(al(c * rows, rows), rows)
    other_rows = pl.ds(al((1 - c) * rows, rows), rows)

    def gather_rows():
        for copy in sent.values():
            copy.wait_recv()
        sums["last"] = net.put(final.at[other_rows], halves, partner)
        grad_weight[:, mine] = final[mine_rows, :].astype(f32)

    def keep():
        sums["last"].wait_recv()
        grad_weight[:, other] = halves[...].astype(f32)

    for step, *at in (
        (tap_from, 1),
        (tap_from, 0),
        (product_own,),
        (conv_quarter, 0),
        (tap_from, 2),
        (conv_quarter, 3),
        (first, 0, 0),
        (first, 0, 1),
        (left_halo,),
        (first, 1, 0),
        (conv_quarter, 1),
        (conv_quarter, 2),
        (first, 1, 1),
        (conv_head, 0),
        (first, 2, 0),
        (conv_head, 1),
        (second, 0, 0),
        (norm, 2),
        (norm, 0),
        (second, 0, 1),
        (norm, 1),
        (norm, 3),
        (first, 2, 1),
        (swap,),
        (second, 1, 0),
        (second, 1, 1),
        (swap_done,),
        (multiply, 0),
        (multiply, 1),
        (product_mate,),
        (send_early, 0),
        (second, 2, 0),
        (second, 2, 1),
        (third, 0, 0),
        (third, 0, 1),
        (third, 1, 0),
        (third, 1, 1),
        (send_early, 1),
        (load, 0),
        (load, 1),
        (multiply, 2),
        (blocks_of, 0),
        (turn_x, 0),
        (turn_y, 0),
        (blocks_of, 1),
        (load, 2),
        (third, 2, 0),
        (multiply, 3),
        (third, 2, 1),
        (send_early, 2),
        (blocks_of, 2),
        (send_early, 3),
        (turn_x, 1),
        (turn_y, 1),
        (back_head,),
        (back, 0),
        (back, 1),
        (back_tiles, 0),
        (hand_on, 0),
        (back_tiles, 1),
        (turn_x, 2),
        (turn_y, 2),
        (back_tiles, 2),
        (send_gain,),
        (add_early,),
        (back_tiles, 3),
        (hand_on, 1),
        (back_tiles, 4),
        (back_tiles, 5),
        (right_halo,),
        (load, 3),
        (back_tail, 0),
        (hand_on, 2),
        (back_tiles, 6),
        (back_tiles, 7),
        (turn_y, 3),
        (turn_x, 3),
        (back_tail, 1),
        (turn_early,),
        (send_terms,),
        (pair_sums,),
        (pair_gain,),
        (hand_on, 3),
        (keep_early,),
        (finish_rows,),
        (add_terms,),
        (line_gain,),
        (spread_rows,),
        (pair_terms,),
        (gather_rows,),
        (keep_gain,),
        (keep_taps,),
        (keep,),
    ):
        step(*at)
    net.finish()


def write_out(*refs):
    held, outs, sems = refs[:5], refs[5:10], refs[10]
    copies = [
        pltpu.make_async_copy(a, b.at[0] if len(b.shape) > len(a.shape) else b, sems.at[i])
        for i, (a, b) in enumerate(zip(held, outs))
    ]
    for copy in copies:
        copy.start()
    for copy in copies:
        copy.wait()


def fused_body(value_half, gate_half, upstream, conv_taps, norm_gain, out_weight):
    f32, bf16 = jnp.float32, jnp.bfloat16
    nsp, ndp = lax.axis_size("sp"), lax.axis_size("dp")
    nz = ndp // 2
    _, length, channels = value_half.shape
    rows = out_weight.shape[0]
    tap_count, width = conv_taps.shape
    halo = (tap_count - 1 + 15) // 16 * 16
    half, share = channels // 2, 2 * rows // nsp
    lead = half // 4
    side, e_side = (half - lead) // 2, lead // 2
    tap_rows = (tap_count + 7) // 8 * 8

    def shape(*dims, dtype=bf16):
        return jax.ShapeDtypeStruct(dims, dtype)

    def vmem(*dims, dtype=bf16):
        return pltpu.VMEM(dims, dtype)

    hbm = pl.BlockSpec(memory_space=pltpu.MemorySpace.HBM)
    remote = 60 + 30 * nz
    results = pl.pallas_call(
        fused,
        out_shape=[
            vmem(length, channels),
            vmem(length, channels),
            vmem(tap_count, width, dtype=f32),
            vmem(1, channels, dtype=f32),
            vmem(rows, channels, dtype=f32),
        ],
        in_specs=[hbm] * 6,
        out_specs=[VMEM] * 5,
        scratch_shapes=[
            vmem(length, channels),
            vmem(length, channels),
            vmem(2 * length, channels),
            vmem(nsp, tap_count, width, dtype=f32),
            vmem(1, channels, dtype=f32),
            vmem(ndp * rows, channels),
            vmem(halo, channels),
            vmem(halo, channels),
            vmem(length + halo, channels, dtype=f32),
            vmem(length, channels, dtype=f32),
            vmem(length, LANES, dtype=f32),
            vmem(2 * length, half),
            vmem(length, channels),
            vmem(nz, 2 * rows, half),
            vmem(nz, 2, share, side),
            vmem(nz, 2, share, side),
            vmem(nz, share, side),
            vmem(nz, share, side),
            vmem(nz, share, half - lead),
            vmem(nz, share, half - lead),
            vmem(2 * rows, half),
            vmem(rows, half),
            vmem(nz, share, side),
            vmem(nz, share, side),
            vmem(nz, 2 * rows, lead),
            vmem(2 * rows, lead),
            vmem(2, share, e_side),
            vmem(2, share, e_side),
            vmem(share, e_side),
            vmem(share, e_side),
            vmem(share, e_side),
            vmem(share, e_side),
            vmem(length, channels, dtype=f32),
            vmem(halo, channels),
            vmem(halo, channels),
            vmem(length + halo, channels, dtype=f32),
            vmem(tap_count, 8, channels, dtype=f32),
            vmem(8, channels, dtype=f32),
            vmem(2, nsp, tap_rows, width // 2, dtype=f32),
            vmem(nsp, tap_rows, width // 2, dtype=f32),
            vmem(nz, tap_rows, width // 2, dtype=f32),
            vmem(tap_rows, width // 2, dtype=f32),
            vmem(tap_rows, width // 2, dtype=f32),
            vmem(tap_rows, width // 2, dtype=f32),
            vmem(nsp, tap_rows, width // 2, dtype=f32),
            vmem(nsp, tap_rows, width // 2, dtype=f32),
            vmem(1, channels, dtype=f32),
            vmem(1, channels, dtype=f32),
            vmem(1, channels, dtype=f32),
            vmem(nsp, 1, channels, dtype=f32),
            vmem(1, channels, dtype=f32),
            vmem(nz, 1, channels, dtype=f32),
            pltpu.SemaphoreType.DMA((remote,)),
            pltpu.SemaphoreType.DMA((remote,)),
            pltpu.SemaphoreType.DMA((8,)),
        ],
        compiler_params=pltpu.CompilerParams(
            collective_id=7, has_side_effects=True, vmem_limit_bytes=58 * 1024 * 1024
        ),
    )(value_half, gate_half, upstream, conv_taps, norm_gain[None], out_weight)
    grad_value, grad_gate, grad_taps, grad_gain, grad_weight = pl.pallas_call(
        write_out,
        out_shape=[
            shape(1, length, channels),
            shape(1, length, channels),
            shape(tap_count, width, dtype=f32),
            shape(1, channels, dtype=f32),
            shape(rows, channels, dtype=f32),
        ],
        in_specs=[VMEM] * 5,
        out_specs=[hbm] * 5,
        scratch_shapes=[pltpu.SemaphoreType.DMA((5,))],
        compiler_params=pltpu.CompilerParams(vmem_limit_bytes=8 * 1024 * 1024),
    )(*results)
    return (grad_value, grad_gate, grad_taps, grad_gain[0], grad_weight)


def solution(mesh):
    tokens = P("dp", "sp", None)
    quarters = mesh.shape["sp"] == 4 and mesh.shape["dp"] == 8
    return jax.shard_map(
        fused_body if quarters else body,
        mesh=mesh,
        in_specs=(tokens, tokens, tokens, P(None, "sp"), P(), P("dp", None)),
        out_specs=(tokens, tokens, P(None, "sp"), P(), P("dp", None)),
        check_vma=False,
    )
```

```python
import functools

import jax
import jax.numpy as jnp
from jax import lax
from jax.experimental import pallas as pl
from jax.experimental.pallas import tpu as pltpu
from jax.sharding import PartitionSpec as P

NORM_EPS = 1e-05
VMEM = pl.BlockSpec(memory_space=pltpu.VMEM)


def when(condition, act):
    if condition is None:
        act()
    else:
        pl.when(condition)(lambda: act())


class Copies:
    def __init__(self, send, recv, local):
        self.send, self.recv, self.local = send, recv, local
        self.n_remote = self.n_local = 0
        self.remote, self.locals = [], []

    def start(self, src, dst, target, sends=None, receives=None):
        i = self.n_remote
        self.n_remote += 1
        copy = pltpu.make_async_remote_copy(
            src_ref=src,
            dst_ref=dst,
            send_sem=self.send.at[i],
            recv_sem=self.recv.at[i],
            device_id=target,
            device_id_type=pl.DeviceIdType.MESH,
        )
        when(sends, copy.start)
        self.remote.append([copy, False, sends, receives])
        return len(self.remote) - 1

    def keep(self, src, dst):
        copy = pltpu.make_async_copy(src, dst, self.local.at[self.n_local])
        self.n_local += 1
        copy.start()
        self.locals.append(copy)

    def arrive(self, i):
        when(self.remote[i][3], self.remote[i][0].wait_recv)
        self.remote[i][1] = True

    def finish(self):
        for copy, arrived, sends, receives in self.remote:
            if not arrived:
                when(receives, copy.wait_recv)
            when(sends, copy.wait_send)
        for copy in self.locals:
            copy.wait()


def greet(axes):
    barrier = pltpu.get_barrier_semaphore()
    count = 0
    for axis in axes:
        n = lax.axis_size(axis)
        me = lax.axis_index(axis)
        for k in range(1, n):
            pl.semaphore_signal(
                barrier,
                inc=1,
                device_id={axis: lax.rem(me + k, n)},
                device_id_type=pl.DeviceIdType.MESH,
            )
            count += 1
    pl.semaphore_wait(barrier, count)


def direct(copies, kind, axis, src, dst):
    n = lax.axis_size(axis)
    me = lax.axis_index(axis)
    if kind == "next" or kind == "prev":
        copies.start(src, dst, {axis: lax.rem(me + (1 if kind == "next" else n - 1), n)})
        return
    if kind == "pair":
        copies.start(src, dst, {axis: me + 1 - 2 * lax.rem(me, 2)})
        return
    if kind == "rows":
        nz, z, c = n // 2, me // 2, lax.rem(me, 2)
        copies.keep(src.at[z], dst.at[z])
        for k in range(1, nz):
            peer = lax.rem(z + k, nz)
            copies.start(src.at[peer], dst.at[z], {axis: 2 * peer + c})
        return
    copies.keep(src.at[me] if kind == "scatter" else src, dst.at[me])
    for k in range(1, n):
        peer = lax.rem(me + k, n)
        copies.start(src.at[peer] if kind == "scatter" else src, dst.at[me], {axis: peer})


def spread_gather(copies, src, dst):
    ns, nz = lax.axis_size("sp"), lax.axis_size("dp") // 2
    s, d = lax.axis_index("sp"), lax.axis_index("dp")
    z, c = d // 2, lax.rem(d, 2)
    partner = {"dp": d + 1 - 2 * c}
    first = [
        copies.start(src.at[s], dst.at[d, s], {"dp": 2 * lax.rem(z + k, nz) + c})
        for k in range(1, nz)
    ]
    yield
    copies.keep(src, dst.at[d])
    copies.start(src, dst.at[d], partner)
    second = {}
    for k in range(1, nz):
        copies.arrive(first[k - 1])
        piece = dst.at[2 * lax.rem(z + nz - k, nz) + c, s]
        for j in range(1, ns):
            second[k, j] = copies.start(piece, piece, {"sp": lax.rem(s + j, ns)})
        copies.start(piece, piece, partner)
    yield
    for k in range(1, nz):
        for j in range(1, ns):
            copies.arrive(second[k, j])
            piece = dst.at[2 * lax.rem(z + nz - k, nz) + c, lax.rem(s + ns - j, ns)]
            copies.start(piece, piece, partner)


def line_gather(copies, src, dst):
    nz = lax.axis_size("dp") // 2
    d = lax.axis_index("dp")
    z, c = d // 2, lax.rem(d, 2)
    partner = {"dp": d + 1 - 2 * c}
    up = {"dp": 2 * lax.rem(z + 1, nz) + c}
    down = {"dp": 2 * lax.rem(z + nz - 1, nz) + c}
    below, above = {}, {}

    def send(k):
        low, high = 2 * lax.rem(z + nz - k, nz) + c, 2 * lax.rem(z + k, nz) + c
        low_src, high_src = (dst.at[low], dst.at[high]) if k else (src, src)
        below[k] = copies.start(
            low_src, dst.at[low], up, jnp.logical_and(z >= k, z < nz - 1), z >= k + 1
        )
        above[k] = copies.start(
            high_src, dst.at[high], down, jnp.logical_and(z + k < nz, z > 0), z + k + 1 < nz
        )

    send(0)
    yield
    copies.keep(src, dst.at[d])
    copies.start(src, dst.at[d], partner)
    for k in range(1, nz):
        copies.arrive(below[k - 1])
        copies.arrive(above[k - 1])
        if k < nz - 1:
            send(k)
        low, high = dst.at[2 * lax.rem(z + nz - k, nz) + c], dst.at[2 * lax.rem(z + k, nz) + c]
        copies.start(low, low, partner, z >= k, z >= k)
        copies.start(high, high, partner, z + k < nz, z + k < nz)
        yield


def run(axes, items, *refs):
    n = len(items)
    copies = Copies(*refs[2 * n :])
    greet(axes)
    waiting = []
    for i, (kind, axis) in enumerate(items):
        src, dst = refs[i], refs[n + i]
        if kind == "spread":
            waiting.append(spread_gather(copies, src, dst))
        elif kind == "line":
            waiting.append(line_gather(copies, src, dst))
        elif kind == "later":
            waiting.append(later(copies, axis, src, dst))
        else:
            direct(copies, kind, axis, src, dst)
    while waiting:
        waiting = [steps for steps in waiting if next(steps, waiting) is None]
    copies.finish()


def later(copies, axis, src, dst):
    yield
    direct(copies, "scatter", axis, src, dst)


def exchange(collective_id, *items):
    ns, nd = lax.axis_size("sp"), lax.axis_size("dp")
    shapes, remote, local = [], 0, 0
    for kind, axis, x in items:
        n = lax.axis_size(axis)
        if kind == "rows":
            shape = x.shape
            remote += n // 2 - 1
            local += 1
        elif kind in ("next", "prev", "pair"):
            shape = x.shape
            remote += 1
        elif kind in ("scatter", "later"):
            shape = x.shape
            remote += n - 1
            local += 1
        else:
            shape = (n,) + x.shape
            local += 1
            if kind == "gather":
                remote += n - 1
            elif kind == "spread":
                remote += (nd // 2 - 1) * 2 * ns + 1
            else:
                remote += (nd // 2 - 1) * 4 + 1
        shapes.append(jax.ShapeDtypeStruct(shape, x.dtype))
    axes = tuple(a for a in ("sp", "dp") if any(axis == a or kind == "spread" for kind, axis, _ in items))
    return pl.pallas_call(
        functools.partial(run, axes, tuple((kind, axis) for kind, axis, _ in items)),
        out_shape=shapes,
        in_specs=[VMEM] * len(items),
        out_specs=[VMEM] * len(items),
        scratch_shapes=[
            pltpu.SemaphoreType.DMA((remote,)),
            pltpu.SemaphoreType.DMA((remote,)),
            pltpu.SemaphoreType.DMA((max(local, 1),)),
        ],
        compiler_params=pltpu.CompilerParams(
            collective_id=collective_id, has_side_effects=True, vmem_limit_bytes=48 * 1024 * 1024
        ),
    )(*[x for _, _, x in items])


def body(value_half, gate_half, upstream, conv_taps, norm_gain, out_weight):
    f32 = jnp.float32
    tap_count = conv_taps.shape[0]
    halo = tap_count - 1
    nsp, ndp = lax.axis_size("sp"), lax.axis_size("dp")
    at_start = lax.axis_index("sp") == 0
    at_end = lax.axis_index("sp") == nsp - 1
    edge = (halo + 15) // 16 * 16

    value = value_half[0].astype(f32)
    gate = gate_half[0].astype(f32)
    length = value.shape[0]
    channels = value.shape[1]
    up = upstream[0]
    rows = out_weight.shape[0]

    tail = (value[length - edge :] * jax.nn.sigmoid(gate[length - edge :])).astype(jnp.bfloat16)
    up_blocks = jnp.swapaxes(up.reshape(length, ndp, rows), 0, 1)
    before, taps = exchange(1, ("next", "sp", tail), ("gather", "sp", conv_taps))
    before = jnp.where(at_start, 0, before)[edge - halo :]
    taps = jnp.swapaxes(taps, 0, 1).reshape(tap_count, channels)
    sig_gate = jax.nn.sigmoid(gate)
    glu = (value * sig_gate).astype(jnp.bfloat16)
    padded = jnp.concatenate([before, glu], axis=0).astype(f32)
    conv = jnp.zeros((length, padded.shape[1]), f32)
    for j in range(tap_count):
        conv = conv + taps[j] * padded[j : j + length]
    conv = conv.astype(jnp.bfloat16).astype(f32)
    mean = jnp.mean(conv, axis=-1, keepdims=True)
    centered = conv - mean
    inv = lax.rsqrt(jnp.mean(centered * centered, axis=-1, keepdims=True) + NORM_EPS)
    normed = centered * inv
    scaled = normed * norm_gain
    sig = jax.nn.sigmoid(scaled)
    activated = (scaled * sig).astype(jnp.bfloat16)

    half = channels // 2
    nz, piece = ndp // 2, rows // nsp
    core = lax.rem(lax.axis_index("dp"), 2)
    by_core = up.reshape(length, nz, 2, nsp, piece)

    def partial(which):
        columns = lax.dynamic_index_in_dim(by_core, which, 2, keepdims=False)
        columns = jnp.swapaxes(columns, 1, 2).reshape(length, nsp * nz * piece)
        return lax.dot_general(
            columns, activated[:, half:], (((0,), (0,)), ((), ())), preferred_element_type=f32
        )

    weight, act_all, up_columns, from_partner = exchange(
        2,
        ("spread", "dp", out_weight.reshape(nsp, rows // nsp, channels)),
        ("line", "dp", activated[:, :half]),
        ("later", "dp", up_blocks),
        ("pair", "dp", partial(1 - core).astype(jnp.bfloat16)),
    )
    weight = weight.reshape(ndp * rows, channels)
    act_all = act_all.reshape(ndp * length, half)
    up_columns = up_columns.reshape(ndp * length, rows)
    owned = lax.dot_general(
        up_columns, act_all, (((0,), (0,)), ((), ())), preferred_element_type=f32
    )
    summed = (partial(core) + from_partner.astype(f32)).astype(jnp.bfloat16)
    summed = summed.reshape(nsp, nz, piece, half)

    grad_act = jnp.dot(up, weight, preferred_element_type=f32)
    grad_scaled = grad_act * sig * (1.0 + scaled * (1.0 - sig))
    gain_part = jnp.sum(grad_scaled * normed, axis=0)
    g = grad_scaled * norm_gain
    grad_conv = inv * (
        g
        - jnp.mean(g, axis=-1, keepdims=True)
        - normed * jnp.mean(g * normed, axis=-1, keepdims=True)
    )
    grad_conv = grad_conv.astype(jnp.bfloat16)
    after, gain_got, owned_got, summed_got = exchange(
        3,
        ("prev", "sp", grad_conv[:edge]),
        ("gather", "sp", gain_part[None]),
        ("scatter", "sp", owned.astype(jnp.bfloat16).reshape(nsp, piece, half)),
        ("scatter", "sp", summed),
    )
    after = jnp.where(at_end, 0, after)[:halo]
    extended = jnp.concatenate([grad_conv, after], axis=0).astype(f32)
    here = grad_conv.astype(f32)
    grad_glu = jnp.zeros_like(here)
    terms = []
    for j in range(tap_count):
        first = halo - j
        grad_glu = grad_glu + taps[j] * extended[first : first + length]
        terms.append(jnp.sum(here * padded[j : j + length], axis=0))
    grad_glu = grad_glu.astype(jnp.bfloat16).astype(f32)
    grad_value = (grad_glu * sig_gate).astype(jnp.bfloat16)
    grad_gate = (grad_glu * value * sig_gate * (1.0 - sig_gate)).astype(jnp.bfloat16)

    width = conv_taps.shape[1]
    tap_blocks = jnp.swapaxes(jnp.stack(terms).reshape(tap_count, nsp, width), 0, 1)
    gain_got, tap_got, low_weight, high_got = exchange(
        4,
        ("gather", "dp", jnp.sum(gain_got, axis=0)),
        ("scatter", "sp", tap_blocks),
        ("gather", "sp", jnp.sum(owned_got.astype(f32), axis=0).astype(jnp.bfloat16)),
        ("rows", "dp", jnp.sum(summed_got.astype(f32), axis=0).astype(jnp.bfloat16)),
    )
    tap_got, high_weight = exchange(
        5,
        ("gather", "dp", jnp.sum(tap_got, axis=0)),
        ("gather", "sp", jnp.sum(high_got.astype(f32), axis=0).astype(jnp.bfloat16)),
    )
    grad_gain = jnp.sum(gain_got, axis=0)[0]
    grad_taps = jnp.sum(tap_got, axis=0)
    grad_weight = jnp.concatenate(
        [low_weight.reshape(rows, half), high_weight.reshape(rows, half)], axis=1
    ).astype(f32)
    return (grad_value[None], grad_gate[None], grad_taps, grad_gain, grad_weight)


BLOCK = 64
LANES = 128


class Net:
    def __init__(self, send, recv, local):
        self.send, self.recv, self.local = send, recv, local
        self.n = self.m = self.sends = 0
        self.free = []
        self.open = []

    def ids(self, count):
        self.n += count
        return self.n - count

    def sender(self):
        if self.free:
            return self.free.pop(0)
        self.sends += 1
        return self.sends - 1

    def put(self, src, dst, to, slot=None, sends=None):
        i = self.sender()
        copy = pltpu.make_async_remote_copy(
            src_ref=src,
            dst_ref=dst,
            send_sem=self.send.at[i],
            recv_sem=self.recv.at[self.ids(1) if slot is None else slot],
            device_id=to,
            device_id_type=pl.DeviceIdType.MESH,
        )
        when(sends, copy.start)
        self.open.append((copy, sends, i))
        return copy

    def arrival(self, ref, slot, to):
        pltpu.make_async_remote_copy(
            src_ref=ref,
            dst_ref=ref,
            send_sem=self.send.at[0],
            recv_sem=self.recv.at[slot],
            device_id=to,
            device_id_type=pl.DeviceIdType.MESH,
        ).wait_recv()

    def load(self, src, dst, here=None):
        copy = pltpu.make_async_copy(src, dst, self.local.at[self.m])
        self.m += 1
        when(here, copy.start)
        return copy if here is None else (copy, here)

    def drain(self, keep=0):
        while len(self.open) > keep:
            copy, sends, i = self.open.pop(0)
            when(sends, copy.wait_send)
            self.free.append(i)


def nearest(z, nz, i):
    low, high = z, nz - 1 - z
    both = 2 * jnp.minimum(low, high)
    away = jnp.where(i < both, i // 2 + 1, i - both // 2 + 1)
    up = jnp.where(i < both, i % 2 == 0, high > low)
    return jnp.where(up, z + away, z - away)


def fused(
    value_hbm, gate_hbm, up_hbm, taps_hbm, gain_hbm, weight_hbm,
    out_value, out_gate, out_taps, out_gain, final,
    grad_value, grad_gate, grad_taps, grad_gain, value, gate, ups, taps, gain, weight, tail, before, padded, conv, scale, acts, act,
    parts, got_x, got_y, got_xy, got_yx, plane, got_z, summed, give_x, give_y,
    got_e, early, e_x, e_y, e_xy, e_yx, e_give_x, e_give_y,
    grad_act, head, after, grads, tap_sums, gain_sum, terms, got_terms, got_dp, row_part, both_parts,
    tap_other, tap_mate, tap_half, gain_row, gain_mate, gain_pair, gain_sp, gain_part, gain_dp,
    send, recv, local,
):
    f32, bf16 = jnp.float32, jnp.bfloat16
    nsp, ndp = lax.axis_size("sp"), lax.axis_size("dp")
    nz = ndp // 2
    s, d = lax.axis_index("sp"), lax.axis_index("dp")
    z, c = d // 2, lax.rem(d, 2)
    xn, yn = s + 1 - 2 * lax.rem(s, 2), lax.rem(s + 2, nsp)
    dg = nsp - 1 - s
    length, channels = value.shape
    halo = before.shape[0]
    tap_count = taps.shape[1]
    width = taps.shape[2]
    rows = weight.shape[0] // ndp
    half = channels // 2
    lead = got_e.shape[2]
    rest = half - lead
    side, e_side = rest // 2, lead // 2
    quarter = channels // nsp
    share = 2 * rows // nsp
    tiles = channels // LANES
    tap_rows, tap_width = terms.shape[2:]
    net = Net(send, recv, local)
    to_x, to_y, to_d, partner = {"sp": xn}, {"sp": yn}, {"sp": dg}, {"dp": d + 1 - 2 * c}

    def at_chip(peer):
        return {"dp": 2 * peer + c}

    def al(i, n):
        return pl.multiple_of(i, n)

    in_up = net.load(up_hbm.at[0], ups.at[pl.ds(0, length)])
    in_weight = net.load(weight_hbm, weight.at[pl.ds(al(d * rows, rows), rows)])
    in_value = net.load(value_hbm.at[0], value)
    in_gate = net.load(gate_hbm.at[0], gate)
    in_taps = net.load(taps_hbm, taps.at[s])
    in_gain = net.load(gain_hbm, gain)

    barrier = pltpu.get_barrier_semaphore()
    cross = [{**to, **partner} for to in (to_x, to_y)]
    peers = [to_x, to_y, to_d, partner] + cross + [at_chip(lax.rem(z + k, nz)) for k in range(1, nz)]
    for peer in peers:
        pl.semaphore_signal(barrier, inc=1, device_id=peer, device_id_type=pl.DeviceIdType.MESH)
    pl.semaphore_wait(barrier, len(peers))

    def piece(owner, q, h):
        r = rows // 2
        return weight.at[
            pl.ds(al(owner * rows + h * r, r), r), pl.ds(al(q * quarter, quarter), quarter)
        ]

    above, below = at_chip(lax.rem(z + 1, nz)), at_chip(lax.rem(z + nz - 1, nz))

    def along(src, h):
        p, slot = piece(2 * src + c, s, h), w_slots + 2 * src + h
        net.put(p, p, above, slot, jnp.logical_and(src <= z, z < nz - 1))
        net.put(p, p, below, slot, jnp.logical_and(src >= z, z > 0))

    in_taps.wait()
    tap_copies = [net.put(taps.at[s], taps.at[s], to) for to in (to_x, to_y, to_d)]
    w_slots = net.ids(2 * nz)
    in_weight.wait()
    for h in range(2):
        along(z, h)

    arrived = {}
    mates = {}

    def first(i, h):
        src = nearest(z, nz, i)
        owner = 2 * src + c
        net.arrival(piece(owner, s, h), w_slots + 2 * src + h, partner)
        along(src, h)
        p = piece(owner, s, h)
        arrived[i, h] = [net.put(p, p, to_x), net.put(p, p, to_y)]
        mates.setdefault(i, []).append(net.put(p, p, partner))

    def second(i, h):
        owner = 2 * nearest(z, nz, i) + c
        from_x, from_y = arrived[i, h]
        px, py = piece(owner, xn, h), piece(owner, yn, h)
        if h == 0:
            from_x.wait_recv()
            arrived[i, h] = net.put(px, px, to_y)
            from_y.wait_recv()
        else:
            from_y.wait_recv()
            arrived[i, h] = net.put(py, py, to_x)
            from_x.wait_recv()
        mates[i] += [net.put(px, px, partner), net.put(py, py, partner)]

    def third(i, h):
        owner = 2 * nearest(z, nz, i) + c
        arrived[i, h].wait_recv()
        p = piece(owner, dg, h)
        mates[i].append(net.put(p, p, partner))

    in_value.wait()
    in_gate.wait()
    v = value[length - halo :, :].astype(f32)
    tail[...] = (v * jax.nn.sigmoid(gate[length - halo :, :].astype(f32))).astype(bf16)

    def glu_rows(i, _):
        r = al(i * 16, 16)
        v = value[pl.ds(r, 16), :].astype(f32)
        g = (v * jax.nn.sigmoid(gate[pl.ds(r, 16), :].astype(f32))).astype(bf16)
        padded[pl.ds(al(r + halo, 8), 16), :] = g.astype(f32)
        return 0

    lax.fori_loop(0, 2, glu_rows, 0)
    left = net.put(tail, before, {"sp": lax.rem(s + 1, nsp)}, None, s < nsp - 1)
    in_up.wait()
    own_rows = weight.at[pl.ds(al(d * rows, rows), rows)]
    own_up = net.put(ups.at[pl.ds(0, length)], ups.at[pl.ds(length, length)], partner)
    own_weight = net.put(own_rows, own_rows, partner)
    lax.fori_loop(2, length // 16, glu_rows, 0)

    def tap_from(n):
        tap_copies[n].wait_recv()

    def left_halo():
        when(s > 0, left.wait_recv)

        @pl.when(s == 0)
        def _():
            before[...] = jnp.zeros_like(before)

        padded[pl.ds(0, halo), :] = before[...].astype(f32)

    per_block = width // LANES

    def tap(t, j):
        q, lane = t // per_block, lax.rem(t, per_block)
        return taps[q, pl.ds(j, 1), pl.ds(al(lane * LANES, LANES), LANES)]

    def turned(window, r):
        return window if r == 0 else pltpu.roll(window, window.shape[0] - r, 0)

    def conv_block(t, i):
        cols = pl.ds(al(t * LANES, LANES), LANES)
        r0 = al(i * BLOCK, BLOCK)
        window = padded[pl.ds(r0, BLOCK + halo), cols]
        total = jnp.zeros((BLOCK, LANES), f32)
        for r in range(8):
            moved = turned(window, r)
            for o in range(r, halo + 1, 8):
                j = o - (halo - tap_count + 1)
                if 0 <= j < tap_count:
                    total = total + tap(t, j) * moved[o - r : o - r + BLOCK]
        conv[pl.ds(r0, BLOCK), cols] = total.astype(bf16).astype(f32)

    row_blocks = length // BLOCK

    def conv_quarter(n):
        q = (s, xn, yn, dg)[n]
        inner = row_blocks - 1

        def one(m, _):
            conv_block(q * per_block + m // inner, 1 + lax.rem(m, inner))
            return 0

        lax.fori_loop(0, per_block * inner, one, 0)

    def conv_head(n):
        def one(t, _):
            conv_block(t, 0)
            return 0

        lax.fori_loop(n * tiles // 2, (n + 1) * tiles // 2, one, 0)

    in_gain.wait()

    def norm_rows(i, _):
        r = al(i * 16, 16)
        rr = pl.ds(r, 16)
        x = conv[rr, :]
        mean = jnp.mean(x, axis=-1, keepdims=True)
        x = x - mean
        inv = lax.rsqrt(jnp.mean(x * x, axis=-1, keepdims=True) + NORM_EPS)
        normed = x * inv
        conv[rr, :] = normed
        scale[rr, :] = jnp.broadcast_to(inv, (16, LANES))
        scaled = normed * gain[...]
        act[rr, :] = (scaled * jax.nn.sigmoid(scaled)).astype(bf16)
        return 0

    blocks = length // 16

    def norm(n):
        lax.fori_loop(n * blocks // 4, (n + 1) * blocks // 4, norm_rows, 0)

    mine = pl.ds(al(c * half, half), half)
    other = pl.ds(al((1 - c) * half, half), half)
    swapped = []

    def swap():
        swapped.append(net.put(act.at[:, other], acts.at[pl.ds(length, length)], partner))
        acts[pl.ds(0, length), :] = act[:, mine]

    def swap_done():
        own_up.wait_recv()
        swapped[0].wait_recv()

    def target(k):
        return nearest(z, nz, nz - 2 - k) if k < nz - 1 else z

    def multiply(k):
        t = target(k)
        step = min(256, 2 * rows)

        def some(m, _):
            u = ups[:, pl.ds(al(t * 2 * rows + m * step, step), step)]
            p = lax.dot_general(u, acts[...], (((0,), (0,)), ((), ())), preferred_element_type=f32)
            parts[k, pl.ds(al(m * step, step), step), :] = p.astype(bf16)
            return 0

        lax.fori_loop(0, 2 * rows // step, some, 0)

    class Plane:
        def __init__(self, src, w, x, y, xy, yx, give_x, give_y):
            self.src, self.w = src, w
            self.x, self.y, self.xy, self.yx = x, y, xy, yx
            self.give_x, self.give_y = give_x, give_y

        def at(self, q, h):
            return pl.ds(al(q * share, share), share), pl.ds(h * self.w, self.w)

        def part(self, q, h):
            return self.src[self.at(q, h)].astype(f32)

        def send(self):
            def unit(q, h):
                return self.src.at[self.at(q, h)]

            self.far_x = net.put(unit(dg, 0), self.x.at[1], to_x)
            self.far_y = net.put(unit(dg, 1), self.y.at[1], to_y)
            self.near_x = net.put(unit(xn, 0), self.x.at[0], to_x)
            self.near_y = net.put(unit(yn, 1), self.y.at[0], to_y)

        def turn_x(self):
            self.far_x.wait_recv()
            self.give_y[...] = (self.part(yn, 0) + self.x[1].astype(f32)).astype(bf16)
            self.last_y = net.put(self.give_y, self.xy, to_y)

        def turn_y(self):
            self.far_y.wait_recv()
            self.give_x[...] = (self.part(xn, 1) + self.y[1].astype(f32)).astype(bf16)
            self.last_x = net.put(self.give_x, self.yx, to_x)

        def total(self):
            for copy in (self.near_x, self.near_y, self.last_x, self.last_y):
                copy.wait_recv()
            low = self.part(s, 0) + self.x[0].astype(f32) + self.xy[...].astype(f32)
            high = self.part(s, 1) + self.y[0].astype(f32) + self.yx[...].astype(f32)
            return low.astype(bf16), high.astype(bf16)

    chunks = [
        Plane(
            parts.at[k], side, got_x.at[k], got_y.at[k], got_xy.at[k], got_yx.at[k],
            give_x.at[k], give_y.at[k],
        )
        for k in range(nz)
    ]
    ahead = Plane(early, e_side, e_x, e_y, e_xy, e_yx, e_give_x, e_give_y)
    z_slots, e_slots = net.ids(nz), net.ids(nz)

    def load(k):
        chunks[k].send()

    def turn_x(k):
        chunks[k].turn_x()

    def turn_y(k):
        chunks[k].turn_y()

    def hand_on(k):
        low, high = chunks[k].total()
        plane[k, :, pl.ds(0, side)] = low
        plane[k, :, pl.ds(side, side)] = high
        if k < nz - 1:
            net.put(plane.at[k], got_z.at[z], at_chip(target(k)), z_slots + z)

    def send_early(k):
        if k < nz - 1:
            tops = parts.at[k, :, pl.ds(rest, lead)]
            net.put(tops, got_e.at[z], at_chip(target(k)), e_slots + z)

    def add_early():
        total = parts[nz - 1, :, pl.ds(rest, lead)].astype(f32)
        for i in range(nz - 1):
            src = nearest(z, nz, i)
            net.arrival(got_e.at[src], e_slots + src, partner)
            total = total + got_e[src].astype(f32)
        early[...] = total.astype(bf16)
        ahead.send()

    def turn_early():
        ahead.turn_x()
        ahead.turn_y()

    written = []

    keeper = s // (nsp // 2)
    same = keeper == c

    class Spread:
        def __init__(self, low, w):
            self.low, self.w, self.slots = low, w, net.ids(14)

        def place(self, q, e, h, count=1):
            r = al(lax.rem(q, nsp // 2) * share, share)
            col = al(e * half + self.low + h * self.w, LANES)
            return pl.ds(r, share), pl.ds(col, count * self.w)

        def send(self):
            def go(h, to, i, count=1):
                src = summed.at[:, pl.ds(self.low + h * self.w, count * self.w)]
                dst = final.at[self.place(s, c, h, count)]
                skip = None if count == 1 else jnp.logical_not(same)
                net.put(src, dst, to, self.slots + 2 * i + c, skip)

            core = {"dp": 2 * z + keeper}
            go(0, {**to_x, **core}, 0)
            go(1, {**to_y, **core}, 3)
            go(0, {**to_y, **core}, 2)
            go(1, {**to_x, **core}, 1)
            go(0, partner, 6, 2)

            src = summed.at[:, pl.ds(self.low, 2 * self.w)]
            written.append(net.load(src, final.at[self.place(s, c, 0, 2)], same))

        def arrive(self, who, q, h, i):
            @pl.when(who)
            def _():
                for e in range(2):
                    net.arrival(final.at[self.place(q, e, h)], self.slots + 2 * i + e, partner)

        def forward(self):
            for who, q, h, near, far, to in (
                (same, xn, 0, 0, 4, to_y),
                (jnp.logical_not(same), yn, 1, 3, 5, to_x),
            ):
                self.arrive(who, q, h, near)
                for e in range(2):
                    piece = final.at[self.place(q, e, h)]
                    net.put(piece, piece, to, self.slots + 2 * far + e, who)

        def gather(self):
            self.arrive(same, xn, 1, 1)
            other = jnp.logical_not(same)
            self.arrive(other, yn, 0, 2)
            self.arrive(other, dg, 0, 4)
            self.arrive(other, dg, 1, 5)

            @pl.when(same)
            def _():
                landed = final.at[self.place(s, 1 - c, 0, 2)]
                net.arrival(landed, self.slots + 12 + 1 - c, partner)

    spread_main, spread_early = Spread(0, side), Spread(rest, e_side)

    def keep_early():
        low, high = ahead.total()
        summed[:, pl.ds(rest, e_side)] = low
        summed[:, pl.ds(rest + e_side, e_side)] = high
        spread_early.send()

    def pass_early():
        spread_early.forward()

    def product(owner, start):
        w = weight[pl.ds(al(owner * rows, rows), rows), :]
        u = ups[pl.ds(0, length), pl.ds(al(owner * rows, rows), rows)]
        p = jnp.dot(u, w, preferred_element_type=f32)
        grad_act[...] = p if start else grad_act[...] + p

    def product_own():
        product(d, True)

    def product_mate():
        own_weight.wait_recv()
        product(d + 1 - 2 * c, False)

    def blocks_of(i):
        assert len(mates[i]) == 8
        for copy in mates[i]:
            copy.wait_recv()
        src = nearest(z, nz, i)

        def one(n, _):
            product(2 * src + n, False)
            return 0

        lax.fori_loop(0, 2, one, 0)

    gain_sum[...] = jnp.zeros_like(gain_sum)

    def back_rows(i, _):
        r = al(i * 16, 16)
        rr = pl.ds(r, 16)
        normed = conv[rr, :]
        scaled = normed * gain[...]
        sig = jax.nn.sigmoid(scaled)
        gs = grad_act[rr, :] * sig * (1.0 + scaled * (1.0 - sig))
        gn = gs * normed
        gain_sum[...] += gn[:8] + gn[8:]
        g = gs * gain[...]
        m1 = jnp.mean(g, axis=-1, keepdims=True)
        m2 = jnp.mean(g * normed, axis=-1, keepdims=True)
        gc = (scale[rr, 0:1] * (g - m1 - normed * m2)).astype(bf16)
        grads[rr, :] = gc.astype(f32)
        return 0

    ready = []

    def back_head():
        lax.fori_loop(0, halo // 16, back_rows, 0)
        head[...] = grads[pl.ds(0, halo), :].astype(bf16)
        ready.append(net.put(head, after, {"sp": lax.rem(s + nsp - 1, nsp)}, None, s > 0))

    def back(n):
        mid = (blocks + halo // 16) // 2
        lax.fori_loop((halo // 16, mid)[n], (mid, blocks)[n], back_rows, 0)

    def right_halo():
        when(s < nsp - 1, ready[0].wait_recv)

        @pl.when(s == nsp - 1)
        def _():
            after[...] = jnp.zeros_like(after)

        grads[pl.ds(length, halo), :] = after[...].astype(f32)

    tap_sums[...] = jnp.zeros_like(tap_sums)

    def back_block(t, i):
        cols = pl.ds(al(t * LANES, LANES), LANES)
        r0 = al(i * BLOCK, BLOCK)
        rr = pl.ds(r0, BLOCK)
        window = grads[pl.ds(r0, BLOCK + halo), cols]
        total = jnp.zeros((BLOCK, LANES), f32)
        for r in range(8):
            moved = turned(window, r)
            for o in range(r, tap_count, 8):
                total = total + tap(t, tap_count - 1 - o) * moved[o - r : o - r + BLOCK]
        gg = total.astype(bf16).astype(f32)
        sg = jax.nn.sigmoid(gate[rr, cols].astype(f32))
        grad_value[rr, cols] = (gg * sg).astype(bf16)
        grad_gate[rr, cols] = (gg * value[rr, cols].astype(f32) * sg * (1.0 - sg)).astype(bf16)
        gc = window[:BLOCK]
        window = padded[pl.ds(r0, BLOCK + halo), cols]
        for r in range(8):
            moved = turned(window, r)
            for o in range(r, halo + 1, 8):
                j = o - (halo - tap_count + 1)
                if 0 <= j < tap_count:
                    term = (gc * moved[o - r : o - r + BLOCK]).reshape(BLOCK // 8, 8, LANES)
                    tap_sums[j, :, cols] += jnp.sum(term, axis=0)

    def back_tiles(n):
        inner = row_blocks - 1

        def one(m, _):
            back_block(m // inner, lax.rem(m, inner))
            return 0

        step = tiles // 8 * inner
        lax.fori_loop(n * step, (n + 1) * step, one, 0)

    def back_tail(n):
        def one(t, _):
            back_block(t, row_blocks - 1)
            cols = pl.ds(al(t * LANES, LANES), LANES)
            q, lane = t // per_block, lax.rem(t, per_block)
            e, lane = lane // (per_block // 2), lax.rem(lane, per_block // 2)
            lanes = pl.ds(al(lane * LANES, LANES), LANES)
            terms[e, q, pl.ds(0, tap_count), lanes] = jnp.sum(tap_sums[:, :, cols], axis=1)
            return 0

        lax.fori_loop(n * tiles // 2, (n + 1) * tiles // 2, one, 0)

    sums = {}

    def send_gain():
        gain_row[...] = jnp.sum(gain_sum[...], axis=0, keepdims=True)
        sums["gain"] = net.put(gain_row, gain_mate, partner)

    def pair_gain():
        sums["gain"].wait_recv()
        gain_pair[...] = gain_row[...] + gain_mate[...]
        gain_sp[s] = gain_pair[...]
        sums["gain"] = [net.put(gain_pair, gain_sp.at[s], to) for to in (to_d, to_x, to_y)]

    gain_slots = net.ids(nz)

    def line_gain():
        for copy in sums["gain"]:
            copy.wait_recv()
        total = gain_sp[0]
        for q in range(1, nsp):
            total = total + gain_sp[q]
        gain_part[...] = total
        gain_dp[z] = total
        for i in range(nz - 1):
            net.put(gain_part, gain_dp.at[z], at_chip(nearest(z, nz, i)), gain_slots + z)

    def keep_gain():
        for i in range(nz - 1):
            src = nearest(z, nz, i)
            net.arrival(gain_dp.at[src], gain_slots + src, partner)
        total = gain_dp[0]
        for i in range(1, nz):
            total = total + gain_dp[i]
        grad_gain[...] = total
        written.append(net.load(grad_gain, out_gain))

    def send_terms():
        sums["mate"] = net.put(terms.at[1 - c], tap_mate, partner)
        written.append(net.load(grad_value, out_value))
        written.append(net.load(grad_gate, out_gate))

    def pair_sums():
        sums["mate"].wait_recv()
        tap_half[...] = terms[c] + tap_mate[...]
        got_terms[s] = tap_half[s]
        sums["sp"] = [
            net.put(tap_half.at[peer], got_terms.at[s], to)
            for peer, to in ((dg, to_d), (xn, to_x), (yn, to_y))
        ]

    tap_slots = net.ids(nz)

    def add_terms():
        for copy in sums["sp"]:
            copy.wait_recv()
        total = got_terms[0]
        for q in range(1, nsp):
            total = total + got_terms[q]
        row_part[...] = total
        got_dp[z] = total
        for i in range(nz - 1):
            net.put(row_part, got_dp.at[z], at_chip(nearest(z, nz, i)), tap_slots + z)

    def finish_rows():
        total = plane[nz - 1].astype(f32)
        for i in range(nz - 1):
            src = nearest(z, nz, i)
            net.arrival(got_z.at[src], z_slots + src, partner)
            total = total + got_z[src].astype(f32)
        summed[:, pl.ds(0, rest)] = total.astype(bf16)
        spread_main.send()

    def pair_terms():
        for i in range(nz - 1):
            src = nearest(z, nz, i)
            net.arrival(got_dp.at[src], tap_slots + src, partner)
        total = got_dp[0]
        for i in range(1, nz):
            total = total + got_dp[i]
        both_parts[...] = total
        sums["pair"] = net.put(both_parts, tap_other, partner)

    def spread_rows():
        spread_main.forward()

    def keep_taps():
        sums["pair"].wait_recv()
        grad_taps[:, pl.ds(al(c * tap_width, tap_width), tap_width)] = both_parts[:tap_count]
        theirs = pl.ds(al((1 - c) * tap_width, tap_width), tap_width)
        grad_taps[:, theirs] = tap_other[:tap_count]
        written.append(net.load(grad_taps, out_taps))

    def gather_rows():
        spread_early.gather()
        spread_main.gather()

    for step, *at in (
        (conv_quarter, 0),
        (tap_from, 0),
        (tap_from, 1),
        (conv_quarter, 2),
        (first, 0, 0),
        (first, 0, 1),
        (tap_from, 2),
        (left_halo,),
        (first, 1, 0),
        (conv_quarter, 3),
        (conv_quarter, 1),
        (first, 1, 1),
        (conv_head, 0),
        (norm, 2),
        (first, 2, 0),
        (norm, 3),
        (second, 0, 0),
        (norm, 1),
        (second, 0, 1),
        (conv_head, 1),
        (product_own,),
        (norm, 0),
        (first, 2, 1),
        (swap,),
        (net.drain, 24),
        (swap_done,),
        (second, 1, 0),
        (net.drain, 24),
        (multiply, 0),
        (second, 1, 1),
        (send_early, 0),
        (second, 2, 0),
        (net.drain, 24),
        (multiply, 3),
        (third, 0, 0),
        (net.drain, 24),
        (multiply, 1),
        (send_early, 3),
        (second, 2, 1),
        (send_early, 1),
        (net.drain, 24),
        (multiply, 2),
        (third, 0, 1),
        (third, 1, 0),
        (load, 0),
        (third, 1, 1),
        (product_mate,),
        (blocks_of, 1),
        (blocks_of, 0),
        (load, 1),
        (third, 2, 0),
        (third, 2, 1),
        (turn_y, 0),
        (blocks_of, 2),
        (send_early, 2),
        (turn_x, 0),
        (net.drain, 24),
        (back_head,),
        (net.drain, 24),
        (back, 0),
        (turn_y, 1),
        (net.drain, 24),
        (back, 1),
        (back_tiles, 0),
        (load, 2),
        (back_tiles, 1),
        (turn_x, 1),
        (net.drain, 24),
        (back_tiles, 2),
        (hand_on, 0),
        (back_tiles, 3),
        (turn_y, 2),
        (net.drain, 24),
        (back_tiles, 4),
        (add_early,),
        (send_gain,),
        (back_tiles, 5),
        (turn_x, 2),
        (load, 3),
        (hand_on, 1),
        (right_halo,),
        (net.drain, 24),
        (back_tiles, 6),
        (back_tiles, 7),
        (back_tail, 0),
        (pair_gain,),
        (hand_on, 2),
        (turn_early,),
        (turn_y, 3),
        (turn_x, 3),
        (back_tail, 1),
        (net.drain, 24),
        (send_terms,),
        (pair_sums,),
        (keep_early,),
        (hand_on, 3),
        (finish_rows,),
        (line_gain,),
        (add_terms,),
        (net.drain, 10),
        (spread_rows,),
        (keep_gain,),
        (pass_early,),
        (pair_terms,),
        (keep_taps,),
        (gather_rows,),
    ):
        step(*at)
    net.drain()
    for copy in written:
        if isinstance(copy, tuple):
            when(copy[1], copy[0].wait)
        else:
            copy.wait()


def write_out(*refs):
    held, outs, wide, sems = refs[:5], refs[5:10], refs[10], refs[11]
    copies = []

    def start(src, dst):
        copies.append(pltpu.make_async_copy(src, dst, sems.at[len(copies)]))
        copies[-1].start()

    for a, b in zip(held[:4], outs):
        start(a, b.at[0] if len(b.shape) > len(a.shape) else b)
    step = wide.shape[0] // 4
    for i in range(4):
        part = pl.ds(i * step, step)
        wide[part, :] = held[4][part, :].astype(wide.dtype)
        start(wide.at[part], outs[4].at[part])
    for copy in copies:
        copy.wait()


def fused_body(value_half, gate_half, upstream, conv_taps, norm_gain, out_weight):
    f32, bf16 = jnp.float32, jnp.bfloat16
    nsp, ndp = lax.axis_size("sp"), lax.axis_size("dp")
    nz = ndp // 2
    _, length, channels = value_half.shape
    rows = out_weight.shape[0]
    tap_count, width = conv_taps.shape
    halo = (tap_count - 1 + 15) // 16 * 16
    half, share = channels // 2, 2 * rows // nsp
    lead = half // 4
    side, e_side = (half - lead) // 2, lead // 2
    tap_rows = (tap_count + 7) // 8 * 8

    def shape(*dims, dtype=bf16):
        return jax.ShapeDtypeStruct(dims, dtype)

    def vmem(*dims, dtype=bf16):
        return pltpu.VMEM(dims, dtype)

    hbm = pl.BlockSpec(memory_space=pltpu.MemorySpace.HBM)
    remote = 31 + 28 * nz
    results = pl.pallas_call(
        fused,
        out_shape=[
            vmem(length, channels),
            vmem(length, channels),
            vmem(tap_count, width, dtype=f32),
            vmem(1, channels, dtype=f32),
            vmem(rows, channels),
        ],
        in_specs=[hbm] * 6,
        out_specs=[pl.BlockSpec(memory_space=pl.ANY)] * 5,
        scratch_shapes=[
            vmem(length, channels),
            vmem(length, channels),
            vmem(tap_count, width, dtype=f32),
            vmem(1, channels, dtype=f32),
            vmem(length, channels),
            vmem(length, channels),
            vmem(2 * length, channels),
            vmem(nsp, tap_count, width, dtype=f32),
            vmem(1, channels, dtype=f32),
            vmem(ndp * rows, channels),
            vmem(halo, channels),
            vmem(halo, channels),
            vmem(length + halo, channels, dtype=f32),
            vmem(length, channels, dtype=f32),
            vmem(length, LANES, dtype=f32),
            vmem(2 * length, half),
            vmem(length, channels),
            vmem(nz, 2 * rows, half),
            vmem(nz, 2, share, side),
            vmem(nz, 2, share, side),
            vmem(nz, share, side),
            vmem(nz, share, side),
            vmem(nz, share, half - lead),
            vmem(nz, share, half - lead),
            vmem(share, half),
            vmem(nz, share, side),
            vmem(nz, share, side),
            vmem(nz, 2 * rows, lead),
            vmem(2 * rows, lead),
            vmem(2, share, e_side),
            vmem(2, share, e_side),
            vmem(share, e_side),
            vmem(share, e_side),
            vmem(share, e_side),
            vmem(share, e_side),
            vmem(length, channels, dtype=f32),
            vmem(halo, channels),
            vmem(halo, channels),
            vmem(length + halo, channels, dtype=f32),
            vmem(tap_count, 8, channels, dtype=f32),
            vmem(8, channels, dtype=f32),
            vmem(2, nsp, tap_rows, width // 2, dtype=f32),
            vmem(nsp, tap_rows, width // 2, dtype=f32),
            vmem(nz, tap_rows, width // 2, dtype=f32),
            vmem(tap_rows, width // 2, dtype=f32),
            vmem(tap_rows, width // 2, dtype=f32),
            vmem(tap_rows, width // 2, dtype=f32),
            vmem(nsp, tap_rows, width // 2, dtype=f32),
            vmem(nsp, tap_rows, width // 2, dtype=f32),
            vmem(1, channels, dtype=f32),
            vmem(1, channels, dtype=f32),
            vmem(1, channels, dtype=f32),
            vmem(nsp, 1, channels, dtype=f32),
            vmem(1, channels, dtype=f32),
            vmem(nz, 1, channels, dtype=f32),
            pltpu.SemaphoreType.DMA((48,)),
            pltpu.SemaphoreType.DMA((remote,)),
            pltpu.SemaphoreType.DMA((12,)),
        ],
        compiler_params=pltpu.CompilerParams(
            collective_id=7, has_side_effects=True, vmem_limit_bytes=58 * 1024 * 1024
        ),
    )(value_half, gate_half, upstream, conv_taps, norm_gain[None], out_weight)
    grad_value, grad_gate, grad_taps, grad_gain, grad_weight = pl.pallas_call(
        write_out,
        out_shape=[
            shape(1, length, channels),
            shape(1, length, channels),
            shape(tap_count, width, dtype=f32),
            shape(1, channels, dtype=f32),
            shape(rows, channels, dtype=f32),
        ],
        in_specs=[pl.BlockSpec(memory_space=pl.ANY)] * 4 + [VMEM],
        out_specs=[hbm] * 5,
        scratch_shapes=[vmem(rows, channels, dtype=f32), pltpu.SemaphoreType.DMA((8,))],
        compiler_params=pltpu.CompilerParams(vmem_limit_bytes=8 * 1024 * 1024),
    )(*results)
    return (grad_value, grad_gate, grad_taps, grad_gain[0], grad_weight)


def solution(mesh):
    tokens = P("dp", "sp", None)
    quarters = mesh.shape["sp"] == 4 and mesh.shape["dp"] == 8
    return jax.shard_map(
        fused_body if quarters else body,
        mesh=mesh,
        in_specs=(tokens, tokens, tokens, P(None, "sp"), P(), P("dp", None)),
        out_specs=(tokens, tokens, P(None, "sp"), P(), P("dp", None)),
        check_vma=False,
    )
```

```python
import functools

import jax
import jax.numpy as jnp
from jax import lax
from jax.experimental import pallas as pl
from jax.experimental.pallas import tpu as pltpu
from jax.sharding import PartitionSpec as P

NORM_EPS = 1e-05
VMEM = pl.BlockSpec(memory_space=pltpu.VMEM)


def when(condition, act):
    if condition is None:
        act()
    else:
        pl.when(condition)(lambda: act())


class Copies:
    def __init__(self, send, recv, local):
        self.send, self.recv, self.local = send, recv, local
        self.n_remote = self.n_local = 0
        self.remote, self.locals = [], []

    def start(self, src, dst, target, sends=None, receives=None):
        i = self.n_remote
        self.n_remote += 1
        copy = pltpu.make_async_remote_copy(
            src_ref=src,
            dst_ref=dst,
            send_sem=self.send.at[i],
            recv_sem=self.recv.at[i],
            device_id=target,
            device_id_type=pl.DeviceIdType.MESH,
        )
        when(sends, copy.start)
        self.remote.append([copy, False, sends, receives])
        return len(self.remote) - 1

    def keep(self, src, dst):
        copy = pltpu.make_async_copy(src, dst, self.local.at[self.n_local])
        self.n_local += 1
        copy.start()
        self.locals.append(copy)

    def arrive(self, i):
        when(self.remote[i][3], self.remote[i][0].wait_recv)
        self.remote[i][1] = True

    def finish(self):
        for copy, arrived, sends, receives in self.remote:
            if not arrived:
                when(receives, copy.wait_recv)
            when(sends, copy.wait_send)
        for copy in self.locals:
            copy.wait()


def greet(axes):
    barrier = pltpu.get_barrier_semaphore()
    count = 0
    for axis in axes:
        n = lax.axis_size(axis)
        me = lax.axis_index(axis)
        for k in range(1, n):
            pl.semaphore_signal(
                barrier,
                inc=1,
                device_id={axis: lax.rem(me + k, n)},
                device_id_type=pl.DeviceIdType.MESH,
            )
            count += 1
    pl.semaphore_wait(barrier, count)


def direct(copies, kind, axis, src, dst):
    n = lax.axis_size(axis)
    me = lax.axis_index(axis)
    if kind == "next" or kind == "prev":
        copies.start(src, dst, {axis: lax.rem(me + (1 if kind == "next" else n - 1), n)})
        return
    if kind == "pair":
        copies.start(src, dst, {axis: me + 1 - 2 * lax.rem(me, 2)})
        return
    if kind == "rows":
        nz, z, c = n // 2, me // 2, lax.rem(me, 2)
        copies.keep(src.at[z], dst.at[z])
        for k in range(1, nz):
            peer = lax.rem(z + k, nz)
            copies.start(src.at[peer], dst.at[z], {axis: 2 * peer + c})
        return
    copies.keep(src.at[me] if kind == "scatter" else src, dst.at[me])
    for k in range(1, n):
        peer = lax.rem(me + k, n)
        copies.start(src.at[peer] if kind == "scatter" else src, dst.at[me], {axis: peer})


def spread_gather(copies, src, dst):
    ns, nz = lax.axis_size("sp"), lax.axis_size("dp") // 2
    s, d = lax.axis_index("sp"), lax.axis_index("dp")
    z, c = d // 2, lax.rem(d, 2)
    partner = {"dp": d + 1 - 2 * c}
    first = [
        copies.start(src.at[s], dst.at[d, s], {"dp": 2 * lax.rem(z + k, nz) + c})
        for k in range(1, nz)
    ]
    yield
    copies.keep(src, dst.at[d])
    copies.start(src, dst.at[d], partner)
    second = {}
    for k in range(1, nz):
        copies.arrive(first[k - 1])
        piece = dst.at[2 * lax.rem(z + nz - k, nz) + c, s]
        for j in range(1, ns):
            second[k, j] = copies.start(piece, piece, {"sp": lax.rem(s + j, ns)})
        copies.start(piece, piece, partner)
    yield
    for k in range(1, nz):
        for j in range(1, ns):
            copies.arrive(second[k, j])
            piece = dst.at[2 * lax.rem(z + nz - k, nz) + c, lax.rem(s + ns - j, ns)]
            copies.start(piece, piece, partner)


def line_gather(copies, src, dst):
    nz = lax.axis_size("dp") // 2
    d = lax.axis_index("dp")
    z, c = d // 2, lax.rem(d, 2)
    partner = {"dp": d + 1 - 2 * c}
    up = {"dp": 2 * lax.rem(z + 1, nz) + c}
    down = {"dp": 2 * lax.rem(z + nz - 1, nz) + c}
    below, above = {}, {}

    def send(k):
        low, high = 2 * lax.rem(z + nz - k, nz) + c, 2 * lax.rem(z + k, nz) + c
        low_src, high_src = (dst.at[low], dst.at[high]) if k else (src, src)
        below[k] = copies.start(
            low_src, dst.at[low], up, jnp.logical_and(z >= k, z < nz - 1), z >= k + 1
        )
        above[k] = copies.start(
            high_src, dst.at[high], down, jnp.logical_and(z + k < nz, z > 0), z + k + 1 < nz
        )

    send(0)
    yield
    copies.keep(src, dst.at[d])
    copies.start(src, dst.at[d], partner)
    for k in range(1, nz):
        copies.arrive(below[k - 1])
        copies.arrive(above[k - 1])
        if k < nz - 1:
            send(k)
        low, high = dst.at[2 * lax.rem(z + nz - k, nz) + c], dst.at[2 * lax.rem(z + k, nz) + c]
        copies.start(low, low, partner, z >= k, z >= k)
        copies.start(high, high, partner, z + k < nz, z + k < nz)
        yield


def run(axes, items, *refs):
    n = len(items)
    copies = Copies(*refs[2 * n :])
    greet(axes)
    waiting = []
    for i, (kind, axis) in enumerate(items):
        src, dst = refs[i], refs[n + i]
        if kind == "spread":
            waiting.append(spread_gather(copies, src, dst))
        elif kind == "line":
            waiting.append(line_gather(copies, src, dst))
        elif kind == "later":
            waiting.append(later(copies, axis, src, dst))
        else:
            direct(copies, kind, axis, src, dst)
    while waiting:
        waiting = [steps for steps in waiting if next(steps, waiting) is None]
    copies.finish()


def later(copies, axis, src, dst):
    yield
    direct(copies, "scatter", axis, src, dst)


def exchange(collective_id, *items):
    ns, nd = lax.axis_size("sp"), lax.axis_size("dp")
    shapes, remote, local = [], 0, 0
    for kind, axis, x in items:
        n = lax.axis_size(axis)
        if kind == "rows":
            shape = x.shape
            remote += n // 2 - 1
            local += 1
        elif kind in ("next", "prev", "pair"):
            shape = x.shape
            remote += 1
        elif kind in ("scatter", "later"):
            shape = x.shape
            remote += n - 1
            local += 1
        else:
            shape = (n,) + x.shape
            local += 1
            if kind == "gather":
                remote += n - 1
            elif kind == "spread":
                remote += (nd // 2 - 1) * 2 * ns + 1
            else:
                remote += (nd // 2 - 1) * 4 + 1
        shapes.append(jax.ShapeDtypeStruct(shape, x.dtype))
    axes = tuple(a for a in ("sp", "dp") if any(axis == a or kind == "spread" for kind, axis, _ in items))
    return pl.pallas_call(
        functools.partial(run, axes, tuple((kind, axis) for kind, axis, _ in items)),
        out_shape=shapes,
        in_specs=[VMEM] * len(items),
        out_specs=[VMEM] * len(items),
        scratch_shapes=[
            pltpu.SemaphoreType.DMA((remote,)),
            pltpu.SemaphoreType.DMA((remote,)),
            pltpu.SemaphoreType.DMA((max(local, 1),)),
        ],
        compiler_params=pltpu.CompilerParams(
            collective_id=collective_id, has_side_effects=True, vmem_limit_bytes=48 * 1024 * 1024
        ),
    )(*[x for _, _, x in items])


def body(value_half, gate_half, upstream, conv_taps, norm_gain, out_weight):
    f32 = jnp.float32
    tap_count = conv_taps.shape[0]
    halo = tap_count - 1
    nsp, ndp = lax.axis_size("sp"), lax.axis_size("dp")
    at_start = lax.axis_index("sp") == 0
    at_end = lax.axis_index("sp") == nsp - 1
    edge = (halo + 15) // 16 * 16

    value = value_half[0].astype(f32)
    gate = gate_half[0].astype(f32)
    length = value.shape[0]
    channels = value.shape[1]
    up = upstream[0]
    rows = out_weight.shape[0]

    tail = (value[length - edge :] * jax.nn.sigmoid(gate[length - edge :])).astype(jnp.bfloat16)
    up_blocks = jnp.swapaxes(up.reshape(length, ndp, rows), 0, 1)
    before, taps = exchange(1, ("next", "sp", tail), ("gather", "sp", conv_taps))
    before = jnp.where(at_start, 0, before)[edge - halo :]
    taps = jnp.swapaxes(taps, 0, 1).reshape(tap_count, channels)
    sig_gate = jax.nn.sigmoid(gate)
    glu = (value * sig_gate).astype(jnp.bfloat16)
    padded = jnp.concatenate([before, glu], axis=0).astype(f32)
    conv = jnp.zeros((length, padded.shape[1]), f32)
    for j in range(tap_count):
        conv = conv + taps[j] * padded[j : j + length]
    conv = conv.astype(jnp.bfloat16).astype(f32)
    mean = jnp.mean(conv, axis=-1, keepdims=True)
    centered = conv - mean
    inv = lax.rsqrt(jnp.mean(centered * centered, axis=-1, keepdims=True) + NORM_EPS)
    normed = centered * inv
    scaled = normed * norm_gain
    sig = jax.nn.sigmoid(scaled)
    activated = (scaled * sig).astype(jnp.bfloat16)

    half = channels // 2
    nz, piece = ndp // 2, rows // nsp
    core = lax.rem(lax.axis_index("dp"), 2)
    by_core = up.reshape(length, nz, 2, nsp, piece)

    def partial(which):
        columns = lax.dynamic_index_in_dim(by_core, which, 2, keepdims=False)
        columns = jnp.swapaxes(columns, 1, 2).reshape(length, nsp * nz * piece)
        return lax.dot_general(
            columns, activated[:, half:], (((0,), (0,)), ((), ())), preferred_element_type=f32
        )

    weight, act_all, up_columns, from_partner = exchange(
        2,
        ("spread", "dp", out_weight.reshape(nsp, rows // nsp, channels)),
        ("line", "dp", activated[:, :half]),
        ("later", "dp", up_blocks),
        ("pair", "dp", partial(1 - core).astype(jnp.bfloat16)),
    )
    weight = weight.reshape(ndp * rows, channels)
    act_all = act_all.reshape(ndp * length, half)
    up_columns = up_columns.reshape(ndp * length, rows)
    owned = lax.dot_general(
        up_columns, act_all, (((0,), (0,)), ((), ())), preferred_element_type=f32
    )
    summed = (partial(core) + from_partner.astype(f32)).astype(jnp.bfloat16)
    summed = summed.reshape(nsp, nz, piece, half)

    grad_act = jnp.dot(up, weight, preferred_element_type=f32)
    grad_scaled = grad_act * sig * (1.0 + scaled * (1.0 - sig))
    gain_part = jnp.sum(grad_scaled * normed, axis=0)
    g = grad_scaled * norm_gain
    grad_conv = inv * (
        g
        - jnp.mean(g, axis=-1, keepdims=True)
        - normed * jnp.mean(g * normed, axis=-1, keepdims=True)
    )
    grad_conv = grad_conv.astype(jnp.bfloat16)
    after, gain_got, owned_got, summed_got = exchange(
        3,
        ("prev", "sp", grad_conv[:edge]),
        ("gather", "sp", gain_part[None]),
        ("scatter", "sp", owned.astype(jnp.bfloat16).reshape(nsp, piece, half)),
        ("scatter", "sp", summed),
    )
    after = jnp.where(at_end, 0, after)[:halo]
    extended = jnp.concatenate([grad_conv, after], axis=0).astype(f32)
    here = grad_conv.astype(f32)
    grad_glu = jnp.zeros_like(here)
    terms = []
    for j in range(tap_count):
        first = halo - j
        grad_glu = grad_glu + taps[j] * extended[first : first + length]
        terms.append(jnp.sum(here * padded[j : j + length], axis=0))
    grad_glu = grad_glu.astype(jnp.bfloat16).astype(f32)
    grad_value = (grad_glu * sig_gate).astype(jnp.bfloat16)
    grad_gate = (grad_glu * value * sig_gate * (1.0 - sig_gate)).astype(jnp.bfloat16)

    width = conv_taps.shape[1]
    tap_blocks = jnp.swapaxes(jnp.stack(terms).reshape(tap_count, nsp, width), 0, 1)
    gain_got, tap_got, low_weight, high_got = exchange(
        4,
        ("gather", "dp", jnp.sum(gain_got, axis=0)),
        ("scatter", "sp", tap_blocks),
        ("gather", "sp", jnp.sum(owned_got.astype(f32), axis=0).astype(jnp.bfloat16)),
        ("rows", "dp", jnp.sum(summed_got.astype(f32), axis=0).astype(jnp.bfloat16)),
    )
    tap_got, high_weight = exchange(
        5,
        ("gather", "dp", jnp.sum(tap_got, axis=0)),
        ("gather", "sp", jnp.sum(high_got.astype(f32), axis=0).astype(jnp.bfloat16)),
    )
    grad_gain = jnp.sum(gain_got, axis=0)[0]
    grad_taps = jnp.sum(tap_got, axis=0)
    grad_weight = jnp.concatenate(
        [low_weight.reshape(rows, half), high_weight.reshape(rows, half)], axis=1
    ).astype(f32)
    return (grad_value[None], grad_gate[None], grad_taps, grad_gain, grad_weight)


BLOCK = 64
LANES = 128


class Net:
    def __init__(self, send, recv, local):
        self.send, self.recv, self.local = send, recv, local
        self.n = self.m = self.sends = 0
        self.free = []
        self.open = []

    def ids(self, count):
        self.n += count
        return self.n - count

    def sender(self):
        if self.free:
            return self.free.pop(0)
        self.sends += 1
        return self.sends - 1

    def put(self, src, dst, to, slot=None, sends=None):
        i = self.sender()
        copy = pltpu.make_async_remote_copy(
            src_ref=src,
            dst_ref=dst,
            send_sem=self.send.at[i],
            recv_sem=self.recv.at[self.ids(1) if slot is None else slot],
            device_id=to,
            device_id_type=pl.DeviceIdType.MESH,
        )
        when(sends, copy.start)
        self.open.append((copy, sends, i))
        return copy

    def arrival(self, ref, slot, to):
        pltpu.make_async_remote_copy(
            src_ref=ref,
            dst_ref=ref,
            send_sem=self.send.at[0],
            recv_sem=self.recv.at[slot],
            device_id=to,
            device_id_type=pl.DeviceIdType.MESH,
        ).wait_recv()

    def load(self, src, dst, here=None):
        copy = pltpu.make_async_copy(src, dst, self.local.at[self.m])
        self.m += 1
        when(here, copy.start)
        return copy if here is None else (copy, here)

    def drain(self, keep=0):
        while len(self.open) > keep:
            copy, sends, i = self.open.pop(0)
            when(sends, copy.wait_send)
            self.free.append(i)


def nearest(z, nz, i):
    low, high = z, nz - 1 - z
    both = 2 * jnp.minimum(low, high)
    away = jnp.where(i < both, i // 2 + 1, i - both // 2 + 1)
    up = jnp.where(i < both, i % 2 == 0, high > low)
    return jnp.where(up, z + away, z - away)


def fused(
    value_hbm, gate_hbm, up_hbm, taps_hbm, gain_hbm, weight_hbm,
    out_value, out_gate, out_taps, out_gain, final,
    grad_value, grad_gate, grad_taps, grad_gain, value, gate, ups, taps, gain, weight, tail, before, padded, conv, scale, acts, act,
    parts, got_x, got_y, got_xy, got_yx, plane, got_z, summed, give_x, give_y,
    got_e, early, e_x, e_y, e_xy, e_yx, e_give_x, e_give_y,
    grad_act, head, after, grads, tap_sums, gain_sum, terms, got_terms, got_dp, row_part, both_parts,
    tap_other, tap_mate, tap_half, gain_row, gain_mate, gain_pair, gain_sp, gain_part, gain_dp,
    send, recv, local,
):
    f32, bf16 = jnp.float32, jnp.bfloat16
    nsp, ndp = lax.axis_size("sp"), lax.axis_size("dp")
    nz = ndp // 2
    s, d = lax.axis_index("sp"), lax.axis_index("dp")
    z, c = d // 2, lax.rem(d, 2)
    xn, yn = s + 1 - 2 * lax.rem(s, 2), lax.rem(s + 2, nsp)
    dg = nsp - 1 - s
    length, channels = value.shape
    halo = before.shape[0]
    tap_count = taps.shape[1]
    width = taps.shape[2]
    rows = weight.shape[0] // ndp
    half = channels // 2
    lead = got_e.shape[2]
    rest = half - lead
    side, e_side = rest // 2, lead // 2
    quarter = channels // nsp
    share = 2 * rows // nsp
    tiles = channels // LANES
    tap_rows, tap_width = terms.shape[2:]
    net = Net(send, recv, local)
    to_x, to_y, to_d, partner = {"sp": xn}, {"sp": yn}, {"sp": dg}, {"dp": d + 1 - 2 * c}

    def at_chip(peer):
        return {"dp": 2 * peer + c}

    def al(i, n):
        return pl.multiple_of(i, n)

    in_up = net.load(up_hbm.at[0], ups.at[pl.ds(0, length)])
    in_weight = net.load(weight_hbm, weight.at[pl.ds(al(d * rows, rows), rows)])
    in_value = net.load(value_hbm.at[0], value)
    in_gate = net.load(gate_hbm.at[0], gate)
    in_taps = net.load(taps_hbm, taps.at[s])
    in_gain = net.load(gain_hbm, gain)

    barrier = pltpu.get_barrier_semaphore()
    cross = [{**to, **partner} for to in (to_x, to_y)]
    peers = [to_x, to_y, to_d, partner] + cross + [at_chip(lax.rem(z + k, nz)) for k in range(1, nz)]
    for peer in peers:
        pl.semaphore_signal(barrier, inc=1, device_id=peer, device_id_type=pl.DeviceIdType.MESH)
    pl.semaphore_wait(barrier, len(peers))

    def piece(owner, q, h):
        r = rows // 2
        return weight.at[
            pl.ds(al(owner * rows + h * r, r), r), pl.ds(al(q * quarter, quarter), quarter)
        ]

    above, below = at_chip(lax.rem(z + 1, nz)), at_chip(lax.rem(z + nz - 1, nz))

    def along(src, h):
        p, slot = piece(2 * src + c, s, h), w_slots + 2 * src + h
        net.put(p, p, above, slot, jnp.logical_and(src <= z, z < nz - 1))
        net.put(p, p, below, slot, jnp.logical_and(src >= z, z > 0))

    in_taps.wait()
    tap_copies = [net.put(taps.at[s], taps.at[s], to) for to in (to_x, to_y, to_d)]
    w_slots = net.ids(2 * nz)
    in_weight.wait()
    for h in range(2):
        along(z, h)

    arrived = {}
    mates = {}

    def first(i, h):
        src = nearest(z, nz, i)
        owner = 2 * src + c
        net.arrival(piece(owner, s, h), w_slots + 2 * src + h, partner)
        along(src, h)
        p = piece(owner, s, h)
        arrived[i, h] = [net.put(p, p, to_x), net.put(p, p, to_y)]
        mates.setdefault(i, []).append(net.put(p, p, partner))

    def second(i, h):
        owner = 2 * nearest(z, nz, i) + c
        from_x, from_y = arrived[i, h]
        px, py = piece(owner, xn, h), piece(owner, yn, h)
        if h == 0:
            from_x.wait_recv()
            arrived[i, h] = net.put(px, px, to_y)
            from_y.wait_recv()
        else:
            from_y.wait_recv()
            arrived[i, h] = net.put(py, py, to_x)
            from_x.wait_recv()
        mates[i] += [net.put(px, px, partner), net.put(py, py, partner)]

    def third(i, h):
        owner = 2 * nearest(z, nz, i) + c
        arrived[i, h].wait_recv()
        p = piece(owner, dg, h)
        mates[i].append(net.put(p, p, partner))

    in_value.wait()
    in_gate.wait()
    v = value[length - halo :, :].astype(f32)
    tail[...] = (v * jax.nn.sigmoid(gate[length - halo :, :].astype(f32))).astype(bf16)

    def glu_rows(i, _):
        r = al(i * 16, 16)
        v = value[pl.ds(r, 16), :].astype(f32)
        g = (v * jax.nn.sigmoid(gate[pl.ds(r, 16), :].astype(f32))).astype(bf16)
        padded[pl.ds(al(r + halo, 8), 16), :] = g.astype(f32)
        return 0

    lax.fori_loop(0, 2, glu_rows, 0)
    left = net.put(tail, before, {"sp": lax.rem(s + 1, nsp)}, None, s < nsp - 1)
    in_up.wait()
    own_rows = weight.at[pl.ds(al(d * rows, rows), rows)]
    own_up = net.put(ups.at[pl.ds(0, length)], ups.at[pl.ds(length, length)], partner)
    own_weight = net.put(own_rows, own_rows, partner)
    lax.fori_loop(2, length // 16, glu_rows, 0)

    def tap_from(n):
        tap_copies[n].wait_recv()

    def left_halo():
        when(s > 0, left.wait_recv)

        @pl.when(s == 0)
        def _():
            before[...] = jnp.zeros_like(before)

        padded[pl.ds(0, halo), :] = before[...].astype(f32)

    per_block = width // LANES

    def tap(t, j):
        q, lane = t // per_block, lax.rem(t, per_block)
        return taps[q, pl.ds(j, 1), pl.ds(al(lane * LANES, LANES), LANES)]

    def turned(window, r):
        return window if r == 0 else pltpu.roll(window, window.shape[0] - r, 0)

    def conv_block(t, i):
        cols = pl.ds(al(t * LANES, LANES), LANES)
        r0 = al(i * BLOCK, BLOCK)
        window = padded[pl.ds(r0, BLOCK + halo), cols]
        total = jnp.zeros((BLOCK, LANES), f32)
        for r in range(8):
            moved = turned(window, r)
            for o in range(r, halo + 1, 8):
                j = o - (halo - tap_count + 1)
                if 0 <= j < tap_count:
                    total = total + tap(t, j) * moved[o - r : o - r + BLOCK]
        conv[pl.ds(r0, BLOCK), cols] = total.astype(bf16).astype(f32)

    row_blocks = length // BLOCK

    def conv_quarter(n):
        q = (s, xn, yn, dg)[n]
        inner = row_blocks - 1

        def one(m, _):
            conv_block(q * per_block + m // inner, 1 + lax.rem(m, inner))
            return 0

        lax.fori_loop(0, per_block * inner, one, 0)

    def conv_head(n):
        def one(t, _):
            conv_block(t, 0)
            return 0

        lax.fori_loop(n * tiles // 2, (n + 1) * tiles // 2, one, 0)

    in_gain.wait()

    def norm_rows(i, _):
        r = al(i * 16, 16)
        rr = pl.ds(r, 16)
        x = conv[rr, :]
        mean = jnp.mean(x, axis=-1, keepdims=True)
        x = x - mean
        inv = lax.rsqrt(jnp.mean(x * x, axis=-1, keepdims=True) + NORM_EPS)
        normed = x * inv
        conv[rr, :] = normed
        scale[rr, :] = jnp.broadcast_to(inv, (16, LANES))
        scaled = normed * gain[...]
        act[rr, :] = (scaled * jax.nn.sigmoid(scaled)).astype(bf16)
        return 0

    blocks = length // 16

    def norm(n):
        lax.fori_loop(n * blocks // 4, (n + 1) * blocks // 4, norm_rows, 0)

    mine = pl.ds(al(c * half, half), half)
    other = pl.ds(al((1 - c) * half, half), half)
    swapped = []

    def swap():
        swapped.append(net.put(act.at[:, other], acts.at[pl.ds(length, length)], partner))
        acts[pl.ds(0, length), :] = act[:, mine]

    def swap_done():
        own_up.wait_recv()
        swapped[0].wait_recv()

    def target(k):
        return nearest(z, nz, nz - 2 - k) if k < nz - 1 else z

    def multiply(k):
        t = target(k)
        step = min(256, 2 * rows)

        def some(m, _):
            u = ups[:, pl.ds(al(t * 2 * rows + m * step, step), step)]
            p = lax.dot_general(u, acts[...], (((0,), (0,)), ((), ())), preferred_element_type=f32)
            parts[k, pl.ds(al(m * step, step), step), :] = p.astype(bf16)
            return 0

        lax.fori_loop(0, 2 * rows // step, some, 0)

    class Plane:
        def __init__(self, src, w, x, y, xy, yx, give_x, give_y):
            self.src, self.w = src, w
            self.x, self.y, self.xy, self.yx = x, y, xy, yx
            self.give_x, self.give_y = give_x, give_y

        def at(self, q, h):
            return pl.ds(al(q * share, share), share), pl.ds(h * self.w, self.w)

        def part(self, q, h):
            return self.src[self.at(q, h)].astype(f32)

        def send(self):
            def unit(q, h):
                return self.src.at[self.at(q, h)]

            self.far_x = net.put(unit(dg, 0), self.x.at[1], to_x)
            self.far_y = net.put(unit(dg, 1), self.y.at[1], to_y)
            self.near_x = net.put(unit(xn, 0), self.x.at[0], to_x)
            self.near_y = net.put(unit(yn, 1), self.y.at[0], to_y)

        def turn_x(self):
            self.far_x.wait_recv()
            self.give_y[...] = (self.part(yn, 0) + self.x[1].astype(f32)).astype(bf16)
            self.last_y = net.put(self.give_y, self.xy, to_y)

        def turn_y(self):
            self.far_y.wait_recv()
            self.give_x[...] = (self.part(xn, 1) + self.y[1].astype(f32)).astype(bf16)
            self.last_x = net.put(self.give_x, self.yx, to_x)

        def total(self):
            for copy in (self.near_x, self.near_y, self.last_x, self.last_y):
                copy.wait_recv()
            low = self.part(s, 0) + self.x[0].astype(f32) + self.xy[...].astype(f32)
            high = self.part(s, 1) + self.y[0].astype(f32) + self.yx[...].astype(f32)
            return low.astype(bf16), high.astype(bf16)

    chunks = [
        Plane(
            parts.at[k], side, got_x.at[k], got_y.at[k], got_xy.at[k], got_yx.at[k],
            give_x.at[k], give_y.at[k],
        )
        for k in range(nz)
    ]
    ahead = Plane(early, e_side, e_x, e_y, e_xy, e_yx, e_give_x, e_give_y)
    z_slots, e_slots = net.ids(nz), net.ids(nz)

    def load(k):
        chunks[k].send()

    def turn_x(k):
        chunks[k].turn_x()

    def turn_y(k):
        chunks[k].turn_y()

    def hand_on(k):
        low, high = chunks[k].total()
        plane[k, :, pl.ds(0, side)] = low
        plane[k, :, pl.ds(side, side)] = high
        if k < nz - 1:
            net.put(plane.at[k], got_z.at[z], at_chip(target(k)), z_slots + z)

    def send_early(k):
        if k < nz - 1:
            tops = parts.at[k, :, pl.ds(rest, lead)]
            net.put(tops, got_e.at[z], at_chip(target(k)), e_slots + z)

    def add_early():
        total = parts[nz - 1, :, pl.ds(rest, lead)].astype(f32)
        for i in range(nz - 1):
            src = nearest(z, nz, i)
            net.arrival(got_e.at[src], e_slots + src, partner)
            total = total + got_e[src].astype(f32)
        early[...] = total.astype(bf16)
        ahead.send()

    def turn_early():
        ahead.turn_x()
        ahead.turn_y()

    written = []

    keeper = s // (nsp // 2)
    same = keeper == c

    class Spread:
        def __init__(self, low, w):
            self.low, self.w, self.slots = low, w, net.ids(14)

        def place(self, q, e, h, count=1):
            r = al(lax.rem(q, nsp // 2) * share, share)
            col = al(e * half + self.low + h * self.w, LANES)
            return pl.ds(r, share), pl.ds(col, count * self.w)

        def send(self):
            def go(h, to, i, count=1):
                src = summed.at[:, pl.ds(self.low + h * self.w, count * self.w)]
                dst = final.at[self.place(s, c, h, count)]
                skip = None if count == 1 else jnp.logical_not(same)
                net.put(src, dst, to, self.slots + 2 * i + c, skip)

            core = {"dp": 2 * z + keeper}
            go(0, {**to_x, **core}, 0)
            go(1, {**to_y, **core}, 3)
            go(0, {**to_y, **core}, 2)
            go(1, {**to_x, **core}, 1)
            go(0, partner, 6, 2)

            src = summed.at[:, pl.ds(self.low, 2 * self.w)]
            written.append(net.load(src, final.at[self.place(s, c, 0, 2)], same))

        def arrive(self, who, q, h, i):
            @pl.when(who)
            def _():
                for e in range(2):
                    net.arrival(final.at[self.place(q, e, h)], self.slots + 2 * i + e, partner)

        def forward(self):
            for who, q, h, near, far, to in (
                (same, xn, 0, 0, 4, to_y),
                (jnp.logical_not(same), yn, 1, 3, 5, to_x),
            ):
                self.arrive(who, q, h, near)
                for e in range(2):
                    piece = final.at[self.place(q, e, h)]
                    net.put(piece, piece, to, self.slots + 2 * far + e, who)

        def gather(self):
            self.arrive(same, xn, 1, 1)
            other = jnp.logical_not(same)
            self.arrive(other, yn, 0, 2)
            self.arrive(other, dg, 0, 4)
            self.arrive(other, dg, 1, 5)

            @pl.when(same)
            def _():
                landed = final.at[self.place(s, 1 - c, 0, 2)]
                net.arrival(landed, self.slots + 12 + 1 - c, partner)

    spread_main, spread_early = Spread(0, side), Spread(rest, e_side)

    def keep_early():
        low, high = ahead.total()
        summed[:, pl.ds(rest, e_side)] = low
        summed[:, pl.ds(rest + e_side, e_side)] = high
        spread_early.send()

    def pass_early():
        spread_early.forward()

    def product(owner, start):
        w = weight[pl.ds(al(owner * rows, rows), rows), :]
        u = ups[pl.ds(0, length), pl.ds(al(owner * rows, rows), rows)]
        p = jnp.dot(u, w, preferred_element_type=f32)
        grad_act[...] = p if start else grad_act[...] + p

    def product_own():
        product(d, True)

    def product_mate():
        own_weight.wait_recv()
        product(d + 1 - 2 * c, False)

    def blocks_of(i):
        assert len(mates[i]) == 8
        for copy in mates[i]:
            copy.wait_recv()
        src = nearest(z, nz, i)

        def one(n, _):
            product(2 * src + n, False)
            return 0

        lax.fori_loop(0, 2, one, 0)

    gain_sum[...] = jnp.zeros_like(gain_sum)

    def back_rows(i, _):
        r = al(i * 16, 16)
        rr = pl.ds(r, 16)
        normed = conv[rr, :]
        scaled = normed * gain[...]
        sig = jax.nn.sigmoid(scaled)
        gs = grad_act[rr, :] * sig * (1.0 + scaled * (1.0 - sig))
        gn = gs * normed
        gain_sum[...] += gn[:8] + gn[8:]
        g = gs * gain[...]
        m1 = jnp.mean(g, axis=-1, keepdims=True)
        m2 = jnp.mean(g * normed, axis=-1, keepdims=True)
        gc = (scale[rr, 0:1] * (g - m1 - normed * m2)).astype(bf16)
        grads[rr, :] = gc.astype(f32)
        return 0

    ready = []

    def back_head():
        lax.fori_loop(0, halo // 16, back_rows, 0)
        head[...] = grads[pl.ds(0, halo), :].astype(bf16)
        ready.append(net.put(head, after, {"sp": lax.rem(s + nsp - 1, nsp)}, None, s > 0))

    def back(n):
        mid = (blocks + halo // 16) // 2
        lax.fori_loop((halo // 16, mid)[n], (mid, blocks)[n], back_rows, 0)

    def right_halo():
        when(s < nsp - 1, ready[0].wait_recv)

        @pl.when(s == nsp - 1)
        def _():
            after[...] = jnp.zeros_like(after)

        grads[pl.ds(length, halo), :] = after[...].astype(f32)

    tap_sums[...] = jnp.zeros_like(tap_sums)

    def back_block(t, i):
        cols = pl.ds(al(t * LANES, LANES), LANES)
        r0 = al(i * BLOCK, BLOCK)
        rr = pl.ds(r0, BLOCK)
        window = grads[pl.ds(r0, BLOCK + halo), cols]
        total = jnp.zeros((BLOCK, LANES), f32)
        for r in range(8):
            moved = turned(window, r)
            for o in range(r, tap_count, 8):
                total = total + tap(t, tap_count - 1 - o) * moved[o - r : o - r + BLOCK]
        gg = total.astype(bf16).astype(f32)
        sg = jax.nn.sigmoid(gate[rr, cols].astype(f32))
        grad_value[rr, cols] = (gg * sg).astype(bf16)
        grad_gate[rr, cols] = (gg * value[rr, cols].astype(f32) * sg * (1.0 - sg)).astype(bf16)
        gc = window[:BLOCK]
        window = padded[pl.ds(r0, BLOCK + halo), cols]
        for r in range(8):
            moved = turned(window, r)
            for o in range(r, halo + 1, 8):
                j = o - (halo - tap_count + 1)
                if 0 <= j < tap_count:
                    term = (gc * moved[o - r : o - r + BLOCK]).reshape(BLOCK // 8, 8, LANES)
                    tap_sums[j, :, cols] += jnp.sum(term, axis=0)

    def back_tiles(n):
        inner = row_blocks - 1

        def one(m, _):
            back_block(m // inner, lax.rem(m, inner))
            return 0

        step = tiles // 8 * inner
        lax.fori_loop(n * step, (n + 1) * step, one, 0)

    def back_tail(n):
        def one(t, _):
            back_block(t, row_blocks - 1)
            cols = pl.ds(al(t * LANES, LANES), LANES)
            q, lane = t // per_block, lax.rem(t, per_block)
            e, lane = lane // (per_block // 2), lax.rem(lane, per_block // 2)
            lanes = pl.ds(al(lane * LANES, LANES), LANES)
            terms[e, q, pl.ds(0, tap_count), lanes] = jnp.sum(tap_sums[:, :, cols], axis=1)
            return 0

        lax.fori_loop(n * tiles // 2, (n + 1) * tiles // 2, one, 0)

    sums = {}

    def send_gain():
        gain_row[...] = jnp.sum(gain_sum[...], axis=0, keepdims=True)
        sums["gain"] = net.put(gain_row, gain_mate, partner)

    def pair_gain():
        sums["gain"].wait_recv()
        gain_pair[...] = gain_row[...] + gain_mate[...]
        gain_sp[s] = gain_pair[...]
        sums["gain"] = [net.put(gain_pair, gain_sp.at[s], to) for to in (to_d, to_x, to_y)]

    gain_slots = net.ids(nz)

    def line_gain():
        for copy in sums["gain"]:
            copy.wait_recv()
        total = gain_sp[0]
        for q in range(1, nsp):
            total = total + gain_sp[q]
        gain_part[...] = total
        gain_dp[z] = total
        for i in range(nz - 1):
            net.put(gain_part, gain_dp.at[z], at_chip(nearest(z, nz, i)), gain_slots + z)

    def keep_gain():
        for i in range(nz - 1):
            src = nearest(z, nz, i)
            net.arrival(gain_dp.at[src], gain_slots + src, partner)
        total = gain_dp[0]
        for i in range(1, nz):
            total = total + gain_dp[i]
        grad_gain[...] = total
        written.append(net.load(grad_gain, out_gain))

    def send_terms():
        sums["mate"] = net.put(terms.at[1 - c], tap_mate, partner)
        written.append(net.load(grad_value, out_value))
        written.append(net.load(grad_gate, out_gate))

    def pair_sums():
        sums["mate"].wait_recv()
        tap_half[...] = terms[c] + tap_mate[...]
        got_terms[s] = tap_half[s]
        sums["sp"] = [
            net.put(tap_half.at[peer], got_terms.at[s], to)
            for peer, to in ((dg, to_d), (xn, to_x), (yn, to_y))
        ]

    tap_slots = net.ids(nz)

    def add_terms():
        for copy in sums["sp"]:
            copy.wait_recv()
        total = got_terms[0]
        for q in range(1, nsp):
            total = total + got_terms[q]
        row_part[...] = total
        got_dp[z] = total
        for i in range(nz - 1):
            net.put(row_part, got_dp.at[z], at_chip(nearest(z, nz, i)), tap_slots + z)

    def finish_rows():
        total = plane[nz - 1].astype(f32)
        for i in range(nz - 1):
            src = nearest(z, nz, i)
            net.arrival(got_z.at[src], z_slots + src, partner)
            total = total + got_z[src].astype(f32)
        summed[:, pl.ds(0, rest)] = total.astype(bf16)
        spread_main.send()

    def pair_terms():
        for i in range(nz - 1):
            src = nearest(z, nz, i)
            net.arrival(got_dp.at[src], tap_slots + src, partner)
        total = got_dp[0]
        for i in range(1, nz):
            total = total + got_dp[i]
        both_parts[...] = total
        sums["pair"] = net.put(both_parts, tap_other, partner)

    def spread_rows():
        spread_main.forward()

    def keep_taps():
        sums["pair"].wait_recv()
        grad_taps[:, pl.ds(al(c * tap_width, tap_width), tap_width)] = both_parts[:tap_count]
        theirs = pl.ds(al((1 - c) * tap_width, tap_width), tap_width)
        grad_taps[:, theirs] = tap_other[:tap_count]
        written.append(net.load(grad_taps, out_taps))

    def gather_rows():
        spread_early.gather()
        spread_main.gather()

    for step, *at in (
        (conv_quarter, 0),
        (tap_from, 1),
        (conv_quarter, 2),
        (tap_from, 0),
        (first, 0, 0),
        (first, 0, 1),
        (tap_from, 2),
        (left_halo,),
        (first, 1, 0),
        (conv_quarter, 3),
        (conv_quarter, 1),
        (first, 1, 1),
        (conv_head, 0),
        (norm, 2),
        (norm, 1),
        (first, 2, 0),
        (norm, 3),
        (second, 0, 0),
        (second, 0, 1),
        (conv_head, 1),
        (product_own,),
        (norm, 0),
        (first, 2, 1),
        (swap,),
        (net.drain, 24),
        (swap_done,),
        (second, 1, 0),
        (net.drain, 24),
        (multiply, 1),
        (net.drain, 24),
        (multiply, 0),
        (send_early, 0),
        (second, 1, 1),
        (second, 2, 0),
        (net.drain, 24),
        (multiply, 3),
        (third, 0, 0),
        (send_early, 3),
        (second, 2, 1),
        (send_early, 1),
        (net.drain, 24),
        (multiply, 2),
        (third, 0, 1),
        (third, 1, 0),
        (load, 0),
        (third, 1, 1),
        (product_mate,),
        (blocks_of, 1),
        (blocks_of, 0),
        (load, 1),
        (third, 2, 0),
        (third, 2, 1),
        (turn_y, 0),
        (blocks_of, 2),
        (send_early, 2),
        (turn_x, 0),
        (net.drain, 24),
        (back_head,),
        (net.drain, 24),
        (back, 0),
        (turn_y, 1),
        (net.drain, 24),
        (back, 1),
        (back_tiles, 0),
        (load, 2),
        (back_tiles, 1),
        (turn_x, 1),
        (net.drain, 24),
        (back_tiles, 2),
        (hand_on, 0),
        (back_tiles, 3),
        (turn_y, 2),
        (net.drain, 24),
        (back_tiles, 4),
        (add_early,),
        (send_gain,),
        (back_tiles, 5),
        (turn_x, 2),
        (load, 3),
        (hand_on, 1),
        (right_halo,),
        (net.drain, 24),
        (back_tiles, 6),
        (back_tiles, 7),
        (back_tail, 0),
        (pair_gain,),
        (hand_on, 2),
        (turn_early,),
        (turn_y, 3),
        (turn_x, 3),
        (back_tail, 1),
        (net.drain, 24),
        (send_terms,),
        (pair_sums,),
        (keep_early,),
        (hand_on, 3),
        (finish_rows,),
        (line_gain,),
        (add_terms,),
        (net.drain, 10),
        (spread_rows,),
        (keep_gain,),
        (pass_early,),
        (pair_terms,),
        (keep_taps,),
        (gather_rows,),
    ):
        step(*at)
    net.drain()
    for copy in written:
        if isinstance(copy, tuple):
            when(copy[1], copy[0].wait)
        else:
            copy.wait()


def write_out(*refs):
    held, outs, wide, sems = refs[:5], refs[5:10], refs[10], refs[11]
    copies = []

    def start(src, dst):
        copies.append(pltpu.make_async_copy(src, dst, sems.at[len(copies)]))
        copies[-1].start()

    for a, b in zip(held[:4], outs):
        start(a, b.at[0] if len(b.shape) > len(a.shape) else b)
    step = wide.shape[0] // 4
    for i in range(4):
        part = pl.ds(i * step, step)
        wide[part, :] = held[4][part, :].astype(wide.dtype)
        start(wide.at[part], outs[4].at[part])
    for copy in copies:
        copy.wait()


def fused_body(value_half, gate_half, upstream, conv_taps, norm_gain, out_weight):
    f32, bf16 = jnp.float32, jnp.bfloat16
    nsp, ndp = lax.axis_size("sp"), lax.axis_size("dp")
    nz = ndp // 2
    _, length, channels = value_half.shape
    rows = out_weight.shape[0]
    tap_count, width = conv_taps.shape
    halo = (tap_count - 1 + 15) // 16 * 16
    half, share = channels // 2, 2 * rows // nsp
    lead = half // 4
    side, e_side = (half - lead) // 2, lead // 2
    tap_rows = (tap_count + 7) // 8 * 8

    def shape(*dims, dtype=bf16):
        return jax.ShapeDtypeStruct(dims, dtype)

    def vmem(*dims, dtype=bf16):
        return pltpu.VMEM(dims, dtype)

    hbm = pl.BlockSpec(memory_space=pltpu.MemorySpace.HBM)
    remote = 31 + 28 * nz
    results = pl.pallas_call(
        fused,
        out_shape=[
            vmem(length, channels),
            vmem(length, channels),
            vmem(tap_count, width, dtype=f32),
            vmem(1, channels, dtype=f32),
            vmem(rows, channels),
        ],
        in_specs=[hbm] * 6,
        out_specs=[pl.BlockSpec(memory_space=pl.ANY)] * 5,
        scratch_shapes=[
            vmem(length, channels),
            vmem(length, channels),
            vmem(tap_count, width, dtype=f32),
            vmem(1, channels, dtype=f32),
            vmem(length, channels),
            vmem(length, channels),
            vmem(2 * length, channels),
            vmem(nsp, tap_count, width, dtype=f32),
            vmem(1, channels, dtype=f32),
            vmem(ndp * rows, channels),
            vmem(halo, channels),
            vmem(halo, channels),
            vmem(length + halo, channels, dtype=f32),
            vmem(length, channels, dtype=f32),
            vmem(length, LANES, dtype=f32),
            vmem(2 * length, half),
            vmem(length, channels),
            vmem(nz, 2 * rows, half),
            vmem(nz, 2, share, side),
            vmem(nz, 2, share, side),
            vmem(nz, share, side),
            vmem(nz, share, side),
            vmem(nz, share, half - lead),
            vmem(nz, share, half - lead),
            vmem(share, half),
            vmem(nz, share, side),
            vmem(nz, share, side),
            vmem(nz, 2 * rows, lead),
            vmem(2 * rows, lead),
            vmem(2, share, e_side),
            vmem(2, share, e_side),
            vmem(share, e_side),
            vmem(share, e_side),
            vmem(share, e_side),
            vmem(share, e_side),
            vmem(length, channels, dtype=f32),
            vmem(halo, channels),
            vmem(halo, channels),
            vmem(length + halo, channels, dtype=f32),
            vmem(tap_count, 8, channels, dtype=f32),
            vmem(8, channels, dtype=f32),
            vmem(2, nsp, tap_rows, width // 2, dtype=f32),
            vmem(nsp, tap_rows, width // 2, dtype=f32),
            vmem(nz, tap_rows, width // 2, dtype=f32),
            vmem(tap_rows, width // 2, dtype=f32),
            vmem(tap_rows, width // 2, dtype=f32),
            vmem(tap_rows, width // 2, dtype=f32),
            vmem(nsp, tap_rows, width // 2, dtype=f32),
            vmem(nsp, tap_rows, width // 2, dtype=f32),
            vmem(1, channels, dtype=f32),
            vmem(1, channels, dtype=f32),
            vmem(1, channels, dtype=f32),
            vmem(nsp, 1, channels, dtype=f32),
            vmem(1, channels, dtype=f32),
            vmem(nz, 1, channels, dtype=f32),
            pltpu.SemaphoreType.DMA((48,)),
            pltpu.SemaphoreType.DMA((remote,)),
            pltpu.SemaphoreType.DMA((12,)),
        ],
        compiler_params=pltpu.CompilerParams(
            collective_id=7, has_side_effects=True, vmem_limit_bytes=58 * 1024 * 1024
        ),
    )(value_half, gate_half, upstream, conv_taps, norm_gain[None], out_weight)
    grad_value, grad_gate, grad_taps, grad_gain, grad_weight = pl.pallas_call(
        write_out,
        out_shape=[
            shape(1, length, channels),
            shape(1, length, channels),
            shape(tap_count, width, dtype=f32),
            shape(1, channels, dtype=f32),
            shape(rows, channels, dtype=f32),
        ],
        in_specs=[pl.BlockSpec(memory_space=pl.ANY)] * 4 + [VMEM],
        out_specs=[hbm] * 5,
        scratch_shapes=[vmem(rows, channels, dtype=f32), pltpu.SemaphoreType.DMA((8,))],
        compiler_params=pltpu.CompilerParams(vmem_limit_bytes=8 * 1024 * 1024),
    )(*results)
    return (grad_value, grad_gate, grad_taps, grad_gain[0], grad_weight)


def solution(mesh):
    tokens = P("dp", "sp", None)
    quarters = mesh.shape["sp"] == 4 and mesh.shape["dp"] == 8
    return jax.shard_map(
        fused_body if quarters else body,
        mesh=mesh,
        in_specs=(tokens, tokens, tokens, P(None, "sp"), P(), P("dp", None)),
        out_specs=(tokens, tokens, P(None, "sp"), P(), P("dp", None)),
        check_vma=False,
    )
```
